128 devices in a mesh: sp: 16 (over z, y), tp: 8 (over x, core).
Axes of the slice: x: 4, y: 4, z: 4, core: 2. Of those that a mesh axis runs over, the one named last changes fastest.
Arguments:
- resid: bfloat16 [6144, 2048], P('sp', 'tp'), may hold values from -6 to 6
- mixer_in: bfloat16 [6144, 2048], P('sp', 'tp'), may hold values from -6 to 6
- log_step: float32 [6144, 128], P('sp', 'tp'), may hold values from -5.2 to -0.79
- decay_real: float32 [128, 64], P('tp'), may hold values from 8.138021e-05 to 0.8
- frequency: float32 [128, 64], P('tp'), may hold values from 0.5 to 6
- input_matrix: float32 [2, 128, 64, 16], P(None, 'tp'), may hold values from -1 to 1
- output_matrix: float32 [2, 128, 16, 64], P(None, 'tp'), may hold values from -0.5 to 0.5
- skip_gain: float32 [2048], P('tp'), may hold values from -4 to 4
- value_weight: bfloat16 [2048, 2048], P(None, 'tp'), may hold values from -0.125 to 0.125
- gate_weight: bfloat16 [2048, 2048], P(None, 'tp'), may hold values from -0.125 to 0.125
- norm_gain: float32 [2048], replicated, may hold values from 0.1 to 1.9
- up_weight: bfloat16 [2048, 8192], P('sp', 'tp'), may hold values from -0.125 to 0.125
- down_weight: bfloat16 [2048, 8192], P('sp', 'tp'), may hold values from -0.0625 to 0.0625
Outputs:
- result: bfloat16 [6144, 2048], P('sp', 'tp')
The draws below stay inside these ranges and needn't reach their ends.
All inputs are finite; a program needn't handle non-finite values.
Results may differ from the reference program's by a relative error of at most 0.014.
Values may be sent and summed in bfloat16 or wider, within the bound.
A program may use at most 128 MiB of HBM per device.

```python
import math
import jax
import jax.numpy as jnp
from jax import lax

D = 2048
FF = 8192
GC = 16
N = 64
TOK_DEV = 384
G = 128
TOKENS = 6144
FF_BLOCK = 1024
N_TP = 8


def draw_log_step(key, part):
    subkeys = jax.random.split(key, 3)
    device_count = TOKENS // TOK_DEV
    device_shift = jax.random.uniform(subkeys[0], (device_count, 1, 1), jnp.float32, -0.7, 0.7)
    group_shift = jax.random.uniform(subkeys[1], (1, 1, G), jnp.float32, -0.5, 0.5)
    jitter = jnp.clip(0.35 * jax.random.normal(subkeys[2], (device_count, TOK_DEV, G), jnp.float32), -1.0, 1.0)
    return (math.log(0.05) + device_shift + group_shift + jitter).reshape(TOKENS, G)


def draw_decay_real(key, part):
    subkeys = jax.random.split(key, 3)
    slow_share = 0.5
    chooser = jax.random.uniform(subkeys[0], (G, N), jnp.float32)
    slow_rate = jnp.exp(jax.random.uniform(subkeys[1], (G, N), jnp.float32, math.log(0.5), math.log(8.0))) / TOKENS
    fast_rate = jnp.exp(jax.random.uniform(subkeys[2], (G, N), jnp.float32, math.log(0.3), math.log(0.8)))
    return jnp.where(chooser < slow_share, slow_rate, fast_rate)


def shard_levels(rng, extent, cuts, smallest, high):
    factor_of = 1.0
    for dim, shards_of in cuts:
        steps = jax.random.uniform(jax.random.fold_in(jax.random.fold_in(rng, 6), dim), (shards_of,), jnp.float32, smallest / len(cuts), high / len(cuts))
        factor_of = factor_of * jnp.repeat(jnp.exp(steps), extent[dim] // shards_of).reshape((-1,) + (1,) * (len(extent) - 1 - dim))
    return factor_of


def normal_values(rng, shape, scale, most, cuts=(), held_as=jnp.bfloat16):
    factor_of = shard_levels(rng, shape, cuts, -0.22, 0.18) if cuts else 1.0
    drawn = jax.random.normal(rng, shape, jnp.float32) * scale * factor_of
    return jnp.minimum(jnp.maximum(drawn, -most), most).astype(held_as)


def setup_inputs(seed: int = 0) -> dict:
    streams_of = jax.random.split(jax.random.key(seed), 14)
    resid = normal_values(streams_of[0], (TOKENS, D), 1.0, 6.0, ((0, 16), (1, 8)))
    mixer_in = normal_values(streams_of[1], (TOKENS, D), 1.0, 6.0, ((0, 16), (1, 8)))
    log_step = draw_log_step(jax.random.fold_in(streams_of[13], 71), 0)
    decay_real = draw_decay_real(jax.random.fold_in(streams_of[13], 71), 0)
    frequency = jnp.clip(0.5 + 5.5 * jax.random.uniform(streams_of[4], (G, N), jnp.float32) ** shard_levels(streams_of[4], (G, N), ((0, 8),), -0.2, 0.2), 0.5, 6.0)
    input_matrix = normal_values(streams_of[5], (2, G, N, GC), (2 * GC) ** -0.5, 1.0, ((1, 8),), jnp.float32)
    output_matrix = normal_values(streams_of[6], (2, G, GC, N), (2 * N) ** -0.5, 0.5, ((1, 8),), jnp.float32)
    skip_gain = normal_values(streams_of[7], (D,), 1.0, 4.0, ((0, 8),), jnp.float32)
    value_weight = normal_values(streams_of[8], (D, D), D ** -0.5, 0.125, ((1, 8),))
    gate_weight = normal_values(streams_of[9], (D, D), D ** -0.5, 0.125, ((1, 8),))
    norm_gain = jnp.clip(1.0 + 0.18 * jax.random.normal(streams_of[10], (D,), jnp.float32), 0.1, 1.9)
    up_weight = normal_values(streams_of[11], (D, FF), D ** -0.5, 0.125, ((0, 16), (1, 8)))
    down_weight = normal_values(streams_of[12], (D, FF), FF ** -0.5, 0.0625, ((0, 16), (1, 8)))
    return dict(resid=resid, mixer_in=mixer_in, log_step=log_step, decay_real=decay_real, frequency=frequency, input_matrix=input_matrix, output_matrix=output_matrix, skip_gain=skip_gain, value_weight=value_weight, gate_weight=gate_weight, norm_gain=norm_gain, up_weight=up_weight, down_weight=down_weight)


rms_eps = 1e-06
highest = lax.Precision.HIGHEST

def chain_link(earlier, later):
    return (earlier[0] * later[0] - earlier[1] * later[1], earlier[0] * later[1] + earlier[1] * later[0], later[0] * earlier[2] - later[1] * earlier[3] + later[2], later[0] * earlier[3] + later[1] * earlier[2] + later[3])

def discretize(log_step, decay_real, frequency):
    states = decay_real.shape[1]
    step_size = jnp.repeat(jnp.exp(log_step), states, axis=1)
    decay_rate = decay_real.reshape(-1)
    angular = frequency.reshape(-1)
    shrink = -decay_rate * step_size
    rotation = angular * step_size
    factor = jnp.exp(shrink)
    decay_re = factor * jnp.cos(rotation)
    decay_im = factor * jnp.sin(rotation)
    half_sine = jnp.sin(0.5 * rotation)
    minus_re = jnp.expm1(shrink) * jnp.cos(rotation) - 2.0 * half_sine * half_sine
    minus_im = decay_im
    modulus = decay_rate * decay_rate + angular * angular
    drive_re = (minus_im * angular - minus_re * decay_rate) / modulus
    drive_im = (-minus_im * decay_rate - minus_re * angular) / modulus
    return (decay_re, decay_im, drive_re, drive_im)

def local_states(mixer_in, log_step, decay_real, frequency, input_matrix):
    tokens = mixer_in.shape[0]
    groups, states = decay_real.shape
    signal = mixer_in.astype(jnp.float32).reshape(tokens, groups, -1)
    proj_re = jnp.einsum('tgk,gnk->tgn', signal, input_matrix[0], precision=highest).reshape(tokens, groups * states)
    proj_im = jnp.einsum('tgk,gnk->tgn', signal, input_matrix[1], precision=highest).reshape(tokens, groups * states)
    decay_re, decay_im, drive_re, drive_im = discretize(log_step, decay_real, frequency)
    feed_re = drive_re * proj_re - drive_im * proj_im
    feed_im = drive_re * proj_im + drive_im * proj_re
    return lax.associative_scan(chain_link, (decay_re, decay_im, feed_re, feed_im), axis=0)

def read_out(state_re, state_im, output_matrix):
    tokens = state_re.shape[0]
    groups = output_matrix.shape[1]
    grid_re = state_re.reshape(tokens, groups, -1)
    grid_im = state_im.reshape(tokens, groups, -1)
    output = jnp.einsum('tgn,gkn->tgk', grid_re, output_matrix[0], precision=highest)
    output = output - jnp.einsum('tgn,gkn->tgk', grid_im, output_matrix[1], precision=highest)
    return output.reshape(tokens, -1)

def reference(resid, mixer_in, log_step, decay_real, frequency, input_matrix, output_matrix, skip_gain, value_weight, gate_weight, norm_gain, up_weight, down_weight):
    group_span = G // N_TP

    def one_block(block_index):
        first_group = block_index * group_span
        columns = lax.dynamic_slice_in_dim(mixer_in, first_group * GC, group_span * GC, 1)
        steps_part = lax.dynamic_slice_in_dim(log_step, first_group, group_span, 1)
        decay_part = lax.dynamic_slice_in_dim(decay_real, first_group, group_span, 0)
        angular = lax.dynamic_slice_in_dim(frequency, first_group, group_span, 0)
        matrix_in = lax.dynamic_slice_in_dim(input_matrix, first_group, group_span, 1)
        matrix_out = lax.dynamic_slice_in_dim(output_matrix, first_group, group_span, 1)
        _, _, state_re, state_im = local_states(columns, steps_part, decay_part, angular, matrix_in)
        return read_out(state_re, state_im, matrix_out)
    outputs = lax.map(one_block, jnp.arange(N_TP, dtype=jnp.int32))
    mechanism = jnp.transpose(outputs, (1, 0, 2)).reshape(TOKENS, D) + skip_gain * mixer_in.astype(jnp.float32)
    mixed_out = jax.nn.gelu(mechanism).astype(jnp.bfloat16)
    value_pre = jnp.dot(mixed_out, value_weight, preferred_element_type=jnp.float32)
    gate_pre = jnp.dot(mixed_out, gate_weight, preferred_element_type=jnp.float32)
    updated = (resid.astype(jnp.float32) + value_pre * jax.nn.sigmoid(gate_pre)).astype(jnp.bfloat16)
    updated_wide = lax.optimization_barrier(updated).astype(jnp.float32)
    inv_rms = lax.rsqrt(lax.optimization_barrier(jnp.mean(updated_wide * updated_wide, axis=1, keepdims=True)) + rms_eps)
    normed = (updated_wide * inv_rms * norm_gain).astype(jnp.bfloat16)
    raised = jnp.dot(normed, up_weight, preferred_element_type=jnp.float32)
    active = jax.nn.relu(raised)
    hidden = (active * active).astype(jnp.bfloat16)

    def add_block(running, block_index):
        start_unit = block_index * FF_BLOCK
        hidden_part = lax.dynamic_slice_in_dim(hidden, start_unit, FF_BLOCK, 1)
        weight_part = lax.dynamic_slice_in_dim(down_weight, start_unit, FF_BLOCK, 1)
        product = lax.dot_general(hidden_part, weight_part, (((1,), (1,)), ((), ())), preferred_element_type=jnp.float32).astype(jnp.bfloat16)
        product = lax.optimization_barrier(product)
        return (running + product.astype(jnp.float32), None)
    down_sum, _ = lax.scan(add_block, jnp.zeros((TOKENS, D), jnp.float32), jnp.arange(N_TP, dtype=jnp.int32))
    return (updated_wide + down_sum).astype(jnp.bfloat16)
```

```python
import functools
import math

import jax
import jax.numpy as jnp
from jax import lax
from jax.experimental import pallas as pl
from jax.experimental.pallas import tpu as pltpu
from jax.sharding import PartitionSpec as P

rms_eps = 1e-06
f32 = jnp.float32
bf16 = jnp.bfloat16
CHUNKS = 8


def onehot(shape, test):
    row = lax.broadcasted_iota(jnp.int32, shape, 0)
    col = lax.broadcasted_iota(jnp.int32, shape, 1)
    return jnp.where(test(row, col), 1.0, 0.0).astype(bf16)


def split3(x):
    hi = x.astype(bf16)
    rest = x - hi.astype(f32)
    mid = rest.astype(bf16)
    return hi, mid, (rest - mid.astype(f32)).astype(bf16)


def dot(a, b):
    return jnp.dot(a, b, preferred_element_type=f32)


def dot_t(a, b):
    return lax.dot_general(a, b, (((1,), (1,)), ((), ())), preferred_element_type=f32)


def spread_row(x, states):
    groups = x.shape[0]
    width = groups * states
    lanes = onehot((states, width), lambda r, c: r == c % states)
    wide = sum(dot(part, lanes) for part in split3(x))
    row = lax.broadcasted_iota(jnp.int32, wide.shape, 0)
    col = lax.broadcasted_iota(jnp.int32, wide.shape, 1)
    return jnp.sum(jnp.where(row == col // states, wide, 0.0), axis=0, keepdims=True)


def prepare(u_ref, ls_ref, dr_ref, fr_ref, bm_ref, cm_ref, uperm, step_wide, proj_re, proj_im, rows, wout):
    tokens, channels = u_ref.shape
    groups, states = dr_ref.shape
    width = groups * states
    per_group = channels // groups
    span = tokens // CHUNKS
    perm = onehot((tokens, tokens), lambda r, c: c == (r % CHUNKS) * span + r // CHUNKS)
    u_sorted = dot(perm, u_ref[...]).astype(bf16)
    uperm[...] = u_sorted
    decay = spread_row(dr_ref[...], states)
    angular = spread_row(fr_ref[...], states)
    rows[0:1, :] = -decay
    rows[1:2, :] = 0.5 * angular
    modulus = decay * decay + angular * angular
    inv_re = -decay / modulus
    inv_im = -angular / modulus
    step = jnp.exp(ls_ref[...])
    step = sum(dot(perm, part) for part in split3(step))
    group_lanes = onehot((groups, width), lambda r, c: r == c // states)
    step_wide[...] = sum(dot(part, group_lanes) for part in split3(step))
    pick = onehot((channels, per_group), lambda r, c: r % per_group == c)
    row = lax.broadcasted_iota(jnp.int32, (channels, width), 0)
    col = lax.broadcasted_iota(jnp.int32, (channels, width), 1)
    same = row // per_group == col // states
    b_re = dot_t(pick, bm_ref[0].astype(bf16))
    b_im = dot_t(pick, bm_ref[1].astype(bf16))
    w_re = jnp.where(same, b_re * inv_re - b_im * inv_im, 0.0).astype(bf16)
    w_im = jnp.where(same, b_re * inv_im + b_im * inv_re, 0.0).astype(bf16)
    proj_re[...] = dot(u_sorted, w_re)
    proj_im[...] = dot(u_sorted, w_im)
    state_lanes = onehot((states, width), lambda r, c: r == c % states)
    wout[:, :width] = jnp.where(same, dot(cm_ref[0].astype(bf16), state_lanes), 0.0).astype(bf16)
    wout[:, width:] = jnp.where(same, -dot(cm_ref[1].astype(bf16), state_lanes), 0.0).astype(bf16)


SIN = (-1.0 / 6, 1.0 / 120, -1.0 / 5040, 1.0 / 362880, -1.0 / 39916800)
COS = (-0.5, 1.0 / 24, -1.0 / 720, 1.0 / 40320, -1.0 / 3628800)


def series(q, terms):
    total = terms[-1] * q
    for term in terms[-2::-1]:
        total = (total + term) * q
    return total


def first_pass(step_wide, proj_re, proj_im, rows, dec_re, dec_im, ends):
    tokens, width = step_wide.shape
    block = 256

    def one_block(b, _):
        lanes = pl.ds(pl.multiple_of(b * block, block), block)
        minus_decay = jnp.broadcast_to(rows[0:1, lanes], (CHUNKS, block))
        half_angular = jnp.broadcast_to(rows[1:2, lanes], (CHUNKS, block))

        def one_step(i, carry):
            a_re, a_im, x_re, x_im = carry
            at = pl.ds(pl.multiple_of(i * CHUNKS, CHUNKS), CHUNKS)
            step = step_wide[at, lanes]
            half = step * half_angular
            q = half * half
            sine = half + half * series(q, SIN)
            cosine = 1.0 + series(q, COS)
            factor = jnp.exp(step * minus_decay)
            twice = factor * (sine + sine)
            d_re = factor - twice * sine
            d_im = twice * cosine
            less = d_re - 1.0
            p_re = proj_re[at, lanes]
            p_im = proj_im[at, lanes]
            u_re = less * p_re - d_im * p_im
            u_im = less * p_im + d_im * p_re
            dec_re[at, lanes] = d_re
            dec_im[at, lanes] = d_im
            proj_re[at, lanes] = u_re
            proj_im[at, lanes] = u_im
            return (
                d_re * a_re - d_im * a_im,
                d_re * a_im + d_im * a_re,
                d_re * x_re - d_im * x_im + u_re,
                d_re * x_im + d_im * x_re + u_im,
            )

        zero = jnp.zeros((CHUNKS, block), f32)
        found = lax.fori_loop(0, tokens // CHUNKS, one_step, (zero + 1.0, zero, zero, zero), unroll=2)
        for k in range(4):
            ends[k, :, lanes] = found[k]
        return 0

    lax.fori_loop(0, width // block, one_block, 0)


def chain(early, late):
    return (
        early[0] * late[0] - early[1] * late[1],
        early[0] * late[1] + early[1] * late[0],
        late[0] * early[2] - late[1] * early[3] + late[2],
        late[0] * early[3] + late[1] * early[2] + late[3],
    )


def chunk_prefix(ends, total):
    width = ends.shape[2]
    value = tuple(ends[k] for k in range(4))
    row = lax.broadcasted_iota(jnp.int32, value[0].shape, 0)
    unit = (1.0, 0.0, 0.0, 0.0)

    def moved(value, by):
        return tuple(
            jnp.where(row >= by, pltpu.roll(part, by, 0), zero) for part, zero in zip(value, unit)
        )

    for by in (1, 2, 4):
        value = chain(moved(value, by), value)
    for k in range(4):
        for j in range(width // 128):
            total[8 * k + j : 8 * k + j + 1, :] = value[k][CHUNKS - 1 :, 128 * j : 128 * j + 128]
    before = moved(value, 1)
    for k in range(4):
        ends[k] = before[k]


def second_pass(dec_re, dec_im, feed_re, feed_im, ends, carry, states):
    tokens, width = dec_re.shape
    block = 512
    for b in range(width // block):
        lanes = pl.ds(b * block, block)
        lanes_im = pl.ds(width + b * block, block)
        per = block // 128
        h_re = jnp.concatenate([carry[per * b + j : per * b + j + 1, :] for j in range(per)], axis=1)
        h_im = jnp.concatenate([carry[8 + per * b + j : 9 + per * b + j, :] for j in range(per)], axis=1)
        a_re, a_im = ends[0, :, lanes], ends[1, :, lanes]
        x_re = ends[2, :, lanes] + a_re * h_re - a_im * h_im
        x_im = ends[3, :, lanes] + a_re * h_im + a_im * h_re

        def one_step(i, value):
            x_re, x_im = value
            seen = []
            for k in range(2):
                at = pl.ds(pl.multiple_of(i * 2 * CHUNKS + k * CHUNKS, CHUNKS), CHUNKS)
                d_re, d_im = dec_re[at, lanes], dec_im[at, lanes]
                x_re, x_im = (
                    d_re * x_re - d_im * x_im + feed_re[at, lanes],
                    d_re * x_im + d_im * x_re + feed_im[at, lanes],
                )
                seen.append((x_re, x_im))
            both = pl.ds(pl.multiple_of(i * 2 * CHUNKS, 2 * CHUNKS), 2 * CHUNKS)
            states[both, lanes] = jnp.concatenate([seen[0][0], seen[1][0]], axis=0).astype(bf16)
            states[both, lanes_im] = jnp.concatenate([seen[0][1], seen[1][1]], axis=0).astype(bf16)
            return x_re, x_im

        lax.fori_loop(0, tokens // (2 * CHUNKS), one_step, (x_re, x_im), unroll=2)


def read_out(states, wout, uperm, skip_ref):
    tokens = states.shape[0]
    span = tokens // CHUNKS
    out = dot_t(states[...], wout[...]) + skip_ref[...] * uperm[...].astype(f32)
    mixed = jax.nn.gelu(out).astype(bf16)
    back = onehot((tokens, tokens), lambda r, c: r == (c % CHUNKS) * span + c // CHUNKS)
    return dot(back, mixed).astype(bf16)


def first_kernel(u_ref, ls_ref, dr_ref, fr_ref, bm_ref, cm_ref, dec_re, dec_im, feed_re, feed_im, ends, total, uperm, wout, step_wide, rows):
    prepare(u_ref, ls_ref, dr_ref, fr_ref, bm_ref, cm_ref, uperm, step_wide, feed_re, feed_im, rows, wout)
    first_pass(step_wide, feed_re, feed_im, rows, dec_re, dec_im, ends)
    chunk_prefix(ends, total)


def second_kernel(dec_re, dec_im, feed_re, feed_im, ends, uperm, wout, skip_ref, carry, mixed, states):
    second_pass(dec_re, dec_im, feed_re, feed_im, ends, carry, states)
    mixed[...] = read_out(states, wout, uperm, skip_ref)


def gather_pieces(value, axis, dim):
    copies = jnp.broadcast_to(value, (lax.axis_size(axis), *value.shape))
    pieces = lax.all_to_all(copies, axis, split_axis=0, concat_axis=0, tiled=True)
    pieces = jnp.moveaxis(pieces, 0, dim)
    lengths = pieces.shape
    return pieces.reshape(*lengths[:dim], lengths[dim] * lengths[dim + 1], *lengths[dim + 2 :])


def sent_and_summed(value, axis):
    devices = lax.axis_size(axis)
    pieces = jnp.moveaxis(value.reshape(value.shape[0], devices, -1), 1, 0)
    arrived = lax.all_to_all(pieces, axis, split_axis=0, concat_axis=0, tiled=True)
    return arrived.astype(f32).sum(axis=0)


def per_device(
    resid, mixer_in, log_step, decay_real, frequency, input_matrix, output_matrix, skip_gain,
    value_weight, gate_weight, norm_gain, up_weight, down_weight,
):
    both = jnp.concatenate((up_weight, down_weight), axis=1)
    whole = lax.all_gather(both, "sp", axis=0, tiled=True)
    up_whole, down_whole = jnp.split(whole, 2, axis=1)
    tokens, channels = mixer_in.shape
    groups, states = decay_real.shape
    width = groups * states
    wide = jax.ShapeDtypeStruct((tokens, width), f32)
    vmem = pl.BlockSpec(memory_space=pltpu.VMEM)
    dec_re, dec_im, feed_re, feed_im, ends, total, uperm, wout = pl.pallas_call(
        first_kernel,
        out_shape=(
            wide, wide, wide, wide,
            jax.ShapeDtypeStruct((4, CHUNKS, width), f32),
            jax.ShapeDtypeStruct((32, 128), f32),
            jax.ShapeDtypeStruct((tokens, channels), bf16),
            jax.ShapeDtypeStruct((channels, 2 * width), bf16),
        ),
        in_specs=[vmem] * 6,
        out_specs=[vmem] * 8,
        scratch_shapes=[pltpu.VMEM((tokens, width), f32), pltpu.VMEM((8, width), f32)],
        name="ssm_first",
        compiler_params=pltpu.CompilerParams(vmem_limit_bytes=40 * 2**20),
    )(
        mixer_in, log_step, decay_real, frequency,
        input_matrix.reshape(2, width, -1), output_matrix.reshape(2, channels, states),
    )
    everyone = lax.all_gather(total, "sp").reshape(-1, 4, 8, 128)
    here = lax.axis_index("sp")
    h_re = jnp.zeros((8, 128), f32)
    h_im = jnp.zeros((8, 128), f32)
    for j in range(everyone.shape[0]):
        a_re, a_im, x_re, x_im = everyone[j]
        n_re = a_re * h_re - a_im * h_im + x_re
        n_im = a_re * h_im + a_im * h_re + x_im
        h_re = jnp.where(j < here, n_re, h_re)
        h_im = jnp.where(j < here, n_im, h_im)
    carry = jnp.concatenate([h_re, h_im], axis=0)
    mixed_out = pl.pallas_call(
        second_kernel,
        out_shape=jax.ShapeDtypeStruct((tokens, channels), bf16),
        in_specs=[vmem] * 9,
        out_specs=vmem,
        scratch_shapes=[pltpu.VMEM((tokens, 2 * width), bf16)],
        name="ssm_second",
        compiler_params=pltpu.CompilerParams(vmem_limit_bytes=40 * 2**20),
    )(dec_re, dec_im, feed_re, feed_im, ends, uperm, wout, skip_gain.reshape(1, -1), carry)
    channels_all = gather_pieces(mixed_out, "tp", 1)
    value_pre = jnp.dot(channels_all, value_weight, preferred_element_type=f32)
    gate_pre = jnp.dot(channels_all, gate_weight, preferred_element_type=f32)
    updated = (resid.astype(f32) + value_pre * jax.nn.sigmoid(gate_pre)).astype(bf16)
    updated_wide = lax.optimization_barrier(updated).astype(f32)
    whole_rows = gather_pieces(updated, "tp", 1).astype(f32)
    inv_rms = lax.rsqrt(jnp.mean(whole_rows * whole_rows, axis=1, keepdims=True) + rms_eps)
    normed = (whole_rows * inv_rms * norm_gain).astype(bf16)
    raised = jnp.dot(normed, up_whole, preferred_element_type=f32)
    active = jax.nn.relu(raised)
    hidden = (active * active).astype(bf16)
    partials = lax.dot_general(
        hidden, down_whole, (((1,), (1,)), ((), ())), preferred_element_type=f32
    )
    down_sum = sent_and_summed(partials.astype(bf16), "tp")
    return (updated_wide + down_sum).astype(bf16)


def solution(mesh):
    in_specs = (
        P("sp", "tp"), P("sp", "tp"), P("sp", "tp"), P("tp", None), P("tp", None),
        P(None, "tp", None, None), P(None, "tp", None, None), P("tp"),
        P(None, "tp"), P(None, "tp"), P(), P("sp", "tp"), P("sp", "tp"),
    )
    return jax.shard_map(
        per_device, mesh=mesh, in_specs=in_specs, out_specs=P("sp", "tp"), check_vma=False
    )
```

```python
import functools
import math

import jax
import jax.numpy as jnp
from jax import lax
from jax.experimental import pallas as pl
from jax.experimental.pallas import tpu as pltpu
from jax.sharding import PartitionSpec as P

rms_eps = 1e-06
f32 = jnp.float32
bf16 = jnp.bfloat16
CHUNKS = 8


def onehot(shape, test):
    row = lax.broadcasted_iota(jnp.int32, shape, 0)
    col = lax.broadcasted_iota(jnp.int32, shape, 1)
    return jnp.where(test(row, col), 1.0, 0.0).astype(bf16)


def split3(x):
    hi = x.astype(bf16)
    rest = x - hi.astype(f32)
    mid = rest.astype(bf16)
    return hi, mid, (rest - mid.astype(f32)).astype(bf16)


def dot(a, b):
    return jnp.dot(a, b, preferred_element_type=f32)


def dot_t(a, b):
    return lax.dot_general(a, b, (((1,), (1,)), ((), ())), preferred_element_type=f32)


def spread_row(x, states):
    groups = x.shape[0]
    width = groups * states
    lanes = onehot((states, width), lambda r, c: r == c % states)
    wide = sum(dot(part, lanes) for part in split3(x))
    row = lax.broadcasted_iota(jnp.int32, wide.shape, 0)
    col = lax.broadcasted_iota(jnp.int32, wide.shape, 1)
    return jnp.sum(jnp.where(row == col // states, wide, 0.0), axis=0, keepdims=True)


def prepare(u_ref, ls_ref, dr_ref, fr_ref, bm_ref, cm_ref, uperm, step_wide, proj_re, proj_im, rows, wout):
    tokens, channels = u_ref.shape
    groups, states = dr_ref.shape
    width = groups * states
    per_group = channels // groups
    span = tokens // CHUNKS
    perm = onehot((tokens, tokens), lambda r, c: c == (r % CHUNKS) * span + r // CHUNKS)
    u_sorted = dot(perm, u_ref[...]).astype(bf16)
    uperm[...] = u_sorted
    decay = spread_row(dr_ref[...], states)
    angular = spread_row(fr_ref[...], states)
    rows[0:1, :] = -decay
    rows[1:2, :] = 0.5 * angular
    modulus = decay * decay + angular * angular
    inv_re = -decay / modulus
    inv_im = -angular / modulus
    step = jnp.exp(ls_ref[...])
    step = sum(dot(perm, part) for part in split3(step))
    group_lanes = onehot((groups, width), lambda r, c: r == c // states)
    step_wide[...] = sum(dot(part, group_lanes) for part in split3(step))
    pick = onehot((channels, per_group), lambda r, c: r % per_group == c)
    row = lax.broadcasted_iota(jnp.int32, (channels, width), 0)
    col = lax.broadcasted_iota(jnp.int32, (channels, width), 1)
    same = row // per_group == col // states
    b_re = dot_t(pick, bm_ref[0].astype(bf16))
    b_im = dot_t(pick, bm_ref[1].astype(bf16))
    w_re = jnp.where(same, b_re * inv_re - b_im * inv_im, 0.0).astype(bf16)
    w_im = jnp.where(same, b_re * inv_im + b_im * inv_re, 0.0).astype(bf16)
    proj_re[...] = dot(u_sorted, w_re)
    proj_im[...] = dot(u_sorted, w_im)
    state_lanes = onehot((states, width), lambda r, c: r == c % states)
    wout[:, :width] = jnp.where(same, dot(cm_ref[0].astype(bf16), state_lanes), 0.0).astype(bf16)
    wout[:, width:] = jnp.where(same, -dot(cm_ref[1].astype(bf16), state_lanes), 0.0).astype(bf16)


SIN = (-1.0 / 6, 1.0 / 120, -1.0 / 5040, 1.0 / 362880, -1.0 / 39916800)
COS = (-0.5, 1.0 / 24, -1.0 / 720, 1.0 / 40320, -1.0 / 3628800)


def series(q, terms):
    total = terms[-1] * q
    for term in terms[-2::-1]:
        total = (total + term) * q
    return total


def first_pass(step_wide, proj_re, proj_im, rows, dec_re, dec_im, ends):
    tokens, width = step_wide.shape
    block = 256

    def one_block(b, _):
        lanes = pl.ds(pl.multiple_of(b * block, block), block)
        minus_decay = jnp.broadcast_to(rows[0:1, lanes], (CHUNKS, block))
        half_angular = jnp.broadcast_to(rows[1:2, lanes], (CHUNKS, block))

        def one_step(i, carry):
            a_re, a_im, x_re, x_im = carry
            at = pl.ds(pl.multiple_of(i * CHUNKS, CHUNKS), CHUNKS)
            step = step_wide[at, lanes]
            half = step * half_angular
            q = half * half
            sine = half + half * series(q, SIN)
            cosine = 1.0 + series(q, COS)
            factor = jnp.exp(step * minus_decay)
            twice = factor * (sine + sine)
            d_re = factor - twice * sine
            d_im = twice * cosine
            less = d_re - 1.0
            p_re = proj_re[at, lanes]
            p_im = proj_im[at, lanes]
            u_re = less * p_re - d_im * p_im
            u_im = less * p_im + d_im * p_re
            dec_re[at, lanes] = d_re
            dec_im[at, lanes] = d_im
            proj_re[at, lanes] = u_re
            proj_im[at, lanes] = u_im
            return (
                d_re * a_re - d_im * a_im,
                d_re * a_im + d_im * a_re,
                d_re * x_re - d_im * x_im + u_re,
                d_re * x_im + d_im * x_re + u_im,
            )

        zero = jnp.zeros((CHUNKS, block), f32)
        found = lax.fori_loop(0, tokens // CHUNKS, one_step, (zero + 1.0, zero, zero, zero), unroll=2)
        for k in range(4):
            ends[k, :, lanes] = found[k]
        return 0

    lax.fori_loop(0, width // block, one_block, 0)


def chain(early, late):
    return (
        early[0] * late[0] - early[1] * late[1],
        early[0] * late[1] + early[1] * late[0],
        late[0] * early[2] - late[1] * early[3] + late[2],
        late[0] * early[3] + late[1] * early[2] + late[3],
    )


def chunk_prefix(ends, total):
    width = ends.shape[2]
    value = tuple(ends[k] for k in range(4))
    row = lax.broadcasted_iota(jnp.int32, value[0].shape, 0)
    unit = (1.0, 0.0, 0.0, 0.0)

    def moved(value, by):
        return tuple(
            jnp.where(row >= by, pltpu.roll(part, by, 0), zero) for part, zero in zip(value, unit)
        )

    for by in (1, 2, 4):
        value = chain(moved(value, by), value)
    for k in range(4):
        for j in range(width // 128):
            total[8 * k + j : 8 * k + j + 1, :] = value[k][CHUNKS - 1 :, 128 * j : 128 * j + 128]
    before = moved(value, 1)
    for k in range(4):
        ends[k] = before[k]


def second_pass(dec_re, dec_im, feed_re, feed_im, ends, carry, states):
    tokens, width = dec_re.shape
    block = 512
    for b in range(width // block):
        lanes = pl.ds(b * block, block)
        lanes_im = pl.ds(width + b * block, block)
        per = block // 128
        h_re = jnp.concatenate([carry[per * b + j : per * b + j + 1, :] for j in range(per)], axis=1)
        h_im = jnp.concatenate([carry[8 + per * b + j : 9 + per * b + j, :] for j in range(per)], axis=1)
        a_re, a_im = ends[0, :, lanes], ends[1, :, lanes]
        x_re = ends[2, :, lanes] + a_re * h_re - a_im * h_im
        x_im = ends[3, :, lanes] + a_re * h_im + a_im * h_re

        def one_step(i, value):
            x_re, x_im = value
            seen = []
            for k in range(2):
                at = pl.ds(pl.multiple_of(i * 2 * CHUNKS + k * CHUNKS, CHUNKS), CHUNKS)
                d_re, d_im = dec_re[at, lanes], dec_im[at, lanes]
                x_re, x_im = (
                    d_re * x_re - d_im * x_im + feed_re[at, lanes],
                    d_re * x_im + d_im * x_re + feed_im[at, lanes],
                )
                seen.append((x_re, x_im))
            both = pl.ds(pl.multiple_of(i * 2 * CHUNKS, 2 * CHUNKS), 2 * CHUNKS)
            states[both, lanes] = jnp.concatenate([seen[0][0], seen[1][0]], axis=0).astype(bf16)
            states[both, lanes_im] = jnp.concatenate([seen[0][1], seen[1][1]], axis=0).astype(bf16)
            return x_re, x_im

        lax.fori_loop(0, tokens // (2 * CHUNKS), one_step, (x_re, x_im), unroll=2)


def read_out(states, wout, uperm, skip_ref):
    tokens = states.shape[0]
    span = tokens // CHUNKS
    out = dot_t(states[...], wout[...]) + skip_ref[...] * uperm[...].astype(f32)
    mixed = jax.nn.gelu(out).astype(bf16)
    back = onehot((tokens, tokens), lambda r, c: r == (c % CHUNKS) * span + c // CHUNKS)
    return dot(back, mixed).astype(bf16)


AXES = pl.DeviceIdType.MESH
SIDE = 4


def around(index, by):
    return lax.rem(index + by + SIDE, SIDE)


class Relay:
    def __init__(self, buf, send_sem, recv_sem, y_first):
        here = lax.axis_index("sp")
        z, y = here // SIDE, lax.rem(here, SIDE)
        self.p, self.q = (y, z) if y_first else (z, y)
        self.y_first = y_first
        self.buf, self.send_sem, self.recv_sem = buf, send_sem, recv_sem
        self.rows = buf.shape[0] // (SIDE * SIDE)
        self.started = []

    def index(self, dp, dq):
        p, q = around(self.p, dp), around(self.q, dq)
        return q * SIDE + p if self.y_first else p * SIDE + q

    def copy(self, number, slot, half, target):
        rows = self.rows // 2
        piece = self.buf.at[pl.ds(pl.multiple_of(slot * self.rows + half * rows, rows), rows), :]
        return pltpu.make_async_remote_copy(
            src_ref=piece,
            dst_ref=piece,
            send_sem=self.send_sem.at[number],
            recv_sem=self.recv_sem.at[slot * 2 + half],
            device_id={"sp": target, "tp": lax.axis_index("tp")},
            device_id_type=AXES,
        )

    def send(self, slot, half, dp, dq):
        copy = self.copy(len(self.started), slot, half, self.index(dp, dq))
        copy.start()
        self.started.append(copy)

    def arrived(self, dp, dq, half):
        self.copy(0, self.index(dp, dq), half, self.index(1, 0)).wait_recv()

    def start_p(self):
        own = self.index(0, 0)
        for k in range(2):
            self.send(own, k, 1, 0)
            self.send(own, 1 - k, -1, 0)

    def send_q(self, slot):
        for k in range(2):
            self.send(slot, k, 0, 1)
            self.send(slot, 1 - k, 0, -1)

    def forward_p(self):
        self.arrived(-1, 0, 0)
        self.send(self.index(-1, 0), 0, 1, 0)
        self.arrived(1, 0, 1)
        self.send(self.index(1, 0), 1, -1, 0)

    def serve_near(self):
        self.arrived(-1, 0, 1)
        self.send_q(self.index(-1, 0))
        self.arrived(1, 0, 0)
        self.send_q(self.index(1, 0))

    def serve_far(self):
        self.arrived(2, 0, 0)
        self.arrived(2, 0, 1)
        self.send_q(self.index(2, 0))

    def forward_q(self, dp):
        self.arrived(dp, -1, 0)
        self.send(self.index(dp, -1), 0, 0, 1)
        self.arrived(dp, 1, 1)
        self.send(self.index(dp, 1), 1, 0, -1)

    def finish(self, dp):
        self.arrived(dp, -1, 1)
        self.arrived(dp, 1, 0)
        self.arrived(dp, 2, 0)
        self.arrived(dp, 2, 1)

    def drain(self):
        for copy in self.started:
            copy.wait_send()


class Gather:
    def __init__(self, buf, send_sem, recv_sem):
        here = lax.axis_index("tp")
        self.x, self.core = here // 2, lax.rem(here, 2)
        self.buf, self.send_sem, self.recv_sem = buf, send_sem, recv_sem
        self.started = []

    def slot(self, dx, other=False):
        core = 1 - self.core if other else self.core
        return around(self.x, dx) * 2 + core

    def copy(self, number, slot, half, target):
        rows = self.buf.shape[1] // 2
        piece = self.buf.at[slot, half * rows : half * rows + rows, :]
        return pltpu.make_async_remote_copy(
            src_ref=piece,
            dst_ref=piece,
            send_sem=self.send_sem.at[number],
            recv_sem=self.recv_sem.at[slot * 2 + half],
            device_id={"sp": lax.axis_index("sp"), "tp": target},
            device_id_type=AXES,
        )

    def send(self, dx, half, target):
        copy = self.copy(len(self.started), self.slot(dx), half, target)
        copy.start()
        self.started.append(copy)

    def arrived(self, dx, half, other=False):
        self.copy(0, self.slot(dx, other), half, self.slot(1)).wait_recv()

    def start(self):
        for k in range(2):
            self.send(0, k, self.slot(1))
            self.send(0, 1 - k, self.slot(-1))
        for k in range(2):
            self.send(0, k, self.slot(0, True))

    def serve_near(self):
        self.arrived(-1, 0)
        self.send(-1, 0, self.slot(1))
        self.arrived(1, 1)
        self.send(1, 1, self.slot(-1))
        self.send(-1, 0, self.slot(0, True))
        self.send(1, 1, self.slot(0, True))
        self.arrived(-1, 1)
        self.send(-1, 1, self.slot(0, True))
        self.arrived(1, 0)
        self.send(1, 0, self.slot(0, True))

    def serve_far(self):
        for k in range(2):
            self.arrived(2, k)
            self.send(2, k, self.slot(0, True))

    def finish(self):
        for dx in (0, -1, 1, 2):
            for k in range(2):
                self.arrived(dx, k, True)

    def drain(self):
        for copy in self.started:
            copy.wait_send()


def layer_kernel(
    resid_ref, u_ref, ls_ref, dr_ref, fr_ref, bm_ref, cm_ref, skip_ref, vw_ref, gw_ref, gain_ref, up_ref, down_ref,
    out_ref,
    up_all, down_all, vg, dec_re, dec_im, feed_re, feed_im, step_wide, rows, ends, total, totals, carry,
    uperm, wout, states, mixed_all, upd_all, normed, glu, hidden, stage_pair, from_pair, mine,
    stage_far, stage_right, stage_left, relay_left, relay_right, from_left, from_right,
    local_sem, up_send, up_recv, down_send, down_recv, tot_send, tot_recv,
    mix_send, mix_recv, upd_send, upd_recv, pair_send, pair_recv, sum_send, sum_recv,
):
    here, lane = lax.axis_index("sp"), lax.axis_index("tp")
    planes = SIDE * SIDE
    tokens, piece = resid_ref.shape
    half = tokens // 2
    up = Relay(up_all, up_send, up_recv, True)
    down = Relay(down_all, down_send, down_recv, False)
    mix = Gather(mixed_all, mix_send, mix_recv)
    upd = Gather(upd_all, upd_send, upd_recv)
    right, left, partner = mix.slot(1), mix.slot(-1), mix.slot(0, True)

    barrier = pltpu.get_barrier_semaphore()
    for by in range(1, planes):
        pl.semaphore_signal(
            barrier, inc=1, device_id={"sp": lax.rem(here + by, planes), "tp": lane}, device_id_type=AXES
        )
    for target in (right, left, partner):
        pl.semaphore_signal(barrier, inc=1, device_id={"sp": here, "tp": target}, device_id_type=AXES)

    own_rows = pl.ds(pl.multiple_of(here * up.rows, up.rows), up.rows)
    local = [
        pltpu.make_async_copy(up_ref, up_all.at[own_rows, :], local_sem.at[0]),
        pltpu.make_async_copy(down_ref, down_all.at[own_rows, :], local_sem.at[1]),
        pltpu.make_async_copy(vw_ref, vg.at[:, :piece], local_sem.at[2]),
        pltpu.make_async_copy(gw_ref, vg.at[:, piece:], local_sem.at[3]),
    ]
    for copy in local:
        copy.start()
    local[0].wait()
    local[1].wait()
    pl.semaphore_wait(barrier, planes + 2)
    up.start_p()
    down.start_p()

    prepare(u_ref, ls_ref, dr_ref, fr_ref, bm_ref, cm_ref, uperm, step_wide, feed_re, feed_im, rows, wout)
    first_pass(step_wide, feed_re, feed_im, rows, dec_re, dec_im, ends)
    chunk_prefix(ends, total)

    def total_copy(by, slot, target):
        return pltpu.make_async_remote_copy(
            src_ref=total,
            dst_ref=totals.at[slot],
            send_sem=tot_send.at[by],
            recv_sem=tot_recv.at[slot],
            device_id={"sp": target, "tp": lane},
            device_id_type=AXES,
        )

    for by in range(1, planes):
        @pl.when(here + by < planes)
        def _():
            total_copy(by, here, lax.rem(here + by, planes)).start()

    up.forward_p()
    down.forward_p()
    own_up, own_down = up.index(0, 0), down.index(0, 0)
    up.send_q(own_up)
    down.send_q(own_down)
    up.serve_near()
    down.serve_near()

    def fold(j, value):
        h_re, h_im = value
        total_copy(0, j, lax.rem(here + 1, planes)).wait_recv()
        a_re, a_im = totals[j, 0:8, :], totals[j, 8:16, :]
        x_re, x_im = totals[j, 16:24, :], totals[j, 24:32, :]
        return a_re * h_re - a_im * h_im + x_re, a_re * h_im + a_im * h_re + x_im

    zero = jnp.zeros((8, 128), f32)
    h_re, h_im = lax.fori_loop(0, here, fold, (zero, zero))
    carry[0:8, :] = h_re
    carry[8:16, :] = h_im
    second_pass(dec_re, dec_im, feed_re, feed_im, ends, carry, states)
    mixed_all[lane] = read_out(states, wout, uperm, skip_ref)
    mix.start()
    up.serve_far()
    down.serve_far()
    mix.serve_near()
    mix.serve_far()
    mix.finish()

    local[2].wait()
    local[3].wait()
    glu[...] = jnp.zeros_like(glu)

    def glu_step(s, _):
        at = pl.ds(pl.multiple_of(s * piece, piece), piece)
        glu[...] += dot(mixed_all[s], vg[at, :])
        return 0

    slots = mixed_all.shape[0]
    lax.fori_loop(0, slots, glu_step, 0)
    updated = (resid_ref[...].astype(f32) + glu[:, :piece] * jax.nn.sigmoid(glu[:, piece:])).astype(bf16)
    upd_all[lane] = updated
    upd.start()
    up.forward_q(0)
    down.forward_q(0)
    upd.serve_near()
    upd.serve_far()
    up.forward_q(-1)
    down.forward_q(-1)
    up.forward_q(1)
    down.forward_q(1)
    upd.finish()

    def square_step(s, total):
        wide = upd_all[s].astype(f32)
        return total + jnp.sum(wide * wide, axis=1, keepdims=True)

    squares = lax.fori_loop(0, slots, square_step, jnp.zeros((tokens, 1), f32))
    inv_rms = lax.rsqrt(squares / (slots * piece) + rms_eps)
    for s in range(slots):
        at = slice(s * piece, s * piece + piece)
        normed[:, at] = (upd_all[s].astype(f32) * inv_rms * gain_ref[:, at]).astype(bf16)
    up.forward_q(2)
    down.forward_q(2)
    for dp in (0, -1, 1, 2):
        up.finish(dp)

    def up_step(n, _):
        at = pl.ds(pl.multiple_of(n * piece, piece), piece)
        active = jnp.maximum(dot(normed[...], up_all[:, at]), 0.0)
        hidden[:, at] = (active * active).astype(bf16)
        return 0

    lax.fori_loop(0, hidden.shape[1] // piece, up_step, 0)
    for dp in (0, -1, 1, 2):
        down.finish(dp)

    def product(slot):
        at = pl.ds(pl.multiple_of(slot * piece, piece), piece)
        return dot_t(hidden[...], down_all[at, :])

    def sum_copy(number, src, dst, target, send_sem, recv_sem):
        return pltpu.make_async_remote_copy(
            src_ref=src,
            dst_ref=dst,
            send_sem=send_sem.at[number],
            recv_sem=recv_sem.at[number],
            device_id={"sp": here, "tp": target},
            device_id_type=AXES,
        )

    order = (2, 1, -1, 0)
    pairs = []
    for k, dx in enumerate(order):
        stage_pair[k] = product(mix.slot(dx, True)).astype(bf16)
        copy = sum_copy(k, stage_pair.at[k], from_pair.at[k], partner, pair_send, pair_recv)
        copy.start()
        pairs.append(copy)
    sums = [
        sum_copy(0, stage_far.at[:half, :], relay_left, right, sum_send, sum_recv),
        sum_copy(1, stage_far.at[half:, :], relay_right, left, sum_send, sum_recv),
        sum_copy(2, stage_right.at[half:, :], from_left.at[half:, :], right, sum_send, sum_recv),
        sum_copy(3, stage_left.at[:half, :], from_right.at[:half, :], left, sum_send, sum_recv),
        sum_copy(4, stage_right.at[:half, :], from_left.at[:half, :], right, sum_send, sum_recv),
        sum_copy(5, stage_left.at[half:, :], from_right.at[half:, :], left, sum_send, sum_recv),
    ]
    for k, dx in enumerate(order):
        mine[...] = product(mix.slot(dx))
        pairs[k].wait_recv()
        mine[...] += from_pair[k].astype(f32)
        if k == 0:
            stage_far[...] = mine[...].astype(bf16)
            sums[0].start()
            sums[1].start()
        elif k == 1:
            stage_right[half:, :] = mine[half:, :].astype(bf16)
            sums[2].start()
            sums[0].wait_recv()
            stage_right[:half, :] = (mine[:half, :] + relay_left[...].astype(f32)).astype(bf16)
            sums[4].start()
        elif k == 2:
            stage_left[:half, :] = mine[:half, :].astype(bf16)
            sums[3].start()
            sums[1].wait_recv()
            stage_left[half:, :] = (mine[half:, :] + relay_right[...].astype(f32)).astype(bf16)
            sums[5].start()
    for k in range(2, 6):
        sums[k].wait_recv()
    result = upd_all[lane].astype(f32) + (mine[...] + from_left[...].astype(f32) + from_right[...].astype(f32))
    out_ref[...] = result.astype(bf16)

    for by in range(1, planes):
        @pl.when(here + by < planes)
        def _():
            total_copy(by, here, lax.rem(here + by, planes)).wait_send()

    for ring in (up, down, mix, upd):
        ring.drain()
    for copy in pairs + sums:
        copy.wait_send()


def per_device(
    resid, mixer_in, log_step, decay_real, frequency, input_matrix, output_matrix, skip_gain,
    value_weight, gate_weight, norm_gain, up_weight, down_weight,
):
    tokens, channels = mixer_in.shape
    groups, states = decay_real.shape
    width = groups * states
    planes, slots = lax.axis_size("sp"), lax.axis_size("tp")
    features = slots * channels
    hidden = up_weight.shape[1]
    vmem = pl.BlockSpec(memory_space=pltpu.VMEM)
    hbm = pl.BlockSpec(memory_space=pl.ANY)
    wide = pltpu.VMEM((tokens, width), f32)
    block = pltpu.VMEM((tokens, channels), bf16)
    halves = pltpu.VMEM((tokens // 2, channels), bf16)
    dma = pltpu.SemaphoreType.DMA
    return pl.pallas_call(
        layer_kernel,
        out_shape=jax.ShapeDtypeStruct((tokens, channels), bf16),
        in_specs=[vmem] * 8 + [hbm] * 2 + [vmem] + [hbm] * 2,
        out_specs=vmem,
        scratch_shapes=[
            pltpu.VMEM((features, hidden), bf16), pltpu.VMEM((features, hidden), bf16),
            pltpu.VMEM((features, 2 * channels), bf16),
            wide, wide, wide, wide, wide,
            pltpu.VMEM((8, width), f32), pltpu.VMEM((4, CHUNKS, width), f32),
            pltpu.VMEM((32, 128), f32), pltpu.VMEM((planes, 32, 128), f32), pltpu.VMEM((16, 128), f32),
            block, pltpu.VMEM((channels, 2 * width), bf16), pltpu.VMEM((tokens, 2 * width), bf16),
            pltpu.VMEM((slots, tokens, channels), bf16), pltpu.VMEM((slots, tokens, channels), bf16),
            pltpu.VMEM((tokens, features), bf16), pltpu.VMEM((tokens, 2 * channels), f32),
            pltpu.VMEM((tokens, hidden), bf16),
            pltpu.VMEM((4, tokens, channels), bf16), pltpu.VMEM((4, tokens, channels), bf16),
            pltpu.VMEM((tokens, channels), f32),
            block, block, block, halves, halves, block, block,
            dma((4,)), dma((30,)), dma((2 * planes,)), dma((30,)), dma((2 * planes,)),
            dma((planes,)), dma((planes,)),
            dma((14,)), dma((2 * slots,)), dma((14,)), dma((2 * slots,)),
            dma((4,)), dma((4,)), dma((6,)), dma((6,)),
        ],
        name="layer",
        compiler_params=pltpu.CompilerParams(
            vmem_limit_bytes=58 * 2**20, collective_id=0, has_side_effects=True
        ),
    )(
        resid, mixer_in, log_step, decay_real, frequency,
        input_matrix.reshape(2, width, -1), output_matrix.reshape(2, channels, states),
        skip_gain.reshape(1, -1), value_weight, gate_weight, norm_gain.reshape(1, -1), up_weight, down_weight,
    )


def solution(mesh):
    in_specs = (
        P("sp", "tp"), P("sp", "tp"), P("sp", "tp"), P("tp", None), P("tp", None),
        P(None, "tp", None, None), P(None, "tp", None, None), P("tp"),
        P(None, "tp"), P(None, "tp"), P(), P("sp", "tp"), P("sp", "tp"),
    )
    return jax.shard_map(
        per_device, mesh=mesh, in_specs=in_specs, out_specs=P("sp", "tp"), check_vma=False
    )
```

```python
import functools
import math

import jax
import jax.numpy as jnp
from jax import lax
from jax.experimental import pallas as pl
from jax.experimental.pallas import tpu as pltpu
from jax.sharding import PartitionSpec as P

rms_eps = 1e-06
f32 = jnp.float32
bf16 = jnp.bfloat16
CHUNKS = 8


def onehot(shape, test):
    row = lax.broadcasted_iota(jnp.int32, shape, 0)
    col = lax.broadcasted_iota(jnp.int32, shape, 1)
    return jnp.where(test(row, col), 1.0, 0.0).astype(bf16)


def split3(x):
    hi = x.astype(bf16)
    rest = x - hi.astype(f32)
    mid = rest.astype(bf16)
    return hi, mid, (rest - mid.astype(f32)).astype(bf16)


def dot(a, b):
    return jnp.dot(a, b, preferred_element_type=f32)


def dot_t(a, b):
    return lax.dot_general(a, b, (((1,), (1,)), ((), ())), preferred_element_type=f32)


def spread_row(x, states):
    groups = x.shape[0]
    width = groups * states
    lanes = onehot((states, width), lambda r, c: r == c % states)
    wide = sum(dot(part, lanes) for part in split3(x))
    row = lax.broadcasted_iota(jnp.int32, wide.shape, 0)
    col = lax.broadcasted_iota(jnp.int32, wide.shape, 1)
    return jnp.sum(jnp.where(row == col // states, wide, 0.0), axis=0, keepdims=True)


def prepare(u_ref, ls_ref, dr_ref, fr_ref, bm_ref, cm_ref, uperm, step_wide, proj_re, proj_im, rows, wout):
    tokens, channels = u_ref.shape
    groups, states = dr_ref.shape
    width = groups * states
    per_group = channels // groups
    span = tokens // CHUNKS
    perm = onehot((tokens, tokens), lambda r, c: c == (r % CHUNKS) * span + r // CHUNKS)
    u_sorted = dot(perm, u_ref[...]).astype(bf16)
    uperm[...] = u_sorted
    decay = spread_row(dr_ref[...], states)
    angular = spread_row(fr_ref[...], states)
    rows[0:1, :] = -decay
    rows[1:2, :] = 0.5 * angular
    modulus = decay * decay + angular * angular
    inv_re = -decay / modulus
    inv_im = -angular / modulus
    step = jnp.exp(ls_ref[...])
    step = sum(dot_t(perm, part) for part in split3(step))
    group_lanes = onehot((groups, width), lambda r, c: r == c // states)
    step_wide[...] = sum(dot(part, group_lanes) for part in split3(step))
    state_lanes = onehot((states, width), lambda r, c: r == c % states)
    row = lax.broadcasted_iota(jnp.int32, (channels, width), 0)
    col = lax.broadcasted_iota(jnp.int32, (channels, width), 1)
    same = row // per_group == col // states
    b_re = dot(bm_ref[0].astype(bf16), state_lanes)
    b_im = dot(bm_ref[1].astype(bf16), state_lanes)
    w_re = jnp.where(same, b_re * inv_re - b_im * inv_im, 0.0).astype(bf16)
    w_im = jnp.where(same, b_re * inv_im + b_im * inv_re, 0.0).astype(bf16)
    proj_re[...] = dot(u_sorted, w_re)
    proj_im[...] = dot(u_sorted, w_im)
    wout[:, :width] = jnp.where(same, dot(cm_ref[0].astype(bf16), state_lanes), 0.0).astype(bf16)
    wout[:, width:] = jnp.where(same, -dot(cm_ref[1].astype(bf16), state_lanes), 0.0).astype(bf16)


SIN = (-1.0 / 6, 1.0 / 120, -1.0 / 5040, 1.0 / 362880, -1.0 / 39916800)
COS = (-0.5, 1.0 / 24, -1.0 / 720, 1.0 / 40320, -1.0 / 3628800)


def series(q, terms):
    total = terms[-1] * q
    for term in terms[-2::-1]:
        total = (total + term) * q
    return total


def first_pass(step_wide, proj_re, proj_im, rows, dec_re, dec_im, ends, first, last):
    tokens, width = step_wide.shape
    block = 256

    def one_block(b, _):
        lanes = pl.ds(pl.multiple_of(b * block, block), block)
        minus_decay = jnp.broadcast_to(rows[0:1, lanes], (CHUNKS, block))
        half_angular = jnp.broadcast_to(rows[1:2, lanes], (CHUNKS, block))

        def one_step(i, carry):
            a_re, a_im, x_re, x_im = carry
            at = pl.ds(pl.multiple_of(i * CHUNKS, CHUNKS), CHUNKS)
            step = step_wide[at, lanes]
            half = step * half_angular
            q = half * half
            sine = half + half * series(q, SIN)
            cosine = 1.0 + series(q, COS)
            factor = jnp.exp(step * minus_decay)
            twice = factor * (sine + sine)
            d_re = factor - twice * sine
            d_im = twice * cosine
            less = d_re - 1.0
            p_re = proj_re[at, lanes]
            p_im = proj_im[at, lanes]
            u_re = less * p_re - d_im * p_im
            u_im = less * p_im + d_im * p_re
            dec_re[at, lanes] = d_re
            dec_im[at, lanes] = d_im
            proj_re[at, lanes] = u_re
            proj_im[at, lanes] = u_im
            return (
                d_re * a_re - d_im * a_im,
                d_re * a_im + d_im * a_re,
                d_re * x_re - d_im * x_im + u_re,
                d_re * x_im + d_im * x_re + u_im,
            )

        zero = jnp.zeros((CHUNKS, block), f32)
        found = lax.fori_loop(0, tokens // CHUNKS, one_step, (zero + 1.0, zero, zero, zero), unroll=2)
        for k in range(4):
            ends[k, :, lanes] = found[k]
        return 0

    lax.fori_loop(first, last, one_block, 0)


def chain(early, late):
    return (
        early[0] * late[0] - early[1] * late[1],
        early[0] * late[1] + early[1] * late[0],
        late[0] * early[2] - late[1] * early[3] + late[2],
        late[0] * early[3] + late[1] * early[2] + late[3],
    )


def chunk_prefix(ends, total):
    width = ends.shape[2]
    value = tuple(ends[k] for k in range(4))
    row = lax.broadcasted_iota(jnp.int32, value[0].shape, 0)
    unit = (1.0, 0.0, 0.0, 0.0)

    def moved(value, by):
        return tuple(
            jnp.where(row >= by, pltpu.roll(part, by, 0), zero) for part, zero in zip(value, unit)
        )

    for by in (1, 2, 4):
        value = chain(moved(value, by), value)
    for k in range(4):
        for j in range(width // 128):
            total[8 * k + j : 8 * k + j + 1, :] = value[k][CHUNKS - 1 :, 128 * j : 128 * j + 128]
    before = moved(value, 1)
    for k in range(4):
        ends[k] = before[k]


def second_pass(dec_re, dec_im, feed_re, feed_im, ends, carry, states):
    tokens, width = dec_re.shape
    block = 512
    for b in range(width // block):
        lanes = pl.ds(b * block, block)
        lanes_im = pl.ds(width + b * block, block)
        per = block // 128
        h_re = jnp.concatenate([carry[per * b + j : per * b + j + 1, :] for j in range(per)], axis=1)
        h_im = jnp.concatenate([carry[8 + per * b + j : 9 + per * b + j, :] for j in range(per)], axis=1)
        a_re, a_im = ends[0, :, lanes], ends[1, :, lanes]
        x_re = ends[2, :, lanes] + a_re * h_re - a_im * h_im
        x_im = ends[3, :, lanes] + a_re * h_im + a_im * h_re

        def one_step(i, value):
            x_re, x_im = value
            seen = []
            for k in range(2):
                at = pl.ds(pl.multiple_of(i * 2 * CHUNKS + k * CHUNKS, CHUNKS), CHUNKS)
                d_re, d_im = dec_re[at, lanes], dec_im[at, lanes]
                x_re, x_im = (
                    d_re * x_re - d_im * x_im + feed_re[at, lanes],
                    d_re * x_im + d_im * x_re + feed_im[at, lanes],
                )
                seen.append((x_re, x_im))
            both = pl.ds(pl.multiple_of(i * 2 * CHUNKS, 2 * CHUNKS), 2 * CHUNKS)
            states[both, lanes] = jnp.concatenate([seen[0][0], seen[1][0]], axis=0).astype(bf16)
            states[both, lanes_im] = jnp.concatenate([seen[0][1], seen[1][1]], axis=0).astype(bf16)
            return x_re, x_im

        lax.fori_loop(0, tokens // (2 * CHUNKS), one_step, (x_re, x_im), unroll=2)


def read_out(states, wout, uperm, skip_ref):
    tokens = states.shape[0]
    span = tokens // CHUNKS
    out = dot_t(states[...], wout[...]) + skip_ref[...] * uperm[...].astype(f32)
    mixed = jax.nn.gelu(out).astype(bf16)
    back = onehot((tokens, tokens), lambda r, c: r == (c % CHUNKS) * span + c // CHUNKS)
    return dot(back, mixed).astype(bf16)


AXES = pl.DeviceIdType.MESH
SIDE = 4


def around(index, by):
    return lax.rem(index + by + SIDE, SIDE)


class Relay:
    def __init__(self, buf, send_sem, recv_sem, y_first):
        here = lax.axis_index("sp")
        z, y = here // SIDE, lax.rem(here, SIDE)
        self.p, self.q = (y, z) if y_first else (z, y)
        self.y_first = y_first
        self.buf, self.send_sem, self.recv_sem = buf, send_sem, recv_sem
        self.rows = buf.shape[0] // (SIDE * SIDE)
        self.started = []

    def index(self, dp, dq):
        p, q = around(self.p, dp), around(self.q, dq)
        return q * SIDE + p if self.y_first else p * SIDE + q

    def copy(self, number, slot, half, target):
        rows = self.rows // 2
        piece = self.buf.at[pl.ds(pl.multiple_of(slot * self.rows + half * rows, rows), rows), :]
        return pltpu.make_async_remote_copy(
            src_ref=piece,
            dst_ref=piece,
            send_sem=self.send_sem.at[number],
            recv_sem=self.recv_sem.at[slot * 2 + half],
            device_id={"sp": target, "tp": lax.axis_index("tp")},
            device_id_type=AXES,
        )

    def send(self, slot, half, dp, dq):
        copy = self.copy(len(self.started), slot, half, self.index(dp, dq))
        copy.start()
        self.started.append(copy)

    def arrived(self, dp, dq, half):
        self.copy(0, self.index(dp, dq), half, self.index(1, 0)).wait_recv()

    def start_p(self):
        own = self.index(0, 0)
        for k in range(2):
            self.send(own, k, 1, 0)
            self.send(own, 1 - k, -1, 0)

    def send_q(self, slot, part=(0, 1)):
        for k in part:
            self.send(slot, k, 0, 1)
            self.send(slot, 1 - k, 0, -1)

    def forward_p(self):
        self.arrived(-1, 0, 0)
        self.send(self.index(-1, 0), 0, 1, 0)
        self.arrived(1, 0, 1)
        self.send(self.index(1, 0), 1, -1, 0)

    def serve_near(self):
        self.arrived(-1, 0, 1)
        self.send_q(self.index(-1, 0))
        self.arrived(1, 0, 0)
        self.send_q(self.index(1, 0))

    def serve_far(self):
        self.arrived(2, 0, 0)
        self.arrived(2, 0, 1)
        self.send_q(self.index(2, 0))

    def forward_q(self, dp):
        self.arrived(dp, -1, 0)
        self.send(self.index(dp, -1), 0, 0, 1)
        self.arrived(dp, 1, 1)
        self.send(self.index(dp, 1), 1, 0, -1)

    def finish(self, dq):
        for dp in (0, -1, 1, 2):
            if dq == 2:
                self.arrived(dp, 2, 0)
                self.arrived(dp, 2, 1)
            elif dq:
                self.arrived(dp, dq, 1 if dq == -1 else 0)

    def drain(self):
        for copy in self.started:
            copy.wait_send()


class Gather:
    def __init__(self, buf, send_sem, recv_sem):
        here = lax.axis_index("tp")
        self.x, self.core = here // 2, lax.rem(here, 2)
        self.buf, self.send_sem, self.recv_sem = buf, send_sem, recv_sem
        self.started = []

    def slot(self, dx, other=False):
        core = 1 - self.core if other else self.core
        return around(self.x, dx) * 2 + core

    def copy(self, number, slot, half, target):
        rows = self.buf.shape[1] // 2
        piece = self.buf.at[slot, half * rows : half * rows + rows, :]
        return pltpu.make_async_remote_copy(
            src_ref=piece,
            dst_ref=piece,
            send_sem=self.send_sem.at[number],
            recv_sem=self.recv_sem.at[slot * 2 + half],
            device_id={"sp": lax.axis_index("sp"), "tp": target},
            device_id_type=AXES,
        )

    def send(self, dx, half, target):
        copy = self.copy(len(self.started), self.slot(dx), half, target)
        copy.start()
        self.started.append(copy)

    def arrived(self, dx, half, other=False):
        self.copy(0, self.slot(dx, other), half, self.slot(1)).wait_recv()

    def start(self):
        for k in range(2):
            self.send(0, k, self.slot(1))
            self.send(0, 1 - k, self.slot(-1))
        for k in range(2):
            self.send(0, k, self.slot(0, True))

    def serve_near(self):
        self.arrived(-1, 0)
        self.send(-1, 0, self.slot(1))
        self.arrived(1, 1)
        self.send(1, 1, self.slot(-1))
        self.send(-1, 0, self.slot(0, True))
        self.send(1, 1, self.slot(0, True))
        self.arrived(-1, 1)
        self.send(-1, 1, self.slot(0, True))
        self.arrived(1, 0)
        self.send(1, 0, self.slot(0, True))

    def serve_far(self):
        for k in range(2):
            self.arrived(2, k)
            self.send(2, k, self.slot(0, True))

    def finish(self):
        for dx in (0, -1, 1, 2):
            for k in range(2):
                self.arrived(dx, k, True)

    def drain(self):
        for copy in self.started:
            copy.wait_send()


class Phases:
    def __init__(self):
        self.scope = None

    def __call__(self, name):
        if self.scope is not None:
            self.scope.__exit__(None, None, None)
        self.scope = jax.named_scope(name) if name else None
        if self.scope is not None:
            self.scope.__enter__()


def layer_kernel(
    resid_hbm, u_hbm, ls_hbm, dr_hbm, fr_hbm, bm_hbm, cm_hbm, skip_hbm, gain_hbm, vw_ref, gw_ref, up_ref, down_ref,
    out_ref,
    resid_ref, u_ref, ls_ref, dr_ref, fr_ref, bm_ref, cm_ref, skip_ref, gain_ref,
    up_all, down_all, vg, dec_re, dec_im, feed_re, feed_im, step_wide, rows, ends, total, totals, carry,
    uperm, wout, states, mixed_all, upd_all, normed, glu, raised, hidden, stage_pair, from_pair, mine,
    stage_far, stage_right, stage_left, relay_left, relay_right, from_left, from_right,
    local_sem, round_sem, up_send, up_recv, down_send, down_recv, tot_send, tot_recv,
    mix_send, mix_recv, upd_send, upd_recv, pair_send, pair_recv, sum_send, sum_recv,
):
    phase = Phases()
    here, lane = lax.axis_index("sp"), lax.axis_index("tp")
    planes = SIDE * SIDE
    tokens, piece = resid_ref.shape
    half = tokens // 2
    up = Relay(up_all, up_send, up_recv, True)
    down = Relay(down_all, down_send, down_recv, False)
    mix = Gather(mixed_all, mix_send, mix_recv)
    upd = Gather(upd_all, upd_send, upd_recv)
    right, left, partner = mix.slot(1), mix.slot(-1), mix.slot(0, True)
    near_planes = [up.index(*by) for by in ((1, 0), (-1, 0), (0, 1), (0, -1))]

    phase("signal")
    barrier = pltpu.get_barrier_semaphore()
    for target in near_planes:
        pl.semaphore_signal(barrier, inc=1, device_id={"sp": target, "tp": lane}, device_id_type=AXES)
    for target in (right, left, partner):
        pl.semaphore_signal(barrier, inc=1, device_id={"sp": here, "tp": target}, device_id_type=AXES)

    own_rows = pl.ds(pl.multiple_of(here * up.rows, up.rows), up.rows)
    moves = (
        (up_ref, up_all.at[own_rows, :]), (down_ref, down_all.at[own_rows, :]),
        (u_hbm, u_ref), (dr_hbm, dr_ref), (fr_hbm, fr_ref), (ls_hbm, ls_ref), (bm_hbm, bm_ref), (cm_hbm, cm_ref),
        (skip_hbm, skip_ref), (vw_ref, vg.at[:, :piece]), (gw_ref, vg.at[:, piece:]),
        (resid_hbm, resid_ref), (gain_hbm, gain_ref),
    )
    local = [pltpu.make_async_copy(src, dst, local_sem.at[k]) for k, (src, dst) in enumerate(moves)]
    for copy in local:
        copy.start()
    local[0].wait()
    local[1].wait()
    phase("barrier")
    pl.semaphore_wait(barrier, 7)
    phase("start_p")
    own_up, own_down = up.index(0, 0), down.index(0, 0)
    up.start_p()
    down.start_p()
    up.send_q(own_up, (0,))
    down.send_q(own_down, (0,))

    def greet(number):
        for target in near_planes:
            pl.semaphore_signal(
                round_sem.at[number], inc=1, device_id={"sp": target, "tp": lane}, device_id_type=AXES
            )

    greet(0)
    for copy in local[2:8]:
        copy.wait()
    phase("prepare")
    prepare(u_ref, ls_ref, dr_ref, fr_ref, bm_ref, cm_ref, uperm, step_wide, feed_re, feed_im, rows, wout)
    pl.semaphore_wait(round_sem.at[0], 4)
    greet(1)
    phase("first_pass")
    scan_refs = (step_wide, feed_re, feed_im, rows, dec_re, dec_im, ends)
    first_pass(*scan_refs, 0, 2)
    pl.semaphore_wait(round_sem.at[1], 4)
    greet(2)
    first_pass(*scan_refs, 2, 4)
    phase("chunk")
    chunk_prefix(ends, total)
    pl.semaphore_wait(round_sem.at[2], 4)

    def total_copy(by, slot, target):
        return pltpu.make_async_remote_copy(
            src_ref=total,
            dst_ref=totals.at[slot],
            send_sem=tot_send.at[by],
            recv_sem=tot_recv.at[slot],
            device_id={"sp": target, "tp": lane},
            device_id_type=AXES,
        )

    phase("totals")
    for by in range(1, planes):
        @pl.when(here + by < planes)
        def _():
            total_copy(by, here, lax.rem(here + by, planes)).start()

    phase("forward_p")
    up.forward_p()
    down.forward_p()
    phase("send_q")
    up.send_q(own_up, (1,))
    down.send_q(own_down, (1,))
    phase("serve_near")
    up.serve_near()
    down.serve_near()

    phase("fold")

    def fold(j, value):
        h_re, h_im = value
        total_copy(0, j, lax.rem(here + 1, planes)).wait_recv()
        a_re, a_im = totals[j, 0:8, :], totals[j, 8:16, :]
        x_re, x_im = totals[j, 16:24, :], totals[j, 24:32, :]
        return a_re * h_re - a_im * h_im + x_re, a_re * h_im + a_im * h_re + x_im

    zero = jnp.zeros((8, 128), f32)
    h_re, h_im = lax.fori_loop(0, here, fold, (zero, zero))
    carry[0:8, :] = h_re
    carry[8:16, :] = h_im
    phase("second_pass")
    second_pass(dec_re, dec_im, feed_re, feed_im, ends, carry, states)
    local[8].wait()
    phase("read_out")
    mixed_all[lane] = read_out(states, wout, uperm, skip_ref)
    phase("mix_start")
    mix.start()
    phase("serve_far")
    up.serve_far()
    down.serve_far()
    up.forward_q(0)
    down.forward_q(0)
    phase("mix_near")
    mix.serve_near()
    phase("mix_far")
    mix.serve_far()
    phase("fq_minus")
    up.forward_q(-1)
    down.forward_q(-1)
    phase("mix_finish")
    mix.finish()

    phase("glu")
    for copy in local[9:]:
        copy.wait()
    glu[...] = jnp.zeros_like(glu)

    def glu_step(s, _):
        at = pl.ds(pl.multiple_of(s * piece, piece), piece)
        glu[...] += dot(mixed_all[s], vg[at, :])
        return 0

    slots = mixed_all.shape[0]
    lax.fori_loop(0, slots, glu_step, 0)
    updated = (resid_ref[...].astype(f32) + glu[:, :piece] * jax.nn.sigmoid(glu[:, piece:])).astype(bf16)
    upd_all[lane] = updated
    phase("upd_start")
    upd.start()
    phase("fq_plus")
    up.forward_q(1)
    down.forward_q(1)
    phase("upd_near")
    upd.serve_near()
    phase("fq_far")
    up.forward_q(2)
    down.forward_q(2)
    phase("upd_far")
    upd.serve_far()
    phase("upd_finish")
    upd.finish()

    phase("norm")

    def square_step(s, total):
        wide = upd_all[s].astype(f32)
        return total + jnp.sum(wide * wide, axis=1, keepdims=True)

    squares = lax.fori_loop(0, slots, square_step, jnp.zeros((tokens, 1), f32))
    inv_rms = lax.rsqrt(squares / (slots * piece) + rms_eps)
    for s in range(slots):
        at = slice(s * piece, s * piece + piece)
        normed[s // 2, :, s % 2 * piece : s % 2 * piece + piece] = (
            upd_all[s].astype(f32) * inv_rms * gain_ref[:, at]
        ).astype(bf16)

    width = hidden.shape[1]
    depth = normed.shape[2]
    for k, dq in enumerate((0, -1, 1, 2)):
        phase(f"up_wait{k}")
        up.finish(dq)
        phase(f"up_mm{k}")
        group = around(up.q, dq)
        deep = pl.ds(pl.multiple_of(group * depth, depth), depth)

        def up_step(n, _):
            at = pl.ds(pl.multiple_of(n * piece, piece), piece)
            product = dot(normed[group], up_all[deep, at])
            if k:
                product = product + raised[:, at]
            if k < 3:
                raised[:, at] = product
            else:
                active = jnp.maximum(product, 0.0)
                hidden[:, at] = (active * active).astype(bf16)
            return 0

        lax.fori_loop(0, width // piece, up_step, 0)
    phase("down_finish")
    for dq in (0, -1, 1, 2):
        down.finish(dq)

    def product(slot):
        at = pl.ds(pl.multiple_of(slot * piece, piece), piece)
        return dot_t(hidden[...], down_all[at, :])

    def sum_copy(number, src, dst, target, send_sem, recv_sem):
        return pltpu.make_async_remote_copy(
            src_ref=src,
            dst_ref=dst,
            send_sem=send_sem.at[number],
            recv_sem=recv_sem.at[number],
            device_id={"sp": here, "tp": target},
            device_id_type=AXES,
        )

    order = (2, 1, -1, 0)
    pairs = [
        sum_copy(k, stage_pair.at[k], from_pair.at[k], partner, pair_send, pair_recv) for k in range(len(order))
    ]
    sums = [
        sum_copy(0, stage_far.at[:half, :], relay_left, right, sum_send, sum_recv),
        sum_copy(1, stage_far.at[half:, :], relay_right, left, sum_send, sum_recv),
        sum_copy(2, stage_right.at[half:, :], from_left.at[half:, :], right, sum_send, sum_recv),
        sum_copy(3, stage_left.at[:half, :], from_right.at[:half, :], left, sum_send, sum_recv),
        sum_copy(4, stage_right.at[:half, :], from_left.at[:half, :], right, sum_send, sum_recv),
        sum_copy(5, stage_left.at[half:, :], from_right.at[half:, :], left, sum_send, sum_recv),
    ]

    def pair_step(k):
        stage_pair[k] = product(mix.slot(order[k], True)).astype(bf16)
        pairs[k].start()

    def own_step(k):
        mine[k] = product(mix.slot(order[k]))

    def pair_sum(k):
        pairs[k].wait_recv()
        return mine[k] + from_pair[k].astype(f32)

    phase("products")
    pair_step(0)
    own_step(0)
    pair_step(1)
    pair_step(2)
    phase("far")
    stage_far[...] = pair_sum(0).astype(bf16)
    sums[0].start()
    sums[1].start()
    phase("near")
    own_step(1)
    own_step(2)
    mine[1] = pair_sum(1)
    stage_right[half:, :] = mine[1, half:, :].astype(bf16)
    sums[2].start()
    mine[2] = pair_sum(2)
    stage_left[:half, :] = mine[2, :half, :].astype(bf16)
    sums[3].start()
    pair_step(3)
    own_step(3)
    phase("relay")
    sums[0].wait_recv()
    stage_right[:half, :] = (mine[1, :half, :] + relay_left[...].astype(f32)).astype(bf16)
    sums[4].start()
    sums[1].wait_recv()
    stage_left[half:, :] = (mine[2, half:, :] + relay_right[...].astype(f32)).astype(bf16)
    sums[5].start()
    mine[3] = pair_sum(3) + upd_all[lane].astype(f32)
    phase("sum_wait")
    for k in range(2, 6):
        sums[k].wait_recv()
    phase("result")
    result = mine[3] + (from_left[...].astype(f32) + from_right[...].astype(f32))
    out_ref[...] = result.astype(bf16)

    phase("drain")
    for by in range(1, planes):
        @pl.when(here + by < planes)
        def _():
            total_copy(by, here, lax.rem(here + by, planes)).wait_send()

    for ring in (up, down, mix, upd):
        ring.drain()
    for copy in pairs + sums:
        copy.wait_send()
    phase(None)


def per_device(
    resid, mixer_in, log_step, decay_real, frequency, input_matrix, output_matrix, skip_gain,
    value_weight, gate_weight, norm_gain, up_weight, down_weight,
):
    tokens, channels = mixer_in.shape
    groups, states = decay_real.shape
    width = groups * states
    planes, slots = lax.axis_size("sp"), lax.axis_size("tp")
    features = slots * channels
    hidden = up_weight.shape[1]
    vmem = pl.BlockSpec(memory_space=pltpu.VMEM)
    hbm = pl.BlockSpec(memory_space=pl.ANY)
    wide = pltpu.VMEM((tokens, width), f32)
    block = pltpu.VMEM((tokens, channels), bf16)
    halves = pltpu.VMEM((tokens // 2, channels), bf16)
    dma = pltpu.SemaphoreType.DMA
    return pl.pallas_call(
        layer_kernel,
        out_shape=jax.ShapeDtypeStruct((tokens, channels), bf16),
        in_specs=[hbm] * 13,
        out_specs=vmem,
        scratch_shapes=[
            block, block, pltpu.VMEM((groups, tokens), f32),
            pltpu.VMEM((groups, states), f32), pltpu.VMEM((groups, states), f32),
            pltpu.VMEM((2, channels, states), f32), pltpu.VMEM((2, channels, states), f32),
            pltpu.VMEM((1, channels), f32), pltpu.VMEM((1, features), f32),
            pltpu.VMEM((features, hidden), bf16), pltpu.VMEM((features, hidden), bf16),
            pltpu.VMEM((features, 2 * channels), bf16),
            wide, wide, wide, wide, wide,
            pltpu.VMEM((8, width), f32), pltpu.VMEM((4, CHUNKS, width), f32),
            pltpu.VMEM((32, 128), f32), pltpu.VMEM((planes, 32, 128), f32), pltpu.VMEM((16, 128), f32),
            block, pltpu.VMEM((channels, 2 * width), bf16), pltpu.VMEM((tokens, 2 * width), bf16),
            pltpu.VMEM((slots, tokens, channels), bf16), pltpu.VMEM((slots, tokens, channels), bf16),
            pltpu.VMEM((SIDE, tokens, features // SIDE), bf16), pltpu.VMEM((tokens, 2 * channels), f32),
            pltpu.VMEM((tokens, hidden), f32), pltpu.VMEM((tokens, hidden), bf16),
            pltpu.VMEM((4, tokens, channels), bf16), pltpu.VMEM((4, tokens, channels), bf16),
            pltpu.VMEM((4, tokens, channels), f32),
            block, block, block, halves, halves, block, block,
            dma((13,)), pltpu.SemaphoreType.REGULAR((3,)), dma((30,)), dma((2 * planes,)), dma((30,)), dma((2 * planes,)),
            dma((planes,)), dma((planes,)),
            dma((14,)), dma((2 * slots,)), dma((14,)), dma((2 * slots,)),
            dma((4,)), dma((4,)), dma((6,)), dma((6,)),
        ],
        name="layer",
        compiler_params=pltpu.CompilerParams(
            vmem_limit_bytes=58 * 2**20, collective_id=0, has_side_effects=True
        ),
    )(
        resid, mixer_in, log_step.T, decay_real, frequency,
        input_matrix.transpose(0, 1, 3, 2).reshape(2, channels, states), output_matrix.reshape(2, channels, states),
        skip_gain.reshape(1, -1), norm_gain.reshape(1, -1), value_weight, gate_weight, up_weight, down_weight,
    )


def solution(mesh):
    in_specs = (
        P("sp", "tp"), P("sp", "tp"), P("sp", "tp"), P("tp", None), P("tp", None),
        P(None, "tp", None, None), P(None, "tp", None, None), P("tp"),
        P(None, "tp"), P(None, "tp"), P(), P("sp", "tp"), P("sp", "tp"),
    )
    return jax.shard_map(
        per_device, mesh=mesh, in_specs=in_specs, out_specs=P("sp", "tp"), check_vma=False
    )
```

```python
import functools
import math

import jax
import jax.numpy as jnp
from jax import lax
from jax.experimental import pallas as pl
from jax.experimental.pallas import tpu as pltpu
from jax.sharding import PartitionSpec as P

rms_eps = 1e-06
f32 = jnp.float32
bf16 = jnp.bfloat16
CHUNKS = 8


def onehot(shape, test):
    row = lax.broadcasted_iota(jnp.int32, shape, 0)
    col = lax.broadcasted_iota(jnp.int32, shape, 1)
    return jnp.where(test(row, col), 1.0, 0.0).astype(bf16)


def split3(x):
    hi = x.astype(bf16)
    rest = x - hi.astype(f32)
    mid = rest.astype(bf16)
    return hi, mid, (rest - mid.astype(f32)).astype(bf16)


def dot(a, b):
    return jnp.dot(a, b, preferred_element_type=f32)


def dot_t(a, b):
    return lax.dot_general(a, b, (((1,), (1,)), ((), ())), preferred_element_type=f32)


def spread_row(x, states):
    groups = x.shape[0]
    width = groups * states
    lanes = onehot((states, width), lambda r, c: r == c % states)
    wide = sum(dot(part, lanes) for part in split3(x))
    row = lax.broadcasted_iota(jnp.int32, wide.shape, 0)
    col = lax.broadcasted_iota(jnp.int32, wide.shape, 1)
    return jnp.sum(jnp.where(row == col // states, wide, 0.0), axis=0, keepdims=True)


def prepare(u_ref, ls_ref, dr_ref, fr_ref, bm_ref, cm_ref, uperm, step_wide, proj_re, proj_im, rows, wout):
    tokens, channels = u_ref.shape
    groups, states = dr_ref.shape
    width = groups * states
    per_group = channels // groups
    span = tokens // CHUNKS
    perm = onehot((tokens, tokens), lambda r, c: c == (r % CHUNKS) * span + r // CHUNKS)
    u_sorted = dot(perm, u_ref[...]).astype(bf16)
    uperm[...] = u_sorted
    decay = spread_row(dr_ref[...], states)
    angular = spread_row(fr_ref[...], states)
    rows[0:1, :] = -decay
    rows[1:2, :] = 0.5 * angular
    modulus = decay * decay + angular * angular
    inv_re = -decay / modulus
    inv_im = -angular / modulus
    step = jnp.exp(ls_ref[...])
    step = sum(dot_t(perm, part) for part in split3(step))
    group_lanes = onehot((groups, width), lambda r, c: r == c // states)
    step_wide[...] = sum(dot(part, group_lanes) for part in split3(step))
    state_lanes = onehot((states, width), lambda r, c: r == c % states)
    row = lax.broadcasted_iota(jnp.int32, (channels, width), 0)
    col = lax.broadcasted_iota(jnp.int32, (channels, width), 1)
    same = row // per_group == col // states
    b_re = dot(bm_ref[0].astype(bf16), state_lanes)
    b_im = dot(bm_ref[1].astype(bf16), state_lanes)
    w_re = jnp.where(same, b_re * inv_re - b_im * inv_im, 0.0).astype(bf16)
    w_im = jnp.where(same, b_re * inv_im + b_im * inv_re, 0.0).astype(bf16)
    proj_re[...] = dot(u_sorted, w_re)
    proj_im[...] = dot(u_sorted, w_im)
    wout[:, :width] = jnp.where(same, dot(cm_ref[0].astype(bf16), state_lanes), 0.0).astype(bf16)
    wout[:, width:] = jnp.where(same, -dot(cm_ref[1].astype(bf16), state_lanes), 0.0).astype(bf16)


SIN = (-1.0 / 6, 1.0 / 120, -1.0 / 5040, 1.0 / 362880, -1.0 / 39916800)
COS = (-0.5, 1.0 / 24, -1.0 / 720, 1.0 / 40320, -1.0 / 3628800)


def series(q, terms):
    total = terms[-1] * q
    for term in terms[-2::-1]:
        total = (total + term) * q
    return total


def first_pass(step_wide, proj_re, proj_im, rows, dec_re, dec_im, ends, first, last):
    tokens, width = step_wide.shape
    block = 256

    def one_block(b, _):
        lanes = pl.ds(pl.multiple_of(b * block, block), block)
        minus_decay = jnp.broadcast_to(rows[0:1, lanes], (CHUNKS, block))
        half_angular = jnp.broadcast_to(rows[1:2, lanes], (CHUNKS, block))

        def one_step(i, carry):
            a_re, a_im, x_re, x_im = carry
            at = pl.ds(pl.multiple_of(i * CHUNKS, CHUNKS), CHUNKS)
            step = step_wide[at, lanes]
            half = step * half_angular
            q = half * half
            sine = half + half * series(q, SIN)
            cosine = 1.0 + series(q, COS)
            factor = jnp.exp(step * minus_decay)
            twice = factor * (sine + sine)
            d_re = factor - twice * sine
            d_im = twice * cosine
            less = d_re - 1.0
            p_re = proj_re[at, lanes]
            p_im = proj_im[at, lanes]
            u_re = less * p_re - d_im * p_im
            u_im = less * p_im + d_im * p_re
            dec_re[at, lanes] = d_re
            dec_im[at, lanes] = d_im
            proj_re[at, lanes] = u_re
            proj_im[at, lanes] = u_im
            return (
                d_re * a_re - d_im * a_im,
                d_re * a_im + d_im * a_re,
                d_re * x_re - d_im * x_im + u_re,
                d_re * x_im + d_im * x_re + u_im,
            )

        zero = jnp.zeros((CHUNKS, block), f32)
        found = lax.fori_loop(0, tokens // CHUNKS, one_step, (zero + 1.0, zero, zero, zero), unroll=2)
        for k in range(4):
            ends[k, :, lanes] = found[k]
        return 0

    lax.fori_loop(first, last, one_block, 0)


def chain(early, late):
    return (
        early[0] * late[0] - early[1] * late[1],
        early[0] * late[1] + early[1] * late[0],
        late[0] * early[2] - late[1] * early[3] + late[2],
        late[0] * early[3] + late[1] * early[2] + late[3],
    )


def chunk_prefix(ends, total):
    width = ends.shape[2]
    value = tuple(ends[k] for k in range(4))
    row = lax.broadcasted_iota(jnp.int32, value[0].shape, 0)
    unit = (1.0, 0.0, 0.0, 0.0)

    def moved(value, by):
        return tuple(
            jnp.where(row >= by, pltpu.roll(part, by, 0), zero) for part, zero in zip(value, unit)
        )

    for by in (1, 2, 4):
        value = chain(moved(value, by), value)
    for k in range(4):
        for j in range(width // 128):
            total[8 * k + j : 8 * k + j + 1, :] = value[k][CHUNKS - 1 :, 128 * j : 128 * j + 128]
    before = moved(value, 1)
    for k in range(4):
        ends[k] = before[k]


def second_pass(dec_re, dec_im, feed_re, feed_im, ends, carry, states):
    tokens, width = dec_re.shape
    block = 512
    for b in range(width // block):
        lanes = pl.ds(b * block, block)
        lanes_im = pl.ds(width + b * block, block)
        per = block // 128
        h_re = jnp.concatenate([carry[per * b + j : per * b + j + 1, :] for j in range(per)], axis=1)
        h_im = jnp.concatenate([carry[8 + per * b + j : 9 + per * b + j, :] for j in range(per)], axis=1)
        a_re, a_im = ends[0, :, lanes], ends[1, :, lanes]
        x_re = ends[2, :, lanes] + a_re * h_re - a_im * h_im
        x_im = ends[3, :, lanes] + a_re * h_im + a_im * h_re

        def one_step(i, value):
            x_re, x_im = value
            seen = []
            for k in range(2):
                at = pl.ds(pl.multiple_of(i * 2 * CHUNKS + k * CHUNKS, CHUNKS), CHUNKS)
                d_re, d_im = dec_re[at, lanes], dec_im[at, lanes]
                x_re, x_im = (
                    d_re * x_re - d_im * x_im + feed_re[at, lanes],
                    d_re * x_im + d_im * x_re + feed_im[at, lanes],
                )
                seen.append((x_re, x_im))
            both = pl.ds(pl.multiple_of(i * 2 * CHUNKS, 2 * CHUNKS), 2 * CHUNKS)
            states[both, lanes] = jnp.concatenate([seen[0][0], seen[1][0]], axis=0).astype(bf16)
            states[both, lanes_im] = jnp.concatenate([seen[0][1], seen[1][1]], axis=0).astype(bf16)
            return x_re, x_im

        lax.fori_loop(0, tokens // (2 * CHUNKS), one_step, (x_re, x_im), unroll=2)


def read_out(states, wout, uperm, skip_ref):
    tokens = states.shape[0]
    span = tokens // CHUNKS
    out = dot_t(states[...], wout[...]) + skip_ref[...] * uperm[...].astype(f32)
    mixed = jax.nn.gelu(out).astype(bf16)
    back = onehot((tokens, tokens), lambda r, c: r == (c % CHUNKS) * span + c // CHUNKS)
    return dot(back, mixed).astype(bf16)


AXES = pl.DeviceIdType.MESH
SIDE = 4


def around(index, by):
    return lax.rem(index + by + SIDE, SIDE)


class Relay:
    def __init__(self, buf, own, send_sem, recv_sem, y_first):
        here = lax.axis_index("sp")
        z, y = here // SIDE, lax.rem(here, SIDE)
        self.p, self.q = (y, z) if y_first else (z, y)
        self.y_first, self.buf, self.own = y_first, buf, own
        self.send_sem, self.recv_sem = send_sem, recv_sem
        self.rows = buf.shape[0] // (SIDE * SIDE)
        self.sent = 0

    def index(self, dp, dq):
        p, q = around(self.p, dp), around(self.q, dq)
        return q * SIDE + p if self.y_first else p * SIDE + q

    def group(self, dp, dq, half):
        if dq == 0:
            return 2 if dp == 2 else int((dp == -1) == (half == 1))
        if dq == 2:
            return 9
        return 3 + dp % SIDE if (dq == -1) == (half == 0) else (7 if dq == -1 else 8)

    def send(self, dp, dq, half, to_p, to_q, hbm=False):
        rows = self.rows // 2
        slot = self.index(dp, dq)
        piece = self.buf.at[pl.ds(pl.multiple_of(slot * self.rows + half * rows, rows), rows), :]
        seen = [(d + 1) % SIDE - 1 for d in (dp - to_p, dq - to_q)]
        pltpu.make_async_remote_copy(
            src_ref=self.own.at[half * rows : half * rows + rows, :] if hbm else piece,
            dst_ref=piece,
            send_sem=self.send_sem,
            recv_sem=self.recv_sem.at[self.group(*seen, half)],
            device_id={"sp": self.index(to_p, to_q), "tp": lax.axis_index("tp")},
            device_id_type=AXES,
        ).start()
        self.sent += 1

    def whole(self, count, group):
        rows = self.buf.at[: count * self.rows // 2, :]
        return pltpu.make_async_remote_copy(
            src_ref=rows,
            dst_ref=rows,
            send_sem=self.send_sem,
            recv_sem=self.recv_sem.at[group],
            device_id={"sp": self.index(1, 0), "tp": lax.axis_index("tp")},
            device_id_type=AXES,
        )

    def arrived(self, group):
        self.whole({7: 4, 8: 4, 9: 8}.get(group, 2), group).wait_recv()

    def send_p(self):
        for k in range(2):
            self.send(0, 0, k, 1, 0, True)
            self.send(0, 0, 1 - k, -1, 0, True)

    def send_q(self, dp, part=(0, 1), hbm=False):
        for k in part:
            self.send(dp, 0, k, 0, 1, hbm)
            self.send(dp, 0, 1 - k, 0, -1, hbm)

    def forward_p(self):
        self.arrived(0)
        self.send(-1, 0, 0, 1, 0)
        self.send(1, 0, 1, -1, 0)

    def near(self):
        self.arrived(1)
        self.send_q(-1)
        self.send_q(1)

    def far(self):
        self.arrived(2)
        self.send_q(2)

    def forward_q(self, dp):
        self.arrived(3 + dp % SIDE)
        self.send(dp, -1, 0, 0, 1)
        self.send(dp, 1, 1, 0, -1)

    def finish(self, dq):
        self.arrived({-1: 7, 1: 8, 2: 9}[dq])

    def drain(self):
        self.whole(self.sent, 0).wait_send()


class Gather:
    def __init__(self, buf, send_sem, recv_sem):
        here = lax.axis_index("tp")
        self.x, self.core = here // 2, lax.rem(here, 2)
        self.buf, self.send_sem, self.recv_sem = buf, send_sem, recv_sem
        self.sent = 0

    def slot(self, dx, other=False):
        core = 1 - self.core if other else self.core
        return around(self.x, dx) * 2 + core

    def send(self, dx, half, to_x):
        rows = self.buf.shape[1] // 2
        piece = self.buf.at[self.slot(dx), half * rows : half * rows + rows, :]
        if to_x:
            seen = (dx - to_x + 1) % SIDE - 1
            group = 2 if seen == 2 else int((seen == -1) == (half == 1))
            target = self.slot(to_x)
        else:
            group, target = 3 + dx % SIDE, self.slot(0, True)
        pltpu.make_async_remote_copy(
            src_ref=piece,
            dst_ref=piece,
            send_sem=self.send_sem,
            recv_sem=self.recv_sem.at[group],
            device_id={"sp": lax.axis_index("sp"), "tp": target},
            device_id_type=AXES,
        ).start()
        self.sent += 1

    def whole(self, pieces, group):
        rows = self.buf.at[pieces]
        return pltpu.make_async_remote_copy(
            src_ref=rows,
            dst_ref=rows,
            send_sem=self.send_sem,
            recv_sem=self.recv_sem.at[group],
            device_id={"sp": lax.axis_index("sp"), "tp": self.slot(1)},
            device_id_type=AXES,
        )

    def arrived(self, group):
        self.whole(0, group).wait_recv()

    def start(self):
        for k in range(2):
            self.send(0, k, 1)
            self.send(0, 1 - k, -1)
        for k in range(2):
            self.send(0, k, 0)

    def near(self):
        self.arrived(0)
        self.send(-1, 0, 1)
        self.send(1, 1, -1)
        self.send(-1, 0, 0)
        self.send(1, 1, 0)
        self.arrived(1)
        self.send(-1, 1, 0)
        self.send(1, 0, 0)

    def far(self):
        self.arrived(2)
        self.send(2, 0, 0)
        self.send(2, 1, 0)

    def finish(self):
        for dx in range(SIDE):
            self.arrived(3 + dx)

    def drain(self):
        self.whole(slice(0, self.sent // 2), 0).wait_send()


class Phases:
    def __init__(self):
        self.scope = None

    def __call__(self, name):
        if self.scope is not None:
            self.scope.__exit__(None, None, None)
        self.scope = jax.named_scope(name) if name else None
        if self.scope is not None:
            self.scope.__enter__()


def layer_kernel(
    resid_hbm, u_hbm, ls_hbm, dr_hbm, fr_hbm, bm_hbm, cm_hbm, skip_hbm, gain_hbm, vw_ref, gw_ref, up_ref, down_ref,
    out_ref,
    resid_ref, u_ref, ls_ref, dr_ref, fr_ref, bm_ref, cm_ref, skip_ref, gain_ref,
    up_all, down_all, vg, dec_re, dec_im, feed_re, feed_im, step_wide, rows, ends, total, totals, carry,
    uperm, wout, states, mixed_all, upd_all, normed, glu, raised, hidden, stage_pair, from_pair, mine,
    stage_far, stage_right, stage_left, relay_left, relay_right, from_left, from_right,
    local_sem, round_sem, ring_send, ring_recv, tot_send, tot_recv, sum_send, sum_recv,
):
    phase = Phases()
    here, lane = lax.axis_index("sp"), lax.axis_index("tp")
    planes = SIDE * SIDE
    tokens, piece = resid_ref.shape
    half = tokens // 2
    up = Relay(up_all, up_ref, ring_send.at[0], ring_recv.at[0], True)
    down = Relay(down_all, down_ref, ring_send.at[1], ring_recv.at[1], False)
    mix = Gather(mixed_all, ring_send.at[2], ring_recv.at[2])
    upd = Gather(upd_all, ring_send.at[3], ring_recv.at[3])
    right, left, partner = mix.slot(1), mix.slot(-1), mix.slot(0, True)
    near_planes = [up.index(*by) for by in ((1, 0), (-1, 0), (0, 1), (0, -1))]

    phase("signal")
    barrier = pltpu.get_barrier_semaphore()
    for target in near_planes:
        pl.semaphore_signal(barrier, inc=1, device_id={"sp": target, "tp": lane}, device_id_type=AXES)
    for target in (right, left, partner):
        pl.semaphore_signal(barrier, inc=1, device_id={"sp": here, "tp": target}, device_id_type=AXES)

    own_rows = pl.ds(pl.multiple_of(here * up.rows, up.rows), up.rows)
    moves = (
        (up_ref, up_all.at[own_rows, :]), (down_ref, down_all.at[own_rows, :]),
        (u_hbm, u_ref), (dr_hbm, dr_ref), (fr_hbm, fr_ref), (ls_hbm, ls_ref), (bm_hbm, bm_ref), (cm_hbm, cm_ref),
        (skip_hbm, skip_ref), (vw_ref, vg.at[:, :piece]), (gw_ref, vg.at[:, piece:]),
        (resid_hbm, resid_ref), (gain_hbm, gain_ref),
    )
    local = [pltpu.make_async_copy(src, dst, local_sem.at[k]) for k, (src, dst) in enumerate(moves)]
    for copy in local:
        copy.start()
    phase("barrier")
    pl.semaphore_wait(barrier, 7)
    phase("start_p")
    up.send_p()
    down.send_p()
    up.send_q(0, (0,), True)
    down.send_q(0, (0,), True)

    def greet(number):
        for target in near_planes:
            pl.semaphore_signal(
                round_sem.at[number], inc=1, device_id={"sp": target, "tp": lane}, device_id_type=AXES
            )

    greet(0)
    for copy in local[2:8]:
        copy.wait()
    phase("prepare")
    prepare(u_ref, ls_ref, dr_ref, fr_ref, bm_ref, cm_ref, uperm, step_wide, feed_re, feed_im, rows, wout)
    pl.semaphore_wait(round_sem.at[0], 4)
    greet(1)
    phase("first_pass")
    scan_refs = (step_wide, feed_re, feed_im, rows, dec_re, dec_im, ends)
    first_pass(*scan_refs, 0, 2)
    pl.semaphore_wait(round_sem.at[1], 4)
    greet(2)
    first_pass(*scan_refs, 2, 4)
    phase("chunk")
    chunk_prefix(ends, total)
    pl.semaphore_wait(round_sem.at[2], 4)

    def total_copy(by, slot, target):
        return pltpu.make_async_remote_copy(
            src_ref=total,
            dst_ref=totals.at[slot],
            send_sem=tot_send.at[by],
            recv_sem=tot_recv.at[slot],
            device_id={"sp": target, "tp": lane},
            device_id_type=AXES,
        )

    phase("totals")
    for by in range(1, planes):
        @pl.when(here + by < planes)
        def _():
            total_copy(by, here, lax.rem(here + by, planes)).start()

    phase("forward_p")
    up.forward_p()
    down.forward_p()
    phase("send_q")
    local[0].wait()
    local[1].wait()
    up.send_q(0, (1,))
    down.send_q(0, (1,))
    phase("serve_near")
    up.near()
    down.near()

    phase("fold")

    def fold(j, value):
        h_re, h_im = value
        total_copy(0, j, lax.rem(here + 1, planes)).wait_recv()
        a_re, a_im = totals[j, 0:8, :], totals[j, 8:16, :]
        x_re, x_im = totals[j, 16:24, :], totals[j, 24:32, :]
        return a_re * h_re - a_im * h_im + x_re, a_re * h_im + a_im * h_re + x_im

    zero = jnp.zeros((8, 128), f32)
    h_re, h_im = lax.fori_loop(0, here, fold, (zero, zero))
    carry[0:8, :] = h_re
    carry[8:16, :] = h_im
    phase("second_pass")
    second_pass(dec_re, dec_im, feed_re, feed_im, ends, carry, states)
    local[8].wait()
    phase("read_out")
    mixed_all[lane] = read_out(states, wout, uperm, skip_ref)
    phase("mix_start")
    mix.start()
    phase("serve_far")
    up.far()
    down.far()
    up.forward_q(0)
    down.forward_q(0)
    phase("mix_near")
    mix.near()
    phase("mix_far")
    mix.far()
    phase("fq_minus")
    up.forward_q(-1)
    down.forward_q(-1)
    phase("mix_finish")
    mix.finish()

    phase("glu")
    for copy in local[9:]:
        copy.wait()
    glu[...] = jnp.zeros_like(glu)

    def glu_step(s, _):
        at = pl.ds(pl.multiple_of(s * piece, piece), piece)
        glu[...] += dot(mixed_all[s], vg[at, :])
        return 0

    slots = mixed_all.shape[0]
    lax.fori_loop(0, slots, glu_step, 0)
    updated = (resid_ref[...].astype(f32) + glu[:, :piece] * jax.nn.sigmoid(glu[:, piece:])).astype(bf16)
    upd_all[lane] = updated
    phase("upd_start")
    upd.start()
    phase("fq_plus")
    up.forward_q(1)
    down.forward_q(1)
    phase("upd_near")
    upd.near()
    phase("fq_far")
    up.forward_q(2)
    down.forward_q(2)
    phase("upd_far")
    upd.far()
    phase("upd_finish")
    upd.finish()

    phase("norm")

    def square_step(s, total):
        wide = upd_all[s].astype(f32)
        return total + jnp.sum(wide * wide, axis=1, keepdims=True)

    squares = lax.fori_loop(0, slots, square_step, jnp.zeros((tokens, 1), f32))
    inv_rms = lax.rsqrt(squares / (slots * piece) + rms_eps)
    for s in range(slots):
        at = slice(s * piece, s * piece + piece)
        normed[s // 2, :, s % 2 * piece : s % 2 * piece + piece] = (
            upd_all[s].astype(f32) * inv_rms * gain_ref[:, at]
        ).astype(bf16)

    depth = normed.shape[2]
    for k, dq in enumerate((0, -1, 1, 2)):
        if k:
            phase(f"up_wait{k}")
            up.finish(dq)
        phase(f"up_mm{k}")
        group = around(up.q, dq)
        product = dot(normed[group], up_all[pl.ds(pl.multiple_of(group * depth, depth), depth), :])
        if k == 0:
            raised[...] = product
        elif k < 3:
            raised[...] += product
        else:
            active = jnp.maximum(raised[...] + product, 0.0)
            hidden[...] = (active * active).astype(bf16)
    phase("down_finish")
    for dq in (-1, 1, 2):
        down.finish(dq)

    def sum_copy(number, src, dst, target):
        return pltpu.make_async_remote_copy(
            src_ref=src,
            dst_ref=dst,
            send_sem=sum_send.at[number],
            recv_sem=sum_recv.at[number],
            device_id={"sp": here, "tp": target},
            device_id_type=AXES,
        )

    order = (2, 1, -1, 0)
    sums = [
        sum_copy(0, stage_far.at[:half, :], relay_left, right),
        sum_copy(1, stage_far.at[half:, :], relay_right, left),
        sum_copy(2, stage_right.at[half:, :], from_left.at[half:, :], right),
        sum_copy(3, stage_left.at[:half, :], from_right.at[:half, :], left),
        sum_copy(4, stage_right.at[:half, :], from_left.at[:half, :], right),
        sum_copy(5, stage_left.at[half:, :], from_right.at[half:, :], left),
    ]
    pairs = [sum_copy(6 + k, stage_pair.at[k], from_pair.at[k], partner) for k in range(len(order))]
    own_cols = pl.ds(pl.multiple_of(mix.core * piece, piece), piece)
    other_cols = pl.ds(pl.multiple_of((1 - mix.core) * piece, piece), piece)

    def step(k):
        at = pl.ds(pl.multiple_of(around(mix.x, order[k]) * 2 * piece, 2 * piece), 2 * piece)
        mine[k] = dot_t(hidden[...], down_all[at, :])
        stage_pair[k] = mine[k, :, other_cols].astype(bf16)
        pairs[k].start()

    def pair_sum(k):
        pairs[k].wait_recv()
        return mine[k, :, own_cols] + from_pair[k].astype(f32)

    phase("products")
    step(0)
    step(1)
    phase("far")
    stage_far[...] = pair_sum(0).astype(bf16)
    sums[0].start()
    sums[1].start()
    phase("near")
    step(2)
    near = pair_sum(1)
    stage_right[half:, :] = near[half:].astype(bf16)
    sums[2].start()
    mine[1, :half, own_cols] = near[:half]
    step(3)
    near = pair_sum(2)
    stage_left[:half, :] = near[:half].astype(bf16)
    sums[3].start()
    mine[2, half:, own_cols] = near[half:]
    mine[3, :, own_cols] = pair_sum(3) + upd_all[lane].astype(f32)
    phase("relay")
    sums[0].wait_recv()
    stage_right[:half, :] = (mine[1, :half, own_cols] + relay_left[...].astype(f32)).astype(bf16)
    sums[4].start()
    sums[1].wait_recv()
    stage_left[half:, :] = (mine[2, half:, own_cols] + relay_right[...].astype(f32)).astype(bf16)
    sums[5].start()
    phase("sum_wait")
    for k in range(2, 6):
        sums[k].wait_recv()
    phase("result")
    result = mine[3, :, own_cols] + (from_left[...].astype(f32) + from_right[...].astype(f32))
    out_ref[...] = result.astype(bf16)

    phase("drain")
    for by in range(1, planes):
        @pl.when(here + by < planes)
        def _():
            total_copy(by, here, lax.rem(here + by, planes)).wait_send()

    for ring in (up, down, mix, upd):
        ring.drain()
    for copy in pairs + sums:
        copy.wait_send()
    phase(None)


def per_device(
    resid, mixer_in, log_step, decay_real, frequency, input_matrix, output_matrix, skip_gain,
    value_weight, gate_weight, norm_gain, up_weight, down_weight,
):
    tokens, channels = mixer_in.shape
    groups, states = decay_real.shape
    width = groups * states
    planes, slots = lax.axis_size("sp"), lax.axis_size("tp")
    features = slots * channels
    hidden = up_weight.shape[1]
    vmem = pl.BlockSpec(memory_space=pltpu.VMEM)
    hbm = pl.BlockSpec(memory_space=pl.ANY)
    wide = pltpu.VMEM((tokens, width), f32)
    block = pltpu.VMEM((tokens, channels), bf16)
    halves = pltpu.VMEM((tokens // 2, channels), bf16)
    dma = pltpu.SemaphoreType.DMA
    return pl.pallas_call(
        layer_kernel,
        out_shape=jax.ShapeDtypeStruct((tokens, channels), bf16),
        in_specs=[hbm] * 13,
        out_specs=vmem,
        scratch_shapes=[
            block, block, pltpu.VMEM((groups, tokens), f32),
            pltpu.VMEM((groups, states), f32), pltpu.VMEM((groups, states), f32),
            pltpu.VMEM((2, channels, states), f32), pltpu.VMEM((2, channels, states), f32),
            pltpu.VMEM((1, channels), f32), pltpu.VMEM((1, features), f32),
            pltpu.VMEM((features, hidden), bf16), pltpu.VMEM((features, hidden), bf16),
            pltpu.VMEM((features, 2 * channels), bf16),
            wide, wide, wide, wide, wide,
            pltpu.VMEM((8, width), f32), pltpu.VMEM((4, CHUNKS, width), f32),
            pltpu.VMEM((32, 128), f32), pltpu.VMEM((planes, 32, 128), f32), pltpu.VMEM((16, 128), f32),
            block, pltpu.VMEM((channels, 2 * width), bf16), pltpu.VMEM((tokens, 2 * width), bf16),
            pltpu.VMEM((slots, tokens, channels), bf16), pltpu.VMEM((slots, tokens, channels), bf16),
            pltpu.VMEM((SIDE, tokens, features // SIDE), bf16), pltpu.VMEM((tokens, 2 * channels), f32),
            pltpu.VMEM((tokens, hidden), f32), pltpu.VMEM((tokens, hidden), bf16),
            pltpu.VMEM((4, tokens, channels), bf16), pltpu.VMEM((4, tokens, channels), bf16),
            pltpu.VMEM((4, tokens, 2 * channels), f32),
            block, block, block, halves, halves, block, block,
            dma((13,)), pltpu.SemaphoreType.REGULAR((3,)), dma((4,)), dma((4, 10)),
            dma((planes,)), dma((planes,)), dma((10,)), dma((10,)),
        ],
        name="layer",
        compiler_params=pltpu.CompilerParams(
            vmem_limit_bytes=58 * 2**20, collective_id=0, has_side_effects=True
        ),
    )(
        resid, mixer_in, log_step.T, decay_real, frequency,
        input_matrix.transpose(0, 1, 3, 2).reshape(2, channels, states), output_matrix.reshape(2, channels, states),
        skip_gain.reshape(1, -1), norm_gain.reshape(1, -1), value_weight, gate_weight, up_weight, down_weight,
    )


def solution(mesh):
    in_specs = (
        P("sp", "tp"), P("sp", "tp"), P("sp", "tp"), P("tp", None), P("tp", None),
        P(None, "tp", None, None), P(None, "tp", None, None), P("tp"),
        P(None, "tp"), P(None, "tp"), P(), P("sp", "tp"), P("sp", "tp"),
    )
    return jax.shard_map(
        per_device, mesh=mesh, in_specs=in_specs, out_specs=P("sp", "tp"), check_vma=False
    )
```

```python
import functools
import math

import jax
import jax.numpy as jnp
from jax import lax
from jax.experimental import pallas as pl
from jax.experimental.pallas import tpu as pltpu
from jax.sharding import PartitionSpec as P

rms_eps = 1e-06
f32 = jnp.float32
bf16 = jnp.bfloat16
CHUNKS = 8


def onehot(shape, test):
    row = lax.broadcasted_iota(jnp.int32, shape, 0)
    col = lax.broadcasted_iota(jnp.int32, shape, 1)
    return jnp.where(test(row, col), 1.0, 0.0).astype(bf16)


def split3(x):
    hi = x.astype(bf16)
    rest = x - hi.astype(f32)
    mid = rest.astype(bf16)
    return hi, mid, (rest - mid.astype(f32)).astype(bf16)


def dot(a, b):
    return jnp.dot(a, b, preferred_element_type=f32)


def dot_t(a, b):
    return lax.dot_general(a, b, (((1,), (1,)), ((), ())), preferred_element_type=f32)


def spread_row(x, states):
    groups = x.shape[0]
    width = groups * states
    lanes = onehot((states, width), lambda r, c: r == c % states)
    wide = sum(dot(part, lanes) for part in split3(x))
    row = lax.broadcasted_iota(jnp.int32, wide.shape, 0)
    col = lax.broadcasted_iota(jnp.int32, wide.shape, 1)
    return jnp.sum(jnp.where(row == col // states, wide, 0.0), axis=0, keepdims=True)


def prepare(u_ref, ls_ref, dr_ref, fr_ref, bm_ref, cm_ref, uperm, step_wide, proj_re, proj_im, rows, wout):
    tokens, channels = u_ref.shape
    groups, states = dr_ref.shape
    width = groups * states
    per_group = channels // groups
    span = tokens // CHUNKS
    perm = onehot((tokens, tokens), lambda r, c: c == (r % CHUNKS) * span + r // CHUNKS)
    u_sorted = dot(perm, u_ref[...]).astype(bf16)
    uperm[...] = u_sorted
    decay = spread_row(dr_ref[...], states)
    angular = spread_row(fr_ref[...], states)
    rows[0:1, :] = -decay
    rows[1:2, :] = 0.5 * angular
    modulus = decay * decay + angular * angular
    inv_re = -decay / modulus
    inv_im = -angular / modulus
    step = jnp.exp(ls_ref[...])
    step = sum(dot_t(perm, part) for part in split3(step))
    group_lanes = onehot((groups, width), lambda r, c: r == c // states)
    step_wide[...] = sum(dot(part, group_lanes) for part in split3(step))
    state_lanes = onehot((states, width), lambda r, c: r == c % states)
    row = lax.broadcasted_iota(jnp.int32, (channels, width), 0)
    col = lax.broadcasted_iota(jnp.int32, (channels, width), 1)
    same = row // per_group == col // states
    b_re = dot(bm_ref[0].astype(bf16), state_lanes)
    b_im = dot(bm_ref[1].astype(bf16), state_lanes)
    w_re = jnp.where(same, b_re * inv_re - b_im * inv_im, 0.0).astype(bf16)
    w_im = jnp.where(same, b_re * inv_im + b_im * inv_re, 0.0).astype(bf16)
    proj_re[...] = dot(u_sorted, w_re)
    proj_im[...] = dot(u_sorted, w_im)
    wout[:, :width] = jnp.where(same, dot(cm_ref[0].astype(bf16), state_lanes), 0.0).astype(bf16)
    wout[:, width:] = jnp.where(same, -dot(cm_ref[1].astype(bf16), state_lanes), 0.0).astype(bf16)


SIN = (-1.0 / 6, 1.0 / 120, -1.0 / 5040, 1.0 / 362880, -1.0 / 39916800)
COS = (-0.5, 1.0 / 24, -1.0 / 720, 1.0 / 40320, -1.0 / 3628800)


def series(q, terms):
    total = terms[-1] * q
    for term in terms[-2::-1]:
        total = (total + term) * q
    return total


def first_pass(step_wide, proj_re, proj_im, rows, dec_re, dec_im, ends, first, last):
    tokens, width = step_wide.shape
    block = 256

    def one_block(b, _):
        lanes = pl.ds(pl.multiple_of(b * block, block), block)
        minus_decay = jnp.broadcast_to(rows[0:1, lanes], (CHUNKS, block))
        half_angular = jnp.broadcast_to(rows[1:2, lanes], (CHUNKS, block))

        def one_step(i, carry):
            a_re, a_im, x_re, x_im = carry
            at = pl.ds(pl.multiple_of(i * CHUNKS, CHUNKS), CHUNKS)
            step = step_wide[at, lanes]
            half = step * half_angular
            q = half * half
            sine = half + half * series(q, SIN)
            cosine = 1.0 + series(q, COS)
            factor = jnp.exp(step * minus_decay)
            twice = factor * (sine + sine)
            d_re = factor - twice * sine
            d_im = twice * cosine
            less = d_re - 1.0
            p_re = proj_re[at, lanes]
            p_im = proj_im[at, lanes]
            u_re = less * p_re - d_im * p_im
            u_im = less * p_im + d_im * p_re
            dec_re[at, lanes] = d_re
            dec_im[at, lanes] = d_im
            proj_re[at, lanes] = u_re
            proj_im[at, lanes] = u_im
            return (
                d_re * a_re - d_im * a_im,
                d_re * a_im + d_im * a_re,
                d_re * x_re - d_im * x_im + u_re,
                d_re * x_im + d_im * x_re + u_im,
            )

        zero = jnp.zeros((CHUNKS, block), f32)
        found = lax.fori_loop(0, tokens // CHUNKS, one_step, (zero + 1.0, zero, zero, zero), unroll=2)
        for k in range(4):
            ends[k, :, lanes] = found[k]
        return 0

    lax.fori_loop(first, last, one_block, 0)


def chain(early, late):
    return (
        early[0] * late[0] - early[1] * late[1],
        early[0] * late[1] + early[1] * late[0],
        late[0] * early[2] - late[1] * early[3] + late[2],
        late[0] * early[3] + late[1] * early[2] + late[3],
    )


def chunk_prefix(ends, total):
    width = ends.shape[2]
    value = tuple(ends[k] for k in range(4))
    row = lax.broadcasted_iota(jnp.int32, value[0].shape, 0)
    unit = (1.0, 0.0, 0.0, 0.0)

    def moved(value, by):
        return tuple(
            jnp.where(row >= by, pltpu.roll(part, by, 0), zero) for part, zero in zip(value, unit)
        )

    for by in (1, 2, 4):
        value = chain(moved(value, by), value)
    for k in range(4):
        for j in range(width // 128):
            total[8 * k + j : 8 * k + j + 1, :] = value[k][CHUNKS - 1 :, 128 * j : 128 * j + 128]
    before = moved(value, 1)
    for k in range(4):
        ends[k] = before[k]


def second_pass(dec_re, dec_im, feed_re, feed_im, ends, carry, states):
    tokens, width = dec_re.shape
    block = 512
    for b in range(width // block):
        lanes = pl.ds(b * block, block)
        lanes_im = pl.ds(width + b * block, block)
        per = block // 128
        h_re = jnp.concatenate([carry[per * b + j : per * b + j + 1, :] for j in range(per)], axis=1)
        h_im = jnp.concatenate([carry[8 + per * b + j : 9 + per * b + j, :] for j in range(per)], axis=1)
        a_re, a_im = ends[0, :, lanes], ends[1, :, lanes]
        x_re = ends[2, :, lanes] + a_re * h_re - a_im * h_im
        x_im = ends[3, :, lanes] + a_re * h_im + a_im * h_re

        def one_step(i, value):
            x_re, x_im = value
            seen = []
            for k in range(2):
                at = pl.ds(pl.multiple_of(i * 2 * CHUNKS + k * CHUNKS, CHUNKS), CHUNKS)
                d_re, d_im = dec_re[at, lanes], dec_im[at, lanes]
                x_re, x_im = (
                    d_re * x_re - d_im * x_im + feed_re[at, lanes],
                    d_re * x_im + d_im * x_re + feed_im[at, lanes],
                )
                seen.append((x_re, x_im))
            both = pl.ds(pl.multiple_of(i * 2 * CHUNKS, 2 * CHUNKS), 2 * CHUNKS)
            states[both, lanes] = jnp.concatenate([seen[0][0], seen[1][0]], axis=0).astype(bf16)
            states[both, lanes_im] = jnp.concatenate([seen[0][1], seen[1][1]], axis=0).astype(bf16)
            return x_re, x_im

        lax.fori_loop(0, tokens // (2 * CHUNKS), one_step, (x_re, x_im), unroll=2)


def read_out(states, wout, uperm, skip_ref):
    tokens = states.shape[0]
    span = tokens // CHUNKS
    out = dot_t(states[...], wout[...]) + skip_ref[...] * uperm[...].astype(f32)
    mixed = jax.nn.gelu(out).astype(bf16)
    back = onehot((tokens, tokens), lambda r, c: r == (c % CHUNKS) * span + c // CHUNKS)
    return dot(back, mixed).astype(bf16)


AXES = pl.DeviceIdType.MESH
SIDE = 4


def around(index, by):
    return lax.rem(index + by + SIDE, SIDE)


class Relay:
    def __init__(self, buf, first, rows, send_sem, recv_sem, own=None):
        here = lax.axis_index("sp")
        self.zy = here // SIDE, lax.rem(here, SIDE)
        self.buf, self.first, self.rows, self.own = buf, first, rows, own
        self.shard = buf.shape[0] // (SIDE * SIDE)
        self.send_sem, self.recv_sem = send_sem, recv_sem
        self.sent = 0

    def index(self, side, dp, dq):
        dz, dy = (dq, dp) if side == 0 else (dp, dq)
        return around(self.zy[0], dz) * SIDE + around(self.zy[1], dy)

    def group(self, dp, dq, half):
        if dq == 0:
            return 2 if dp == 2 else int((dp == -1) == (half == 1))
        return 3 + dp % SIDE if dq != 2 and (dq == -1) == (half == 0) else 7

    def send(self, side, dp, dq, half, to_p, to_q):
        width = self.buf.shape[1] // 2
        cols = slice(half * width, half * width + width)
        row = pl.multiple_of(self.index(side, dp, dq) * self.shard + side * self.rows, self.rows)
        piece = self.buf.at[pl.ds(row, self.rows), cols]
        own = self.own is not None and dp == 0 and dq == 0
        first = self.first + side * self.rows
        seen = [(d + 1) % SIDE - 1 for d in (dp - to_p, dq - to_q)]
        pltpu.make_async_remote_copy(
            src_ref=self.own.at[first : first + self.rows, cols] if own else piece,
            dst_ref=piece,
            send_sem=self.send_sem,
            recv_sem=self.recv_sem.at[self.group(*seen, half)],
            device_id={"sp": self.index(side, to_p, to_q), "tp": lax.axis_index("tp")},
            device_id_type=AXES,
        ).start()
        self.sent += 1

    def whole(self, count, group):
        rows = self.buf.at[: count * self.rows // 2, :]
        return pltpu.make_async_remote_copy(
            src_ref=rows,
            dst_ref=rows,
            send_sem=self.send_sem,
            recv_sem=self.recv_sem.at[group],
            device_id={"sp": self.index(0, 1, 0), "tp": lax.axis_index("tp")},
            device_id_type=AXES,
        )

    def arrived(self, group):
        self.whole(32 if group == 7 else 4, group).wait_recv()

    def send_p(self):
        for k in range(2):
            for side in range(2):
                self.send(side, 0, 0, k, 1, 0)
                self.send(side, 0, 0, 1 - k, -1, 0)

    def send_q(self, dp):
        for k in range(2):
            for side in range(2):
                self.send(side, dp, 0, k, 0, 1)
                self.send(side, dp, 0, 1 - k, 0, -1)

    def forward_p(self):
        self.arrived(0)
        for side in range(2):
            self.send(side, -1, 0, 0, 1, 0)
            self.send(side, 1, 0, 1, -1, 0)

    def near(self):
        self.arrived(1)
        self.send_q(-1)
        self.send_q(1)

    def far(self):
        self.arrived(2)
        self.send_q(2)

    def forward_q(self, dp):
        self.arrived(3 + dp % SIDE)
        for side in range(2):
            self.send(side, dp, -1, 0, 0, 1)
            self.send(side, dp, 1, 1, 0, -1)

    def finish(self):
        self.arrived(7)

    def drain(self):
        self.whole(self.sent, 0).wait_send()


class Gather:
    def __init__(self, buf, send_sem, recv_sem):
        here = lax.axis_index("tp")
        self.x, self.core = here // 2, lax.rem(here, 2)
        self.buf, self.send_sem, self.recv_sem = buf, send_sem, recv_sem
        self.sent = 0

    def device(self, dx, other=False):
        return around(self.x, dx) * 2 + (1 - self.core if other else self.core)

    def cols(self, core):
        width = self.buf.shape[2] // 2
        return pl.ds(pl.multiple_of(core * width, width), width)

    def send(self, dx, half, to_x):
        rows = self.buf.shape[1] // 2
        piece = self.buf.at[around(self.x, dx), half * rows : half * rows + rows, self.cols(self.core)]
        if to_x:
            seen = (dx - to_x + 1) % SIDE - 1
            group = 2 if seen == 2 else int((seen == -1) == (half == 1))
        else:
            group = 3 + dx % SIDE
        pltpu.make_async_remote_copy(
            src_ref=piece,
            dst_ref=piece,
            send_sem=self.send_sem,
            recv_sem=self.recv_sem.at[group],
            device_id={"sp": lax.axis_index("sp"), "tp": self.device(to_x, not to_x)},
            device_id_type=AXES,
        ).start()
        self.sent += 1

    def whole(self, rows, group):
        return pltpu.make_async_remote_copy(
            src_ref=rows,
            dst_ref=rows,
            send_sem=self.send_sem,
            recv_sem=self.recv_sem.at[group],
            device_id={"sp": lax.axis_index("sp"), "tp": self.device(1)},
            device_id_type=AXES,
        )

    def arrived(self, group):
        self.whole(self.buf.at[0, :, : self.buf.shape[2] // 2], group).wait_recv()

    def start(self):
        for k in range(2):
            self.send(0, k, 1)
            self.send(0, 1 - k, -1)
        for k in range(2):
            self.send(0, k, 0)

    def near(self):
        self.arrived(0)
        self.send(-1, 0, 1)
        self.send(1, 1, -1)
        self.send(-1, 0, 0)
        self.send(1, 1, 0)
        self.arrived(1)
        self.send(-1, 1, 0)
        self.send(1, 0, 0)

    def far(self):
        self.arrived(2)
        self.send(2, 0, 0)
        self.send(2, 1, 0)

    def across(self, dx):
        self.arrived(3 + dx % SIDE)

    def drain(self):
        self.whole(self.buf.at[:, : self.buf.shape[1] * self.sent // 16, :], 0).wait_send()


class Phases:
    def __init__(self):
        self.scope = None

    def __call__(self, name):
        if self.scope is not None:
            self.scope.__exit__(None, None, None)
        self.scope = jax.named_scope(name) if name else None
        if self.scope is not None:
            self.scope.__enter__()


def layer_kernel(
    resid_hbm, u_hbm, ls_hbm, dr_hbm, fr_hbm, bm_hbm, cm_hbm, skip_hbm, gain_hbm, vw_ref, gw_ref, up_ref, down_ref,
    out_ref,
    resid_ref, u_ref, ls_ref, dr_ref, fr_ref, bm_ref, cm_ref, skip_ref, gain_ref,
    up_all, down_first, down_last, vg, dec_re, dec_im, feed_re, feed_im, step_wide, rows, ends, total, totals, carry,
    uperm, wout, states, mixed_all, upd_all, glu, raised, squares, hidden,
    products, stage_far, relay_in, stage_near, from_near, kept, stage_own, from_own, own_part,
    local_sem, round_sem, ring_send, ring_recv, tot_send, tot_recv, cross_send, cross_recv, sum_send, sum_recv,
):
    phase = Phases()
    here, lane = lax.axis_index("sp"), lax.axis_index("tp")
    planes = SIDE * SIDE
    tokens, piece = resid_ref.shape
    half = tokens // 2
    shard = up_ref.shape[0]
    mix = Gather(mixed_all, ring_send.at[3], ring_recv.at[3])
    upd = Gather(upd_all, ring_send.at[4], ring_recv.at[4])
    right, left, partner = mix.device(1), mix.device(-1), mix.device(0, True)

    up = Relay(up_all, 0, shard // 2, ring_send.at[0], ring_recv.at[0], up_ref)
    first = Relay(down_first, 0, shard // 8, ring_send.at[1], ring_recv.at[1])
    last = Relay(down_last, 0, shard // 8, ring_send.at[2], ring_recv.at[2])
    near_planes = [up.index(0, *by) for by in ((1, 0), (-1, 0), (0, 1), (0, -1))]

    phase("signal")
    barrier = pltpu.get_barrier_semaphore()
    for target in near_planes:
        pl.semaphore_signal(barrier, inc=1, device_id={"sp": target, "tp": lane}, device_id_type=AXES)
    for target in (right, left, partner):
        pl.semaphore_signal(barrier, inc=1, device_id={"sp": here, "tp": target}, device_id_type=AXES)

    own_up = pl.ds(pl.multiple_of(here * shard, shard), shard)
    slim, width = shard // 4, up_ref.shape[1]
    own_down = pl.ds(pl.multiple_of(here * slim, slim), slim)
    own_units = pl.ds(pl.multiple_of(mix.core * width, width), width)

    def down_rows(core, k):
        return down_ref.at[pl.ds(pl.multiple_of(core * 2 * slim + k * slim, slim), slim), :]

    def cross_copy(number, src, dst):
        return pltpu.make_async_remote_copy(
            src_ref=src,
            dst_ref=dst,
            send_sem=cross_send.at[number],
            recv_sem=cross_recv.at[number],
            device_id={"sp": here, "tp": partner},
            device_id_type=AXES,
        )

    crossing = [
        cross_copy(k, down_rows(1 - mix.core, k), buf.at[own_down, own_units])
        for k, buf in enumerate((down_first, down_last))
    ]
    moves = (
        (u_hbm, u_ref), (dr_hbm, dr_ref), (fr_hbm, fr_ref), (ls_hbm, ls_ref), (bm_hbm, bm_ref), (cm_hbm, cm_ref),
        (up_ref, up_all.at[own_up, :]),
        (down_rows(mix.core, 0), down_first.at[own_down, own_units]),
        (down_rows(mix.core, 1), down_last.at[own_down, own_units]),
        (skip_hbm, skip_ref), (vw_ref, vg.at[:, :piece]), (gw_ref, vg.at[:, piece:]),
        (resid_hbm, resid_ref), (gain_hbm, gain_ref),
    )
    local = [pltpu.make_async_copy(src, dst, local_sem.at[k]) for k, (src, dst) in enumerate(moves)]
    for copy in local:
        copy.start()
    phase("barrier")
    pl.semaphore_wait(barrier, 7)
    phase("start_p")
    up.send_p()
    up.send_q(0)
    for copy in crossing:
        copy.start()

    def greet(number):
        for target in near_planes:
            pl.semaphore_signal(
                round_sem.at[number], inc=1, device_id={"sp": target, "tp": lane}, device_id_type=AXES
            )

    greet(0)
    for copy in local[:6]:
        copy.wait()
    phase("prepare")
    prepare(u_ref, ls_ref, dr_ref, fr_ref, bm_ref, cm_ref, uperm, step_wide, feed_re, feed_im, rows, wout)
    pl.semaphore_wait(round_sem.at[0], 4)
    greet(1)
    phase("first_pass")
    scan_refs = (step_wide, feed_re, feed_im, rows, dec_re, dec_im, ends)
    first_pass(*scan_refs, 0, 2)
    pl.semaphore_wait(round_sem.at[1], 4)
    greet(2)
    first_pass(*scan_refs, 2, 4)
    phase("chunk")
    chunk_prefix(ends, total)
    pl.semaphore_wait(round_sem.at[2], 4)

    def total_copy(by, slot, target):
        return pltpu.make_async_remote_copy(
            src_ref=total,
            dst_ref=totals.at[slot],
            send_sem=tot_send.at[by],
            recv_sem=tot_recv.at[slot],
            device_id={"sp": target, "tp": lane},
            device_id_type=AXES,
        )

    phase("totals")
    for by in range(1, planes):
        @pl.when(here + by < planes)
        def _():
            total_copy(by, here, lax.rem(here + by, planes)).start()

    phase("serve1")
    up.forward_p()
    up.near()
    up.forward_q(0)

    phase("fold")

    def fold(j, value):
        h_re, h_im = value
        total_copy(0, j, lax.rem(here + 1, planes)).wait_recv()
        a_re, a_im = totals[j, 0:8, :], totals[j, 8:16, :]
        x_re, x_im = totals[j, 16:24, :], totals[j, 24:32, :]
        return a_re * h_re - a_im * h_im + x_re, a_re * h_im + a_im * h_re + x_im

    zero = jnp.zeros((8, 128), f32)
    h_re, h_im = lax.fori_loop(0, here, fold, (zero, zero))
    carry[0:8, :] = h_re
    carry[8:16, :] = h_im
    phase("serve2")
    up.far()
    for copy in local[6:9]:
        copy.wait()
    for copy in crossing:
        copy.wait_recv()
    first.send_p()
    phase("second_pass")
    second_pass(dec_re, dec_im, feed_re, feed_im, ends, carry, states)
    local[9].wait()
    phase("read_out")
    own_cols = mix.cols(mix.core)
    mixed_all[mix.x, :, own_cols] = read_out(states, wout, uperm, skip_ref)
    phase("mix_start")
    mix.start()

    depth = 2 * piece

    def glu_part(chip, core=None):
        if core is None:
            lhs, at = mixed_all[chip], pl.ds(pl.multiple_of(chip * depth, depth), depth)
        else:
            lhs, at = mixed_all[chip, :, mix.cols(core)], pl.ds(pl.multiple_of((chip * 2 + core) * piece, piece), piece)
        return dot(lhs, vg[at, :])

    phase("mix_own")
    for copy in local[10:]:
        copy.wait()
    mix.across(0)
    glu[...] = glu_part(mix.x)
    phase("serve3")
    up.forward_q(-1)
    up.forward_q(1)
    first.send_q(0)
    phase("mix_near")
    mix.near()
    phase("serve4")
    up.forward_q(2)
    phase("mix_left")
    mix.across(-1)
    glu[...] += glu_part(around(mix.x, -1))
    phase("mix_right")
    mix.across(1)
    glu[...] += glu_part(around(mix.x, 1))
    phase("mix_far")
    mix.far()
    phase("mix_last")
    far_chip = around(mix.x, 2)
    glu[...] += glu_part(far_chip, mix.core)
    mix.across(2)
    glu[...] += glu_part(far_chip, 1 - mix.core)
    phase("updated")
    updated = (resid_ref[...].astype(f32) + glu[:, :piece] * jax.nn.sigmoid(glu[:, piece:])).astype(bf16)
    upd_all[upd.x, :, own_cols] = updated
    phase("upd_start")
    upd.start()
    phase("serve5")
    first.forward_p()
    first.near()
    last.send_p()

    def up_part(chip, start, core=None):
        if core is None:
            wide, at = upd_all[chip], pl.ds(pl.multiple_of(chip * depth, depth), depth)
        else:
            wide, at = upd_all[chip, :, upd.cols(core)], pl.ds(pl.multiple_of((chip * 2 + core) * piece, piece), piece)
        wide = wide.astype(f32)
        square = wide * wide
        square = sum(square[:, 128 * k : 128 * k + 128] for k in range(square.shape[1] // 128))
        product = dot((wide * gain_ref[:, at]).astype(bf16), up_all[at, :])
        if start:
            squares[...] = square
            raised[...] = product
        else:
            squares[...] += square
            raised[...] += product

    phase("up_wait")
    up.finish()
    phase("upd_own")
    upd.across(0)
    up_part(upd.x, True)
    phase("serve6")
    first.forward_q(0)
    first.far()
    last.send_q(0)
    phase("upd_near")
    upd.near()
    phase("upd_left")
    upd.across(-1)
    last.forward_p()
    up_part(around(upd.x, -1), False)
    phase("serve7")
    first.forward_q(-1)
    first.forward_q(1)
    phase("upd_right")
    upd.across(1)
    up_part(around(upd.x, 1), False)
    phase("serve8")
    first.forward_q(2)
    last.near()
    phase("upd_far")
    upd.far()
    up_part(far_chip, False, upd.core)
    phase("upd_last")
    upd.across(2)
    up_part(far_chip, False, 1 - upd.core)
    phase("hidden")
    inv_rms = lax.rsqrt(jnp.sum(squares[...], axis=1, keepdims=True) / (SIDE * depth) + rms_eps)
    active = jnp.maximum(raised[...] * inv_rms, 0.0)
    hidden[:, own_units] = (active * active).astype(bf16)
    crossing.append(cross_copy(2, hidden.at[:, own_units], hidden.at[:, own_units]))
    crossing[2].start()
    phase("serve9")
    last.far()
    last.forward_q(0)

    span = piece // 2
    quarter = half // 2

    def low_lanes(rows):
        return lax.broadcasted_iota(jnp.int32, (rows, span), 1) < span // 2

    def turned(value, by=None):
        return pltpu.roll(value, span // 2 if by is None else by, 1)

    def packed(value, core):
        top, low = value[:quarter], value[quarter:]
        if core == 0:
            return jnp.where(low_lanes(quarter), top, turned(low))
        return jnp.where(low_lanes(quarter), turned(top), low)

    class Sum:
        def __init__(self, k, buf):
            self.k, self.buf = k, buf
            self.relays = [
                self.copy(0, j, stage_far.at[k, j], relay_in.at[k, j], target) for j, target in enumerate((right, left))
            ]
            self.own = self.copy(1, 2, stage_own.at[k], from_own.at[k], partner)
            self.near = self.copy(2, 3, stage_near.at[k], from_near.at[k], right)

        def copy(self, send, recv, src, dst, target):
            return pltpu.make_async_remote_copy(
                src_ref=src,
                dst_ref=dst,
                send_sem=sum_send.at[self.k, send],
                recv_sem=sum_recv.at[self.k, recv],
                device_id={"sp": here, "tp": target},
                device_id_type=AXES,
            )

        def product(self, dx):
            return products[:, pl.ds(pl.multiple_of(around(mix.x, dx) * span, span), span)]

        def send_near(self, side, part, value):
            chip = around(mix.x, 1 - 2 * side)
            for core in range(2):
                stage_near[self.k, side, core, part] = packed(value, core).astype(bf16)
                self.copy(
                    2, 3, stage_near.at[self.k, side, core, part], from_near.at[self.k, mix.core, side, part],
                    chip * 2 + core,
                ).start()

        def start(self, *serve):
            k = self.k
            products[...] = dot_t(hidden[...], self.buf[...])
            far = self.product(2).astype(bf16)
            for j in range(2):
                stage_far[k, j] = far[j * half : j * half + half]
                self.relays[j].start()
            near = self.product(1)
            self.send_near(0, 1, near[half:])
            kept[k, 0] = near[:half]
            near = self.product(-1)
            self.send_near(1, 0, near[:half])
            kept[k, 1] = near[half:]
            if serve:
                serve[0]()
            own = self.product(0)
            for j in range(2):
                both = [packed(own[j * half : j * half + half], core) for core in range(2)]
                own_part[k, j] = jnp.where(mix.core == 0, both[0], both[1])
                stage_own[k, j] = jnp.where(mix.core == 0, both[1], both[0]).astype(bf16)
            self.own.start()
            if serve:
                serve[1]()

        def relay(self):
            for j in range(2):
                self.relays[j].wait_recv()
                self.send_near(j, j, kept[self.k, j] + relay_in[self.k, j].astype(f32))

        def result(self):
            k = self.k
            self.own.wait_recv()
            self.near.wait_recv()
            found = []
            for core in range(2):
                rows = []
                for j in range(2):
                    here_part = jnp.where(mix.core == core, own_part[k, j], from_own[k, j].astype(f32))
                    total = here_part + (from_near[k, core, 0, j].astype(f32) + from_near[k, core, 1, j].astype(f32))
                    rows += [total, turned(total)]
                found.append(jnp.concatenate(rows, axis=0))
            return found

        def drain(self):
            self.own.wait_send()
            self.near.wait_send()
            self.copy(0, 0, stage_far.at[self.k], stage_far.at[self.k], right).wait_send()

    phase("first_wait")
    first.finish()
    crossing[2].wait_recv()
    phase("first_sum")
    early, late = Sum(0, down_first), Sum(1, down_last)

    def serve_near():
        last.forward_q(-1)
        last.forward_q(1)

    def serve_far():
        last.forward_q(2)

    early.start(serve_near, serve_far)
    phase("first_relay")
    early.relay()
    phase("last_wait")
    last.finish()
    phase("last_sum")
    late.start()
    phase("last_relay")
    late.relay()
    phase("first_result")
    one = early.result()
    phase("last_result")
    two = late.result()
    phase("result")
    lane_group = lax.broadcasted_iota(jnp.int32, (tokens, span), 1) // slim
    blocks = []
    for b in range(2):
        block = None
        for core in range(2):
            for k, part in enumerate((one[core], two[core])):
                place = core * 2 + k
                moved = turned(part, (place - b) % 4 * slim) if place != b else part
                block = moved if block is None else jnp.where(lane_group == place, moved, block)
        blocks.append(block)
    down_sum = jnp.concatenate(blocks, axis=1)
    out_ref[...] = (upd_all[upd.x, :, own_cols].astype(f32) + down_sum).astype(bf16)

    phase("drain")
    for by in range(1, planes):
        @pl.when(here + by < planes)
        def _():
            total_copy(by, here, lax.rem(here + by, planes)).wait_send()

    for part in (up, first, last, mix, upd, early, late):
        part.drain()
    for copy in crossing:
        copy.wait_send()
    phase(None)


def per_device(
    resid, mixer_in, log_step, decay_real, frequency, input_matrix, output_matrix, skip_gain,
    value_weight, gate_weight, norm_gain, up_weight, down_weight,
):
    tokens, channels = mixer_in.shape
    groups, states = decay_real.shape
    width = groups * states
    planes, slots = lax.axis_size("sp"), lax.axis_size("tp")
    features = slots * channels
    hidden = up_weight.shape[1]
    span = channels // 2
    vmem = pl.BlockSpec(memory_space=pltpu.VMEM)
    hbm = pl.BlockSpec(memory_space=pl.ANY)
    wide = pltpu.VMEM((tokens, width), f32)
    block = pltpu.VMEM((tokens, channels), bf16)
    halves = pltpu.VMEM((2, 2, tokens // 2, span), bf16)
    packs = pltpu.VMEM((2, 2, tokens // 4, span), bf16)
    near = pltpu.VMEM((2, 2, 2, 2, tokens // 4, span), bf16)
    pieces = pltpu.VMEM((SIDE, tokens, 2 * channels), bf16)
    matrix = pltpu.VMEM((2, channels, states), f32)
    down = pltpu.VMEM((features // 4, 2 * hidden), bf16)
    dma = pltpu.SemaphoreType.DMA
    return pl.pallas_call(
        layer_kernel,
        out_shape=jax.ShapeDtypeStruct((tokens, channels), bf16),
        in_specs=[hbm] * 13,
        out_specs=vmem,
        scratch_shapes=[
            block, block, pltpu.VMEM((groups, tokens), f32),
            pltpu.VMEM((groups, states), f32), pltpu.VMEM((groups, states), f32), matrix, matrix,
            pltpu.VMEM((1, channels), f32), pltpu.VMEM((1, features), f32),
            pltpu.VMEM((features, hidden), bf16), down, down, pltpu.VMEM((features, 2 * channels), bf16),
            wide, wide, wide, wide, wide,
            pltpu.VMEM((8, width), f32), pltpu.VMEM((4, CHUNKS, width), f32),
            pltpu.VMEM((32, 128), f32), pltpu.VMEM((planes, 32, 128), f32), pltpu.VMEM((16, 128), f32),
            block, pltpu.VMEM((channels, 2 * width), bf16), pltpu.VMEM((tokens, 2 * width), bf16),
            pieces, pieces, pltpu.VMEM((tokens, 2 * channels), f32),
            pltpu.VMEM((tokens, hidden), f32), pltpu.VMEM((tokens, 128), f32), pltpu.VMEM((tokens, 2 * hidden), bf16),
            pltpu.VMEM((tokens, SIDE * span), f32), halves, halves, near, near, pltpu.VMEM((2, 2, tokens // 2, span), f32),
            packs, packs, pltpu.VMEM((2, 2, tokens // 4, span), f32),
            dma((14,)), pltpu.SemaphoreType.REGULAR((3,)), dma((5,)), dma((5, 8)),
            dma((planes,)), dma((planes,)), dma((3,)), dma((3,)), dma((2, 3)), dma((2, 4)),
        ],
        name="layer",
        compiler_params=pltpu.CompilerParams(
            vmem_limit_bytes=58 * 2**20, collective_id=0, has_side_effects=True
        ),
    )(
        resid, mixer_in, log_step.T, decay_real, frequency,
        input_matrix.transpose(0, 1, 3, 2).reshape(2, channels, states), output_matrix.reshape(2, channels, states),
        skip_gain.reshape(1, -1), norm_gain.reshape(1, -1), value_weight, gate_weight, up_weight, down_weight,
    )


def solution(mesh):
    in_specs = (
        P("sp", "tp"), P("sp", "tp"), P("sp", "tp"), P("tp", None), P("tp", None),
        P(None, "tp", None, None), P(None, "tp", None, None), P("tp"),
        P(None, "tp"), P(None, "tp"), P(), P("sp", "tp"), P("sp", "tp"),
    )
    return jax.shard_map(
        per_device, mesh=mesh, in_specs=in_specs, out_specs=P("sp", "tp"), check_vma=False
    )
```

```python
import functools
import math

import jax
import jax.numpy as jnp
from jax import lax
from jax.experimental import pallas as pl
from jax.experimental.pallas import tpu as pltpu
from jax.sharding import PartitionSpec as P

rms_eps = 1e-06
f32 = jnp.float32
bf16 = jnp.bfloat16
CHUNKS = 8


def onehot(shape, test):
    row = lax.broadcasted_iota(jnp.int32, shape, 0)
    col = lax.broadcasted_iota(jnp.int32, shape, 1)
    return jnp.where(test(row, col), 1.0, 0.0).astype(bf16)


def split3(x):
    hi = x.astype(bf16)
    rest = x - hi.astype(f32)
    mid = rest.astype(bf16)
    return hi, mid, (rest - mid.astype(f32)).astype(bf16)


def dot(a, b):
    return jnp.dot(a, b, preferred_element_type=f32)


def dot_t(a, b):
    return lax.dot_general(a, b, (((1,), (1,)), ((), ())), preferred_element_type=f32)


def spread_row(x, states):
    groups = x.shape[0]
    width = groups * states
    lanes = onehot((states, width), lambda r, c: r == c % states)
    wide = sum(dot(part, lanes) for part in split3(x))
    row = lax.broadcasted_iota(jnp.int32, wide.shape, 0)
    col = lax.broadcasted_iota(jnp.int32, wide.shape, 1)
    return jnp.sum(jnp.where(row == col // states, wide, 0.0), axis=0, keepdims=True)


def prepare(u_ref, ls_ref, dr_ref, fr_ref, bm_ref, cm_ref, uperm, step_wide, proj_re, proj_im, rows, wout):
    tokens, channels = u_ref.shape
    groups, states = dr_ref.shape
    width = groups * states
    per_group = channels // groups
    span = tokens // CHUNKS
    perm = onehot((tokens, tokens), lambda r, c: c == (r % CHUNKS) * span + r // CHUNKS)
    u_sorted = dot(perm, u_ref[...]).astype(bf16)
    uperm[...] = u_sorted
    decay = spread_row(dr_ref[...], states)
    angular = spread_row(fr_ref[...], states)
    rows[0:1, :] = -decay
    rows[1:2, :] = 0.5 * angular
    modulus = decay * decay + angular * angular
    inv_re = -decay / modulus
    inv_im = -angular / modulus
    step = jnp.exp(ls_ref[...])
    step = sum(dot_t(perm, part) for part in split3(step))
    group_lanes = onehot((groups, width), lambda r, c: r == c // states)
    step_wide[...] = sum(dot(part, group_lanes) for part in split3(step))
    state_lanes = onehot((states, width), lambda r, c: r == c % states)
    row = lax.broadcasted_iota(jnp.int32, (channels, width), 0)
    col = lax.broadcasted_iota(jnp.int32, (channels, width), 1)
    same = row // per_group == col // states
    b_re = dot(bm_ref[0].astype(bf16), state_lanes)
    b_im = dot(bm_ref[1].astype(bf16), state_lanes)
    w_re = jnp.where(same, b_re * inv_re - b_im * inv_im, 0.0).astype(bf16)
    w_im = jnp.where(same, b_re * inv_im + b_im * inv_re, 0.0).astype(bf16)
    proj_re[...] = dot(u_sorted, w_re)
    proj_im[...] = dot(u_sorted, w_im)
    wout[:, :width] = jnp.where(same, dot(cm_ref[0].astype(bf16), state_lanes), 0.0).astype(bf16)
    wout[:, width:] = jnp.where(same, -dot(cm_ref[1].astype(bf16), state_lanes), 0.0).astype(bf16)


SIN = (-1.0 / 6, 1.0 / 120, -1.0 / 5040, 1.0 / 362880, -1.0 / 39916800)
COS = (-0.5, 1.0 / 24, -1.0 / 720, 1.0 / 40320, -1.0 / 3628800)


def series(q, terms):
    total = terms[-1] * q
    for term in terms[-2::-1]:
        total = (total + term) * q
    return total


def first_pass(step_wide, proj_re, proj_im, rows, dec_re, dec_im, ends, first, last):
    tokens, width = step_wide.shape
    block = 256

    def one_block(b, _):
        lanes = pl.ds(pl.multiple_of(b * block, block), block)
        minus_decay = jnp.broadcast_to(rows[0:1, lanes], (CHUNKS, block))
        half_angular = jnp.broadcast_to(rows[1:2, lanes], (CHUNKS, block))

        def one_step(i, carry):
            a_re, a_im, x_re, x_im = carry
            at = pl.ds(pl.multiple_of(i * CHUNKS, CHUNKS), CHUNKS)
            step = step_wide[at, lanes]
            half = step * half_angular
            q = half * half
            sine = half + half * series(q, SIN)
            cosine = 1.0 + series(q, COS)
            factor = jnp.exp(step * minus_decay)
            twice = factor * (sine + sine)
            d_re = factor - twice * sine
            d_im = twice * cosine
            less = d_re - 1.0
            p_re = proj_re[at, lanes]
            p_im = proj_im[at, lanes]
            u_re = less * p_re - d_im * p_im
            u_im = less * p_im + d_im * p_re
            dec_re[at, lanes] = d_re
            dec_im[at, lanes] = d_im
            proj_re[at, lanes] = u_re
            proj_im[at, lanes] = u_im
            return (
                d_re * a_re - d_im * a_im,
                d_re * a_im + d_im * a_re,
                d_re * x_re - d_im * x_im + u_re,
                d_re * x_im + d_im * x_re + u_im,
            )

        zero = jnp.zeros((CHUNKS, block), f32)
        found = lax.fori_loop(0, tokens // CHUNKS, one_step, (zero + 1.0, zero, zero, zero), unroll=2)
        for k in range(4):
            ends[k, :, lanes] = found[k]
        return 0

    lax.fori_loop(first, last, one_block, 0)


def chain(early, late):
    return (
        early[0] * late[0] - early[1] * late[1],
        early[0] * late[1] + early[1] * late[0],
        late[0] * early[2] - late[1] * early[3] + late[2],
        late[0] * early[3] + late[1] * early[2] + late[3],
    )


def chunk_prefix(ends, total):
    width = ends.shape[2]
    value = tuple(ends[k] for k in range(4))
    row = lax.broadcasted_iota(jnp.int32, value[0].shape, 0)
    unit = (1.0, 0.0, 0.0, 0.0)

    def moved(value, by):
        return tuple(
            jnp.where(row >= by, pltpu.roll(part, by, 0), zero) for part, zero in zip(value, unit)
        )

    for by in (1, 2, 4):
        value = chain(moved(value, by), value)
    for k in range(4):
        for j in range(width // 128):
            total[8 * k + j : 8 * k + j + 1, :] = value[k][CHUNKS - 1 :, 128 * j : 128 * j + 128]
    before = moved(value, 1)
    for k in range(4):
        ends[k] = before[k]


def second_pass(dec_re, dec_im, feed_re, feed_im, ends, carry, states):
    tokens, width = dec_re.shape
    block = 512
    for b in range(width // block):
        lanes = pl.ds(b * block, block)
        lanes_im = pl.ds(width + b * block, block)
        per = block // 128
        h_re = jnp.concatenate([carry[per * b + j : per * b + j + 1, :] for j in range(per)], axis=1)
        h_im = jnp.concatenate([carry[8 + per * b + j : 9 + per * b + j, :] for j in range(per)], axis=1)
        a_re, a_im = ends[0, :, lanes], ends[1, :, lanes]
        x_re = ends[2, :, lanes] + a_re * h_re - a_im * h_im
        x_im = ends[3, :, lanes] + a_re * h_im + a_im * h_re

        def one_step(i, value):
            x_re, x_im = value
            seen = []
            for k in range(2):
                at = pl.ds(pl.multiple_of(i * 2 * CHUNKS + k * CHUNKS, CHUNKS), CHUNKS)
                d_re, d_im = dec_re[at, lanes], dec_im[at, lanes]
                x_re, x_im = (
                    d_re * x_re - d_im * x_im + feed_re[at, lanes],
                    d_re * x_im + d_im * x_re + feed_im[at, lanes],
                )
                seen.append((x_re, x_im))
            both = pl.ds(pl.multiple_of(i * 2 * CHUNKS, 2 * CHUNKS), 2 * CHUNKS)
            states[both, lanes] = jnp.concatenate([seen[0][0], seen[1][0]], axis=0).astype(bf16)
            states[both, lanes_im] = jnp.concatenate([seen[0][1], seen[1][1]], axis=0).astype(bf16)
            return x_re, x_im

        lax.fori_loop(0, tokens // (2 * CHUNKS), one_step, (x_re, x_im), unroll=2)


def read_out(states, wout, uperm, skip_ref):
    tokens = states.shape[0]
    span = tokens // CHUNKS
    out = dot_t(states[...], wout[...]) + skip_ref[...] * uperm[...].astype(f32)
    mixed = jax.nn.gelu(out).astype(bf16)
    back = onehot((tokens, tokens), lambda r, c: r == (c % CHUNKS) * span + c // CHUNKS)
    return dot(back, mixed).astype(bf16)


AXES = pl.DeviceIdType.MESH
SIDE = 4


def around(index, by):
    return lax.rem(index + by + SIDE, SIDE)


class Relay:
    def __init__(self, buf, first, rows, send_sem, recv_sem, own=None):
        here = lax.axis_index("sp")
        self.zy = here // SIDE, lax.rem(here, SIDE)
        self.buf, self.first, self.rows, self.own = buf, first, rows, own
        self.shard = buf.shape[0] // (SIDE * SIDE)
        self.send_sem, self.recv_sem = send_sem, recv_sem
        self.sent = 0

    def index(self, side, dp, dq):
        dz, dy = (dq, dp) if side == 0 else (dp, dq)
        return around(self.zy[0], dz) * SIDE + around(self.zy[1], dy)

    def group(self, dp, dq, half):
        if dq == 0:
            return 2 if dp == 2 else int((dp == -1) == (half == 1))
        return 3 + dp % SIDE if dq != 2 and (dq == -1) == (half == 0) else 7

    def send(self, side, dp, dq, half, to_p, to_q):
        width = self.buf.shape[1] // 2
        cols = slice(half * width, half * width + width)
        row = pl.multiple_of(self.index(side, dp, dq) * self.shard + side * self.rows, self.rows)
        piece = self.buf.at[pl.ds(row, self.rows), cols]
        own = self.own is not None and dp == 0 and dq == 0
        first = self.first + side * self.rows
        seen = [(d + 1) % SIDE - 1 for d in (dp - to_p, dq - to_q)]
        pltpu.make_async_remote_copy(
            src_ref=self.own.at[first : first + self.rows, cols] if own else piece,
            dst_ref=piece,
            send_sem=self.send_sem,
            recv_sem=self.recv_sem.at[self.group(*seen, half)],
            device_id={"sp": self.index(side, to_p, to_q), "tp": lax.axis_index("tp")},
            device_id_type=AXES,
        ).start()
        self.sent += 1

    def whole(self, count, group):
        rows = self.buf.at[: count * self.rows // 2, :]
        return pltpu.make_async_remote_copy(
            src_ref=rows,
            dst_ref=rows,
            send_sem=self.send_sem,
            recv_sem=self.recv_sem.at[group],
            device_id={"sp": self.index(0, 1, 0), "tp": lax.axis_index("tp")},
            device_id_type=AXES,
        )

    def arrived(self, group):
        self.whole(32 if group == 7 else 4, group).wait_recv()

    def send_p(self):
        for k in range(2):
            for side in range(2):
                self.send(side, 0, 0, k, 1, 0)
                self.send(side, 0, 0, 1 - k, -1, 0)

    def send_q(self, dp, k):
        for side in range(2):
            self.send(side, dp, 0, k, 0, 1)
            self.send(side, dp, 0, 1 - k, 0, -1)

    def forward_p(self):
        self.arrived(0)
        for side in range(2):
            self.send(side, -1, 0, 0, 1, 0)
            self.send(side, 1, 0, 1, -1, 0)

    def near(self):
        self.arrived(1)
        self.send_q(-1, 0)
        self.send_q(1, 0)

    def near_rest(self):
        self.send_q(-1, 1)
        self.send_q(1, 1)

    def far(self):
        self.arrived(2)
        self.send_q(2, 0)

    def far_rest(self):
        self.send_q(2, 1)

    def forward_q(self, dp):
        self.arrived(3 + dp % SIDE)
        for side in range(2):
            self.send(side, dp, -1, 0, 0, 1)
            self.send(side, dp, 1, 1, 0, -1)

    def finish(self):
        self.arrived(7)

    def drain(self):
        self.whole(self.sent, 0).wait_send()


class Gather:
    def __init__(self, buf, send_sem, recv_sem):
        here = lax.axis_index("tp")
        self.x, self.core = here // 2, lax.rem(here, 2)
        self.buf, self.send_sem, self.recv_sem = buf, send_sem, recv_sem
        self.sent = 0

    def device(self, dx, other=False):
        return around(self.x, dx) * 2 + (1 - self.core if other else self.core)

    def cols(self, core):
        width = self.buf.shape[2] // 2
        return pl.ds(pl.multiple_of(core * width, width), width)

    def send(self, dx, half, to_x):
        rows = self.buf.shape[1] // 2
        piece = self.buf.at[around(self.x, dx), half * rows : half * rows + rows, self.cols(self.core)]
        if to_x:
            seen = (dx - to_x + 1) % SIDE - 1
            group = 2 if seen == 2 else int((seen == -1) == (half == 1))
        else:
            group = 3 + dx % SIDE
        pltpu.make_async_remote_copy(
            src_ref=piece,
            dst_ref=piece,
            send_sem=self.send_sem,
            recv_sem=self.recv_sem.at[group],
            device_id={"sp": lax.axis_index("sp"), "tp": self.device(to_x, not to_x)},
            device_id_type=AXES,
        ).start()
        self.sent += 1

    def whole(self, rows, group):
        return pltpu.make_async_remote_copy(
            src_ref=rows,
            dst_ref=rows,
            send_sem=self.send_sem,
            recv_sem=self.recv_sem.at[group],
            device_id={"sp": lax.axis_index("sp"), "tp": self.device(1)},
            device_id_type=AXES,
        )

    def arrived(self, group):
        self.whole(self.buf.at[0, :, : self.buf.shape[2] // 2], group).wait_recv()

    def start(self):
        for k in range(2):
            self.send(0, k, 1)
            self.send(0, 1 - k, -1)
        for k in range(2):
            self.send(0, k, 0)

    def near(self):
        self.arrived(0)
        self.send(-1, 0, 1)
        self.send(1, 1, -1)
        self.send(-1, 0, 0)
        self.send(1, 1, 0)
        self.arrived(1)
        self.send(-1, 1, 0)
        self.send(1, 0, 0)

    def far(self):
        self.arrived(2)
        self.send(2, 0, 0)
        self.send(2, 1, 0)

    def across(self, dx):
        self.arrived(3 + dx % SIDE)

    def drain(self):
        self.whole(self.buf.at[:, : self.buf.shape[1] * self.sent // 16, :], 0).wait_send()


class Phases:
    def __init__(self):
        self.scope = None

    def __call__(self, name):
        if self.scope is not None:
            self.scope.__exit__(None, None, None)
        self.scope = jax.named_scope(name) if name else None
        if self.scope is not None:
            self.scope.__enter__()


def layer_kernel(
    resid_hbm, u_hbm, ls_hbm, dr_hbm, fr_hbm, bm_hbm, cm_hbm, skip_hbm, gain_hbm, vw_ref, gw_ref, up_ref, down_ref,
    out_ref,
    resid_ref, u_ref, ls_ref, dr_ref, fr_ref, bm_ref, cm_ref, skip_ref, gain_ref,
    up_all, down_first, down_last, vg, dec_re, dec_im, feed_re, feed_im, step_wide, rows, ends, total, totals, carry,
    uperm, wout, states, mixed_all, upd_all, glu, raised, squares, hidden,
    products, stage_far, relay_in, stage_near, from_near, kept, stage_own, from_own, own_part, kept_out,
    local_sem, round_sem, ring_send, ring_recv, tot_send, tot_recv, cross_send, cross_recv, sum_send, sum_recv,
):
    phase = Phases()
    here, lane = lax.axis_index("sp"), lax.axis_index("tp")
    planes = SIDE * SIDE
    tokens, piece = resid_ref.shape
    half = tokens // 2
    shard = up_ref.shape[0]
    mix = Gather(mixed_all, ring_send.at[3], ring_recv.at[3])
    upd = Gather(upd_all, ring_send.at[4], ring_recv.at[4])
    right, left, partner = mix.device(1), mix.device(-1), mix.device(0, True)

    up = Relay(up_all, 0, shard // 2, ring_send.at[0], ring_recv.at[0], up_ref)
    first = Relay(down_first, 0, shard // 8, ring_send.at[1], ring_recv.at[1])
    last = Relay(down_last, 0, shard // 8, ring_send.at[2], ring_recv.at[2])
    near_planes = [up.index(0, *by) for by in ((1, 0), (-1, 0), (0, 1), (0, -1))]

    phase("signal")
    barrier = pltpu.get_barrier_semaphore()
    for target in near_planes:
        pl.semaphore_signal(barrier, inc=1, device_id={"sp": target, "tp": lane}, device_id_type=AXES)
    for target in (right, left, partner):
        pl.semaphore_signal(barrier, inc=1, device_id={"sp": here, "tp": target}, device_id_type=AXES)

    own_up = pl.ds(pl.multiple_of(here * shard, shard), shard)
    slim, width = shard // 4, up_ref.shape[1]
    own_down = pl.ds(pl.multiple_of(here * slim, slim), slim)
    own_units = pl.ds(pl.multiple_of(mix.core * width, width), width)

    def down_rows(core, k):
        return down_ref.at[pl.ds(pl.multiple_of(core * 2 * slim + k * slim, slim), slim), :]

    def cross_copy(number, src, dst):
        return pltpu.make_async_remote_copy(
            src_ref=src,
            dst_ref=dst,
            send_sem=cross_send.at[number],
            recv_sem=cross_recv.at[number],
            device_id={"sp": here, "tp": partner},
            device_id_type=AXES,
        )

    crossing = [
        cross_copy(k, down_rows(1 - mix.core, k), buf.at[own_down, own_units])
        for k, buf in enumerate((down_first, down_last))
    ]
    moves = (
        (u_hbm, u_ref), (dr_hbm, dr_ref), (fr_hbm, fr_ref), (ls_hbm, ls_ref), (bm_hbm, bm_ref), (cm_hbm, cm_ref),
        (up_ref, up_all.at[own_up, :]),
        (down_rows(mix.core, 0), down_first.at[own_down, own_units]),
        (down_rows(mix.core, 1), down_last.at[own_down, own_units]),
        (skip_hbm, skip_ref), (vw_ref, vg.at[:, :piece]), (gw_ref, vg.at[:, piece:]),
        (resid_hbm, resid_ref), (gain_hbm, gain_ref),
    )
    local = [pltpu.make_async_copy(src, dst, local_sem.at[k]) for k, (src, dst) in enumerate(moves)]
    for copy in local:
        copy.start()
    phase("barrier")
    pl.semaphore_wait(barrier, 7)
    phase("start_p")
    up.send_p()
    up.send_q(0, 0)
    up.send_q(0, 1)
    for copy in crossing:
        copy.start()

    def greet(number):
        for target in near_planes:
            pl.semaphore_signal(
                round_sem.at[number], inc=1, device_id={"sp": target, "tp": lane}, device_id_type=AXES
            )

    greet(0)
    for copy in local[:6]:
        copy.wait()
    phase("prepare")
    prepare(u_ref, ls_ref, dr_ref, fr_ref, bm_ref, cm_ref, uperm, step_wide, feed_re, feed_im, rows, wout)
    pl.semaphore_wait(round_sem.at[0], 4)
    greet(1)
    phase("first_pass")
    scan_refs = (step_wide, feed_re, feed_im, rows, dec_re, dec_im, ends)
    first_pass(*scan_refs, 0, 2)
    pl.semaphore_wait(round_sem.at[1], 4)
    greet(2)
    first_pass(*scan_refs, 2, 4)
    phase("chunk")
    chunk_prefix(ends, total)
    pl.semaphore_wait(round_sem.at[2], 4)

    def total_copy(src, dst, target):
        return pltpu.make_async_remote_copy(
            src_ref=src,
            dst_ref=dst,
            send_sem=tot_send.at[0],
            recv_sem=tot_recv.at[0],
            device_id={"sp": target, "tp": lane},
            device_id_type=AXES,
        )

    phase("totals")
    for by in range(1, planes):
        @pl.when(here + by < planes)
        def _():
            total_copy(total, totals.at[here], lax.rem(here + by, planes)).start()

    phase("serve1")
    up.forward_p()
    up.near()
    up.forward_q(0)
    up.near_rest()

    phase("fold")

    for count in range(1, planes):
        @pl.when(here == count)
        def _():
            total_copy(totals.at[:count], totals.at[:count], lax.rem(here + 1, planes)).wait_recv()

    def fold(j, value):
        h_re, h_im = value
        a_re, a_im = totals[j, 0:8, :], totals[j, 8:16, :]
        x_re, x_im = totals[j, 16:24, :], totals[j, 24:32, :]
        return a_re * h_re - a_im * h_im + x_re, a_re * h_im + a_im * h_re + x_im

    zero = jnp.zeros((8, 128), f32)
    h_re, h_im = lax.fori_loop(0, here, fold, (zero, zero))
    carry[0:8, :] = h_re
    carry[8:16, :] = h_im
    phase("serve2")
    up.far()
    up.far_rest()
    for copy in local[6:9]:
        copy.wait()
    for copy in crossing:
        copy.wait_recv()
    first.send_p()
    phase("second_pass")
    second_pass(dec_re, dec_im, feed_re, feed_im, ends, carry, states)
    local[9].wait()
    phase("read_out")
    own_cols = mix.cols(mix.core)
    mixed_all[mix.x, :, own_cols] = read_out(states, wout, uperm, skip_ref)
    phase("mix_start")
    mix.start()

    depth = 2 * piece

    def glu_part(chip, core=None):
        if core is None:
            lhs, at = mixed_all[chip], pl.ds(pl.multiple_of(chip * depth, depth), depth)
        else:
            lhs, at = mixed_all[chip, :, mix.cols(core)], pl.ds(pl.multiple_of((chip * 2 + core) * piece, piece), piece)
        return dot(lhs, vg[at, :])

    phase("mix_own")
    for copy in local[10:]:
        copy.wait()
    mix.across(0)
    glu[...] = glu_part(mix.x)
    phase("serve3")
    up.forward_q(-1)
    up.forward_q(1)
    first.send_q(0, 0)
    first.send_q(0, 1)
    phase("mix_near")
    mix.near()
    phase("serve4")
    up.forward_q(2)
    phase("mix_left")
    mix.across(-1)
    glu[...] += glu_part(around(mix.x, -1))
    phase("mix_right")
    mix.across(1)
    glu[...] += glu_part(around(mix.x, 1))
    phase("mix_far")
    mix.far()
    phase("mix_last")
    far_chip = around(mix.x, 2)
    glu[...] += glu_part(far_chip, mix.core)
    mix.across(2)
    glu[...] += glu_part(far_chip, 1 - mix.core)
    phase("updated")
    updated = (resid_ref[...].astype(f32) + glu[:, :piece] * jax.nn.sigmoid(glu[:, piece:])).astype(bf16)
    upd_all[upd.x, :, own_cols] = updated
    phase("upd_start")
    upd.start()
    phase("serve5")
    first.forward_p()
    first.near()
    first.near_rest()
    last.send_p()

    def up_part(chip, start, core=None):
        if core is None:
            wide, at = upd_all[chip], pl.ds(pl.multiple_of(chip * depth, depth), depth)
        else:
            wide, at = upd_all[chip, :, upd.cols(core)], pl.ds(pl.multiple_of((chip * 2 + core) * piece, piece), piece)
        wide = wide.astype(f32)
        square = wide * wide
        square = sum(square[:, 128 * k : 128 * k + 128] for k in range(square.shape[1] // 128))
        product = dot((wide * gain_ref[:, at]).astype(bf16), up_all[at, :])
        if start:
            squares[...] = square
            raised[...] = product
        else:
            squares[...] += square
            raised[...] += product

    phase("up_wait")
    up.finish()
    phase("upd_own")
    upd.across(0)
    up_part(upd.x, True)
    phase("serve6")
    first.forward_q(0)
    first.far()
    last.send_q(0, 0)
    first.far_rest()
    last.send_q(0, 1)
    phase("upd_near")
    upd.near()
    phase("upd_left")
    upd.across(-1)
    last.forward_p()
    up_part(around(upd.x, -1), False)
    phase("serve7")
    first.forward_q(-1)
    first.forward_q(1)
    phase("upd_right")
    upd.across(1)
    up_part(around(upd.x, 1), False)
    phase("serve8")
    first.forward_q(2)
    last.near()
    phase("upd_far")
    upd.far()
    up_part(far_chip, False, upd.core)
    phase("upd_last")
    upd.across(2)
    up_part(far_chip, False, 1 - upd.core)
    phase("hidden")
    inv_rms = lax.rsqrt(jnp.sum(squares[...], axis=1, keepdims=True) / (SIDE * depth) + rms_eps)
    active = jnp.maximum(raised[...] * inv_rms, 0.0)
    hidden[:, own_units] = (active * active).astype(bf16)
    crossing.append(cross_copy(2, hidden.at[:, own_units], hidden.at[:, own_units]))
    crossing[2].start()
    phase("serve9")
    last.far()
    last.forward_q(0)
    last.near_rest()
    last.far_rest()

    span = piece // 2
    quarter = half // 2

    chunk = quarter // 2

    def turned(value, by=None):
        return pltpu.roll(value, span // 2 if by is None else by, 1)

    low_lanes = lax.broadcasted_iota(jnp.int32, (chunk, span), 1) < span // 2

    def packed(value, core):
        parts = []
        for c in range(value.shape[0] // quarter):
            top, low = (value[c * quarter + k * chunk : c * quarter + k * chunk + chunk] for k in range(2))
            parts.append(jnp.where(low_lanes, top, turned(low)) if core == 0 else jnp.where(low_lanes, turned(top), low))
        return jnp.concatenate(parts, axis=0)

    class Sum:
        def __init__(self, k, buf):
            self.k, self.buf = k, buf
            self.relays = [
                [
                    self.copy(
                        0, 2 * j + c, stage_far.at[k, j, c * quarter : c * quarter + quarter],
                        relay_in.at[k, j, c * quarter : c * quarter + quarter], target,
                    )
                    for c in range(2)
                ]
                for j, target in enumerate((right, left))
            ]
            self.own = self.copy(1, 4, stage_own.at[k], from_own.at[k], partner)
            self.near = self.copy(2, 5, stage_near.at[k], from_near.at[k], right)

        def copy(self, send, recv, src, dst, target):
            return pltpu.make_async_remote_copy(
                src_ref=src,
                dst_ref=dst,
                send_sem=sum_send.at[self.k, send],
                recv_sem=sum_recv.at[self.k, recv],
                device_id={"sp": here, "tp": target},
                device_id_type=AXES,
            )

        def product(self, dx):
            return products[:, pl.ds(pl.multiple_of(around(mix.x, dx) * span, span), span)]

        def send_near(self, side, part, value, first=0):
            chip = around(mix.x, 1 - 2 * side)
            rows = slice(first, first + value.shape[0] // 2)
            for core in range(2):
                stage_near[self.k, side, core, part, rows] = packed(value, core).astype(bf16)
                self.copy(
                    2, 5, stage_near.at[self.k, side, core, part, rows],
                    from_near.at[self.k, mix.core, side, part, rows], chip * 2 + core,
                ).start()

        def start(self, *serve):
            k = self.k
            products[...] = dot_t(hidden[...], self.buf[...])
            far = self.product(2).astype(bf16)
            for j in range(2):
                stage_far[k, j] = far[j * half : j * half + half]
            for c in range(2):
                for j in range(2):
                    self.relays[j][c].start()
            near = self.product(1)
            self.send_near(0, 1, near[half:])
            kept[k, 0] = near[:half]
            near = self.product(-1)
            self.send_near(1, 0, near[:half])
            kept[k, 1] = near[half:]
            if serve:
                serve[0]()
            own = self.product(0)
            for j in range(2):
                both = [packed(own[j * half : j * half + half], core) for core in range(2)]
                own_part[k, j] = jnp.where(mix.core == 0, both[0], both[1])
                stage_own[k, j] = jnp.where(mix.core == 0, both[1], both[0]).astype(bf16)
            self.own.start()
            if serve:
                serve[1]()

        def relay(self):
            k = self.k
            for c in range(2):
                rows = slice(c * quarter, c * quarter + quarter)
                for j in range(2):
                    self.relays[j][c].wait_recv()
                    self.send_near(j, j, kept[k, j, rows] + relay_in[k, j, rows].astype(f32), c * chunk)

        def result(self):
            k = self.k
            self.own.wait_recv()
            self.near.wait_recv()
            found = []
            for core in range(2):
                rows = []
                for j in range(2):
                    here_part = jnp.where(mix.core == core, own_part[k, j], from_own[k, j].astype(f32))
                    total = here_part + (from_near[k, core, 0, j].astype(f32) + from_near[k, core, 1, j].astype(f32))
                    for c in range(2):
                        part = total[c * chunk : c * chunk + chunk]
                        rows += [part, turned(part)]
                found.append(jnp.concatenate(rows, axis=0))
            return found

        def drain(self):
            self.own.wait_send()
            self.near.wait_send()
            self.copy(0, 0, stage_far.at[self.k], stage_far.at[self.k], right).wait_send()

    phase("first_wait")
    first.finish()
    crossing[2].wait_recv()
    phase("first_sum")
    early, late = Sum(0, down_first), Sum(1, down_last)

    def serve_near():
        last.forward_q(-1)
        last.forward_q(1)

    def serve_far():
        last.forward_q(2)

    early.start(serve_near, serve_far)
    phase("first_relay")
    early.relay()
    phase("last_wait")
    last.finish()
    phase("last_sum")
    late.start()
    phase("last_relay")
    late.relay()
    phase("first_result")
    lane_group = lax.broadcasted_iota(jnp.int32, (tokens, span), 1) // slim
    blocks = [upd_all[upd.x, :, own_cols].astype(f32)[:, b * span : b * span + span] for b in range(2)]

    def put_in(k, found):
        for b in range(2):
            for core in range(2):
                place = core * 2 + k
                moved = turned(found[core], (place - b) % 4 * slim) if place != b else found[core]
                blocks[b] = blocks[b] + jnp.where(lane_group == place, moved, 0.0)

    put_in(0, early.result())
    for b in range(2):
        kept_out[:, b * span : b * span + span] = blocks[b]
    phase("last_result")
    two = late.result()
    phase("result")
    blocks = [kept_out[:, b * span : b * span + span] for b in range(2)]
    put_in(1, two)
    out_ref[...] = jnp.concatenate(blocks, axis=1).astype(bf16)

    phase("drain")
    for count in range(1, planes):
        @pl.when(planes - 1 - here == count)
        def _():
            total_copy(totals.at[:count], totals.at[:count], lax.rem(here + 1, planes)).wait_send()

    for part in (up, first, last, mix, upd, early, late):
        part.drain()
    for copy in crossing:
        copy.wait_send()
    phase(None)


def per_device(
    resid, mixer_in, log_step, decay_real, frequency, input_matrix, output_matrix, skip_gain,
    value_weight, gate_weight, norm_gain, up_weight, down_weight,
):
    tokens, channels = mixer_in.shape
    groups, states = decay_real.shape
    width = groups * states
    planes, slots = lax.axis_size("sp"), lax.axis_size("tp")
    features = slots * channels
    hidden = up_weight.shape[1]
    span = channels // 2
    vmem = pl.BlockSpec(memory_space=pltpu.VMEM)
    hbm = pl.BlockSpec(memory_space=pl.ANY)
    wide = pltpu.VMEM((tokens, width), f32)
    block = pltpu.VMEM((tokens, channels), bf16)
    halves = pltpu.VMEM((2, 2, tokens // 2, span), bf16)
    packs = pltpu.VMEM((2, 2, tokens // 4, span), bf16)
    near = pltpu.VMEM((2, 2, 2, 2, tokens // 4, span), bf16)
    pieces = pltpu.VMEM((SIDE, tokens, 2 * channels), bf16)
    matrix = pltpu.VMEM((2, channels, states), f32)
    down = pltpu.VMEM((features // 4, 2 * hidden), bf16)
    dma = pltpu.SemaphoreType.DMA
    return pl.pallas_call(
        layer_kernel,
        out_shape=jax.ShapeDtypeStruct((tokens, channels), bf16),
        in_specs=[hbm] * 13,
        out_specs=vmem,
        scratch_shapes=[
            block, block, pltpu.VMEM((groups, tokens), f32),
            pltpu.VMEM((groups, states), f32), pltpu.VMEM((groups, states), f32), matrix, matrix,
            pltpu.VMEM((1, channels), f32), pltpu.VMEM((1, features), f32),
            pltpu.VMEM((features, hidden), bf16), down, down, pltpu.VMEM((features, 2 * channels), bf16),
            wide, wide, wide, wide, wide,
            pltpu.VMEM((8, width), f32), pltpu.VMEM((4, CHUNKS, width), f32),
            pltpu.VMEM((32, 128), f32), pltpu.VMEM((planes, 32, 128), f32), pltpu.VMEM((16, 128), f32),
            block, pltpu.VMEM((channels, 2 * width), bf16), pltpu.VMEM((tokens, 2 * width), bf16),
            pieces, pieces, pltpu.VMEM((tokens, 2 * channels), f32),
            pltpu.VMEM((tokens, hidden), f32), pltpu.VMEM((tokens, 128), f32), pltpu.VMEM((tokens, 2 * hidden), bf16),
            pltpu.VMEM((tokens, SIDE * span), f32), halves, halves, near, near, pltpu.VMEM((2, 2, tokens // 2, span), f32),
            packs, packs, pltpu.VMEM((2, 2, tokens // 4, span), f32), pltpu.VMEM((tokens, channels), f32),
            dma((14,)), pltpu.SemaphoreType.REGULAR((3,)), dma((5,)), dma((5, 8)),
            dma((1,)), dma((1,)), dma((3,)), dma((3,)), dma((2, 3)), dma((2, 6)),
        ],
        name="layer",
        compiler_params=pltpu.CompilerParams(
            vmem_limit_bytes=58 * 2**20, collective_id=0, has_side_effects=True
        ),
    )(
        resid, mixer_in, log_step.T, decay_real, frequency,
        input_matrix.transpose(0, 1, 3, 2).reshape(2, channels, states), output_matrix.reshape(2, channels, states),
        skip_gain.reshape(1, -1), norm_gain.reshape(1, -1), value_weight, gate_weight, up_weight, down_weight,
    )


def solution(mesh):
    in_specs = (
        P("sp", "tp"), P("sp", "tp"), P("sp", "tp"), P("tp", None), P("tp", None),
        P(None, "tp", None, None), P(None, "tp", None, None), P("tp"),
        P(None, "tp"), P(None, "tp"), P(), P("sp", "tp"), P("sp", "tp"),
    )
    return jax.shard_map(
        per_device, mesh=mesh, in_specs=in_specs, out_specs=P("sp", "tp"), check_vma=False
    )
```

```python
import functools
import math

import jax
import jax.numpy as jnp
from jax import lax
from jax.experimental import pallas as pl
from jax.experimental.pallas import tpu as pltpu
from jax.sharding import PartitionSpec as P

rms_eps = 1e-06
f32 = jnp.float32
bf16 = jnp.bfloat16
CHUNKS = 8


def onehot(shape, test):
    row = lax.broadcasted_iota(jnp.int32, shape, 0)
    col = lax.broadcasted_iota(jnp.int32, shape, 1)
    return jnp.where(test(row, col), 1.0, 0.0).astype(bf16)


def split3(x):
    hi = x.astype(bf16)
    rest = x - hi.astype(f32)
    mid = rest.astype(bf16)
    return hi, mid, (rest - mid.astype(f32)).astype(bf16)


def dot(a, b):
    return jnp.dot(a, b, preferred_element_type=f32)


def dot_t(a, b):
    return lax.dot_general(a, b, (((1,), (1,)), ((), ())), preferred_element_type=f32)


def spread_row(x, states):
    groups = x.shape[0]
    width = groups * states
    lanes = onehot((states, width), lambda r, c: r == c % states)
    wide = sum(dot(part, lanes) for part in split3(x))
    row = lax.broadcasted_iota(jnp.int32, wide.shape, 0)
    col = lax.broadcasted_iota(jnp.int32, wide.shape, 1)
    return jnp.sum(jnp.where(row == col // states, wide, 0.0), axis=0, keepdims=True)


def prepare(u_ref, ls_ref, dr_ref, fr_ref, bm_ref, cm_ref, uperm, step_wide, proj_re, proj_im, rows, wout):
    tokens, channels = u_ref.shape
    groups, states = dr_ref.shape
    width = groups * states
    per_group = channels // groups
    span = tokens // CHUNKS
    perm = onehot((tokens, tokens), lambda r, c: c == (r % CHUNKS) * span + r // CHUNKS)
    u_sorted = dot(perm, u_ref[...]).astype(bf16)
    uperm[...] = u_sorted
    decay = spread_row(dr_ref[...], states)
    angular = spread_row(fr_ref[...], states)
    rows[0:1, :] = -decay
    rows[1:2, :] = 0.5 * angular
    modulus = decay * decay + angular * angular
    inv_re = -decay / modulus
    inv_im = -angular / modulus
    step = jnp.exp(ls_ref[...])
    step = sum(dot_t(perm, part) for part in split3(step))
    group_lanes = onehot((groups, width), lambda r, c: r == c // states)
    step_wide[...] = sum(dot(part, group_lanes) for part in split3(step))
    state_lanes = onehot((states, width), lambda r, c: r == c % states)
    row = lax.broadcasted_iota(jnp.int32, (channels, width), 0)
    col = lax.broadcasted_iota(jnp.int32, (channels, width), 1)
    same = row // per_group == col // states
    b_re = dot(bm_ref[0].astype(bf16), state_lanes)
    b_im = dot(bm_ref[1].astype(bf16), state_lanes)
    w_re = jnp.where(same, b_re * inv_re - b_im * inv_im, 0.0).astype(bf16)
    w_im = jnp.where(same, b_re * inv_im + b_im * inv_re, 0.0).astype(bf16)
    proj_re[...] = dot(u_sorted, w_re)
    proj_im[...] = dot(u_sorted, w_im)
    wout[:, :width] = jnp.where(same, dot(cm_ref[0].astype(bf16), state_lanes), 0.0).astype(bf16)
    wout[:, width:] = jnp.where(same, -dot(cm_ref[1].astype(bf16), state_lanes), 0.0).astype(bf16)


SIN = (-1.0 / 6, 1.0 / 120, -1.0 / 5040, 1.0 / 362880, -1.0 / 39916800)
COS = (-0.5, 1.0 / 24, -1.0 / 720, 1.0 / 40320, -1.0 / 3628800)


def series(q, terms):
    total = terms[-1] * q
    for term in terms[-2::-1]:
        total = (total + term) * q
    return total


def first_pass(step_wide, proj_re, proj_im, rows, dec_re, dec_im, ends, first, last):
    tokens, width = step_wide.shape
    block = 256

    def one_block(b, _):
        lanes = pl.ds(pl.multiple_of(b * block, block), block)
        minus_decay = jnp.broadcast_to(rows[0:1, lanes], (CHUNKS, block))
        half_angular = jnp.broadcast_to(rows[1:2, lanes], (CHUNKS, block))

        def one_step(i, carry):
            a_re, a_im, x_re, x_im = carry
            at = pl.ds(pl.multiple_of(i * CHUNKS, CHUNKS), CHUNKS)
            step = step_wide[at, lanes]
            half = step * half_angular
            q = half * half
            sine = half + half * series(q, SIN)
            cosine = 1.0 + series(q, COS)
            factor = jnp.exp(step * minus_decay)
            twice = factor * (sine + sine)
            d_re = factor - twice * sine
            d_im = twice * cosine
            less = d_re - 1.0
            p_re = proj_re[at, lanes]
            p_im = proj_im[at, lanes]
            u_re = less * p_re - d_im * p_im
            u_im = less * p_im + d_im * p_re
            dec_re[at, lanes] = d_re
            dec_im[at, lanes] = d_im
            proj_re[at, lanes] = u_re
            proj_im[at, lanes] = u_im
            return (
                d_re * a_re - d_im * a_im,
                d_re * a_im + d_im * a_re,
                d_re * x_re - d_im * x_im + u_re,
                d_re * x_im + d_im * x_re + u_im,
            )

        zero = jnp.zeros((CHUNKS, block), f32)
        found = lax.fori_loop(0, tokens // CHUNKS, one_step, (zero + 1.0, zero, zero, zero), unroll=2)
        for k in range(4):
            ends[k, :, lanes] = found[k]
        return 0

    lax.fori_loop(first, last, one_block, 0)


def chain(early, late):
    return (
        early[0] * late[0] - early[1] * late[1],
        early[0] * late[1] + early[1] * late[0],
        late[0] * early[2] - late[1] * early[3] + late[2],
        late[0] * early[3] + late[1] * early[2] + late[3],
    )


def chunk_prefix(ends, total):
    width = ends.shape[2]
    value = tuple(ends[k] for k in range(4))
    row = lax.broadcasted_iota(jnp.int32, value[0].shape, 0)
    unit = (1.0, 0.0, 0.0, 0.0)

    def moved(value, by):
        return tuple(
            jnp.where(row >= by, pltpu.roll(part, by, 0), zero) for part, zero in zip(value, unit)
        )

    for by in (1, 2, 4):
        value = chain(moved(value, by), value)
    for k in range(4):
        for j in range(width // 128):
            total[8 * k + j : 8 * k + j + 1, :] = value[k][CHUNKS - 1 :, 128 * j : 128 * j + 128]
    before = moved(value, 1)
    for k in range(4):
        ends[k] = before[k]


def second_pass(dec_re, dec_im, feed_re, feed_im, ends, carry, states):
    tokens, width = dec_re.shape
    block = 512
    for b in range(width // block):
        lanes = pl.ds(b * block, block)
        lanes_im = pl.ds(width + b * block, block)
        per = block // 128
        h_re = jnp.concatenate([carry[per * b + j : per * b + j + 1, :] for j in range(per)], axis=1)
        h_im = jnp.concatenate([carry[8 + per * b + j : 9 + per * b + j, :] for j in range(per)], axis=1)
        a_re, a_im = ends[0, :, lanes], ends[1, :, lanes]
        x_re = ends[2, :, lanes] + a_re * h_re - a_im * h_im
        x_im = ends[3, :, lanes] + a_re * h_im + a_im * h_re

        def one_step(i, value):
            x_re, x_im = value
            seen = []
            for k in range(2):
                at = pl.ds(pl.multiple_of(i * 2 * CHUNKS + k * CHUNKS, CHUNKS), CHUNKS)
                d_re, d_im = dec_re[at, lanes], dec_im[at, lanes]
                x_re, x_im = (
                    d_re * x_re - d_im * x_im + feed_re[at, lanes],
                    d_re * x_im + d_im * x_re + feed_im[at, lanes],
                )
                seen.append((x_re, x_im))
            both = pl.ds(pl.multiple_of(i * 2 * CHUNKS, 2 * CHUNKS), 2 * CHUNKS)
            states[both, lanes] = jnp.concatenate([seen[0][0], seen[1][0]], axis=0).astype(bf16)
            states[both, lanes_im] = jnp.concatenate([seen[0][1], seen[1][1]], axis=0).astype(bf16)
            return x_re, x_im

        lax.fori_loop(0, tokens // (2 * CHUNKS), one_step, (x_re, x_im), unroll=2)


def read_out(states, wout, uperm, skip_ref):
    tokens = states.shape[0]
    span = tokens // CHUNKS
    out = dot_t(states[...], wout[...]) + skip_ref[...] * uperm[...].astype(f32)
    mixed = jax.nn.gelu(out).astype(bf16)
    back = onehot((tokens, tokens), lambda r, c: r == (c % CHUNKS) * span + c // CHUNKS)
    return dot(back, mixed).astype(bf16)


AXES = pl.DeviceIdType.MESH
SIDE = 4


def around(index, by):
    return lax.rem(index + by + SIDE, SIDE)


class Relay:
    def __init__(self, buf, first, rows, send_sem, recv_sem, own=None):
        here = lax.axis_index("sp")
        self.zy = here // SIDE, lax.rem(here, SIDE)
        self.buf, self.first, self.rows, self.own = buf, first, rows, own
        self.shard = buf.shape[0] // (SIDE * SIDE)
        self.send_sem, self.recv_sem = send_sem, recv_sem
        self.sent = 0

    def index(self, side, dp, dq):
        dz, dy = (dq, dp) if side == 0 else (dp, dq)
        return around(self.zy[0], dz) * SIDE + around(self.zy[1], dy)

    def group(self, dp, dq, half):
        if dq == 0:
            return 2 if dp == 2 else int((dp == -1) == (half == 1))
        return 3 + dp % SIDE if dq != 2 and (dq == -1) == (half == 0) else 7

    def send(self, side, dp, dq, half, to_p, to_q):
        width = self.buf.shape[1] // 2
        cols = slice(half * width, half * width + width)
        row = pl.multiple_of(self.index(side, dp, dq) * self.shard + side * self.rows, self.rows)
        piece = self.buf.at[pl.ds(row, self.rows), cols]
        own = self.own is not None and dp == 0 and dq == 0
        first = self.first + side * self.rows
        seen = [(d + 1) % SIDE - 1 for d in (dp - to_p, dq - to_q)]
        pltpu.make_async_remote_copy(
            src_ref=self.own.at[first : first + self.rows, cols] if own else piece,
            dst_ref=piece,
            send_sem=self.send_sem,
            recv_sem=self.recv_sem.at[self.group(*seen, half)],
            device_id={"sp": self.index(side, to_p, to_q), "tp": lax.axis_index("tp")},
            device_id_type=AXES,
        ).start()
        self.sent += 1

    def whole(self, count, group):
        rows = self.buf.at[: count * self.rows // 2, :]
        return pltpu.make_async_remote_copy(
            src_ref=rows,
            dst_ref=rows,
            send_sem=self.send_sem,
            recv_sem=self.recv_sem.at[group],
            device_id={"sp": self.index(0, 1, 0), "tp": lax.axis_index("tp")},
            device_id_type=AXES,
        )

    def arrived(self, group):
        self.whole(32 if group == 7 else 4, group).wait_recv()

    def send_p(self, k):
        for side in range(2):
            self.send(side, 0, 0, k, 1, 0)
            self.send(side, 0, 0, 1 - k, -1, 0)

    def send_q(self, dp, k):
        for side in range(2):
            self.send(side, dp, 0, k, 0, 1)
            self.send(side, dp, 0, 1 - k, 0, -1)

    def forward_p(self):
        self.arrived(0)
        for side in range(2):
            self.send(side, -1, 0, 0, 1, 0)
            self.send(side, 1, 0, 1, -1, 0)

    def near(self):
        self.arrived(1)
        self.send_q(-1, 0)
        self.send_q(1, 0)

    def near_rest(self):
        self.send_q(-1, 1)
        self.send_q(1, 1)

    def far(self):
        self.arrived(2)
        self.send_q(2, 0)

    def far_rest(self):
        self.send_q(2, 1)

    def forward_q(self, dp):
        self.arrived(3 + dp % SIDE)
        for side in range(2):
            self.send(side, dp, -1, 0, 0, 1)
            self.send(side, dp, 1, 1, 0, -1)

    def finish(self):
        self.arrived(7)

    def drain(self):
        self.whole(self.sent, 0).wait_send()


class Gather:
    def __init__(self, buf, send_sem, recv_sem):
        here = lax.axis_index("tp")
        self.x, self.core = here // 2, lax.rem(here, 2)
        self.buf, self.send_sem, self.recv_sem = buf, send_sem, recv_sem
        self.sent = 0

    def device(self, dx, other=False):
        return around(self.x, dx) * 2 + (1 - self.core if other else self.core)

    def cols(self, core):
        width = self.buf.shape[2] // 2
        return pl.ds(pl.multiple_of(core * width, width), width)

    def send(self, dx, half, to_x):
        rows = self.buf.shape[1] // 2
        piece = self.buf.at[around(self.x, dx), half * rows : half * rows + rows, self.cols(self.core)]
        if to_x:
            seen = (dx - to_x + 1) % SIDE - 1
            group = 2 if seen == 2 else int((seen == -1) == (half == 1))
        else:
            group = 3 + dx % SIDE
        pltpu.make_async_remote_copy(
            src_ref=piece,
            dst_ref=piece,
            send_sem=self.send_sem,
            recv_sem=self.recv_sem.at[group],
            device_id={"sp": lax.axis_index("sp"), "tp": self.device(to_x, not to_x)},
            device_id_type=AXES,
        ).start()
        self.sent += 1

    def whole(self, rows, group):
        return pltpu.make_async_remote_copy(
            src_ref=rows,
            dst_ref=rows,
            send_sem=self.send_sem,
            recv_sem=self.recv_sem.at[group],
            device_id={"sp": lax.axis_index("sp"), "tp": self.device(1)},
            device_id_type=AXES,
        )

    def arrived(self, group):
        self.whole(self.buf.at[0, :, : self.buf.shape[2] // 2], group).wait_recv()

    def start(self):
        for k in range(2):
            self.send(0, k, 1)
            self.send(0, 1 - k, -1)
        for k in range(2):
            self.send(0, k, 0)

    def near(self):
        self.arrived(0)
        self.send(-1, 0, 1)
        self.send(1, 1, -1)
        self.send(-1, 0, 0)
        self.send(1, 1, 0)
        self.arrived(1)
        self.send(-1, 1, 0)
        self.send(1, 0, 0)

    def far(self):
        self.arrived(2)
        self.send(2, 0, 0)
        self.send(2, 1, 0)

    def across(self, dx):
        self.arrived(3 + dx % SIDE)

    def drain(self):
        self.whole(self.buf.at[:, : self.buf.shape[1] * self.sent // 16, :], 0).wait_send()


class Phases:
    def __init__(self):
        self.scope = None

    def __call__(self, name):
        if self.scope is not None:
            self.scope.__exit__(None, None, None)
        self.scope = jax.named_scope(name) if name else None
        if self.scope is not None:
            self.scope.__enter__()


def layer_kernel(
    resid_hbm, u_hbm, ls_hbm, dr_hbm, fr_hbm, bm_hbm, cm_hbm, skip_hbm, gain_hbm, vw_ref, gw_ref, up_ref, down_ref,
    out_ref,
    resid_ref, u_ref, ls_ref, dr_ref, fr_ref, bm_ref, cm_ref, skip_ref, gain_ref,
    up_all, down_first, down_last, vg, dec_re, dec_im, feed_re, feed_im, step_wide, rows, ends, total, totals, carry,
    uperm, wout, states, mixed_all, upd_all, glu, raised, squares, hidden,
    products, stage_far, relay_in, stage_near, from_near, kept, stage_own, from_own, own_part, kept_out,
    local_sem, round_sem, ring_send, ring_recv, tot_send, tot_recv, cross_send, cross_recv, sum_send, sum_recv,
):
    phase = Phases()
    here, lane = lax.axis_index("sp"), lax.axis_index("tp")
    planes = SIDE * SIDE
    tokens, piece = resid_ref.shape
    half = tokens // 2
    shard = up_ref.shape[0]
    mix = Gather(mixed_all, ring_send.at[3], ring_recv.at[3])
    upd = Gather(upd_all, ring_send.at[4], ring_recv.at[4])
    right, left, partner = mix.device(1), mix.device(-1), mix.device(0, True)

    up = Relay(up_all, 0, shard // 2, ring_send.at[0], ring_recv.at[0], up_ref)
    first = Relay(down_first, 0, shard // 8, ring_send.at[1], ring_recv.at[1])
    last = Relay(down_last, 0, shard // 8, ring_send.at[2], ring_recv.at[2])
    near_planes = [up.index(0, *by) for by in ((1, 0), (-1, 0), (0, 1), (0, -1))]

    phase("signal")
    barrier = pltpu.get_barrier_semaphore()
    for target in near_planes:
        pl.semaphore_signal(barrier, inc=1, device_id={"sp": target, "tp": lane}, device_id_type=AXES)
    for target in (right, left, partner):
        pl.semaphore_signal(barrier, inc=1, device_id={"sp": here, "tp": target}, device_id_type=AXES)

    own_up = pl.ds(pl.multiple_of(here * shard, shard), shard)
    slim, width = shard // 4, up_ref.shape[1]
    own_down = pl.ds(pl.multiple_of(here * slim, slim), slim)
    own_units = pl.ds(pl.multiple_of(mix.core * width, width), width)

    def down_rows(core, k):
        return down_ref.at[pl.ds(pl.multiple_of(core * 2 * slim + k * slim, slim), slim), :]

    def cross_copy(number, src, dst):
        return pltpu.make_async_remote_copy(
            src_ref=src,
            dst_ref=dst,
            send_sem=cross_send.at[number],
            recv_sem=cross_recv.at[number],
            device_id={"sp": here, "tp": partner},
            device_id_type=AXES,
        )

    crossing = [
        cross_copy(k, down_rows(1 - mix.core, k), buf.at[own_down, own_units])
        for k, buf in enumerate((down_first, down_last))
    ]
    moves = (
        (u_hbm, u_ref), (dr_hbm, dr_ref), (fr_hbm, fr_ref), (ls_hbm, ls_ref), (bm_hbm, bm_ref), (cm_hbm, cm_ref),
        (up_ref, up_all.at[own_up, :]),
        (down_rows(mix.core, 0), down_first.at[own_down, own_units]),
        (down_rows(mix.core, 1), down_last.at[own_down, own_units]),
        (skip_hbm, skip_ref), (vw_ref, vg.at[:, :piece]), (gw_ref, vg.at[:, piece:]),
        (resid_hbm, resid_ref), (gain_hbm, gain_ref),
    )
    local = [pltpu.make_async_copy(src, dst, local_sem.at[k]) for k, (src, dst) in enumerate(moves)]
    for copy in local:
        copy.start()
    phase("barrier")
    pl.semaphore_wait(barrier, 7)
    phase("start_p")
    up.send_p(0)
    up.send_p(1)
    up.send_q(0, 0)
    up.send_q(0, 1)
    for copy in crossing:
        copy.start()

    def greet(number):
        for target in near_planes:
            pl.semaphore_signal(
                round_sem.at[number], inc=1, device_id={"sp": target, "tp": lane}, device_id_type=AXES
            )

    greet(0)
    for copy in local[:6]:
        copy.wait()
    phase("prepare")
    prepare(u_ref, ls_ref, dr_ref, fr_ref, bm_ref, cm_ref, uperm, step_wide, feed_re, feed_im, rows, wout)
    pl.semaphore_wait(round_sem.at[0], 4)
    greet(1)
    phase("first_pass")
    scan_refs = (step_wide, feed_re, feed_im, rows, dec_re, dec_im, ends)
    first_pass(*scan_refs, 0, 2)
    pl.semaphore_wait(round_sem.at[1], 4)
    greet(2)
    for copy in local[6:9]:
        copy.wait()
    for copy in crossing:
        copy.wait_recv()
    first.send_p(0)
    first_pass(*scan_refs, 2, 4)
    phase("chunk")
    chunk_prefix(ends, total)
    pl.semaphore_wait(round_sem.at[2], 4)

    def total_copy(src, dst, target):
        return pltpu.make_async_remote_copy(
            src_ref=src,
            dst_ref=dst,
            send_sem=tot_send.at[0],
            recv_sem=tot_recv.at[0],
            device_id={"sp": target, "tp": lane},
            device_id_type=AXES,
        )

    phase("totals")
    for by in range(1, planes):
        @pl.when(here + by < planes)
        def _():
            total_copy(total, totals.at[here], lax.rem(here + by, planes)).start()

    phase("serve1")
    up.forward_p()
    up.near()
    up.forward_q(0)
    up.near_rest()

    phase("fold")

    for count in range(1, planes):
        @pl.when(here == count)
        def _():
            total_copy(totals.at[:count], totals.at[:count], lax.rem(here + 1, planes)).wait_recv()

    def fold(j, value):
        h_re, h_im = value
        a_re, a_im = totals[j, 0:8, :], totals[j, 8:16, :]
        x_re, x_im = totals[j, 16:24, :], totals[j, 24:32, :]
        return a_re * h_re - a_im * h_im + x_re, a_re * h_im + a_im * h_re + x_im

    zero = jnp.zeros((8, 128), f32)
    h_re, h_im = lax.fori_loop(0, here, fold, (zero, zero))
    carry[0:8, :] = h_re
    carry[8:16, :] = h_im
    phase("second_pass")
    second_pass(dec_re, dec_im, feed_re, feed_im, ends, carry, states)
    phase("serve2")
    up.far()
    up.far_rest()
    first.send_p(1)
    local[9].wait()
    phase("read_out")
    own_cols = mix.cols(mix.core)
    mixed_all[mix.x, :, own_cols] = read_out(states, wout, uperm, skip_ref)
    phase("mix_start")
    mix.start()

    depth = 2 * piece

    def glu_part(chip, core=None):
        if core is None:
            lhs, at = mixed_all[chip], pl.ds(pl.multiple_of(chip * depth, depth), depth)
        else:
            lhs, at = mixed_all[chip, :, mix.cols(core)], pl.ds(pl.multiple_of((chip * 2 + core) * piece, piece), piece)
        return dot(lhs, vg[at, :])

    phase("mix_own")
    for copy in local[10:]:
        copy.wait()
    mix.across(0)
    glu[...] = glu_part(mix.x)
    phase("serve3")
    up.forward_q(-1)
    up.forward_q(1)
    first.send_q(0, 0)
    first.send_q(0, 1)
    phase("mix_near")
    mix.near()
    phase("serve4")
    up.forward_q(2)
    phase("mix_left")
    mix.across(-1)
    glu[...] += glu_part(around(mix.x, -1))
    phase("mix_right")
    mix.across(1)
    glu[...] += glu_part(around(mix.x, 1))
    phase("mix_far")
    mix.far()
    phase("mix_last")
    far_chip = around(mix.x, 2)
    glu[...] += glu_part(far_chip, mix.core)
    mix.across(2)
    glu[...] += glu_part(far_chip, 1 - mix.core)
    phase("updated")
    updated = (resid_ref[...].astype(f32) + glu[:, :piece] * jax.nn.sigmoid(glu[:, piece:])).astype(bf16)
    upd_all[upd.x, :, own_cols] = updated
    phase("upd_start")
    upd.start()
    phase("serve5")
    first.forward_p()
    first.near()
    first.near_rest()
    last.send_p(0)
    last.send_p(1)

    def up_part(chip, start, core=None):
        if core is None:
            wide, at = upd_all[chip], pl.ds(pl.multiple_of(chip * depth, depth), depth)
        else:
            wide, at = upd_all[chip, :, upd.cols(core)], pl.ds(pl.multiple_of((chip * 2 + core) * piece, piece), piece)
        wide = wide.astype(f32)
        square = wide * wide
        square = sum(square[:, 128 * k : 128 * k + 128] for k in range(square.shape[1] // 128))
        product = dot((wide * gain_ref[:, at]).astype(bf16), up_all[at, :])
        if start:
            squares[...] = square
            raised[...] = product
        else:
            squares[...] += square
            raised[...] += product

    phase("up_wait")
    up.finish()
    phase("upd_own")
    upd.across(0)
    up_part(upd.x, True)
    phase("serve6")
    first.forward_q(0)
    first.far()
    last.send_q(0, 0)
    first.far_rest()
    last.send_q(0, 1)
    phase("upd_near")
    upd.near()
    phase("upd_left")
    upd.across(-1)
    last.forward_p()
    up_part(around(upd.x, -1), False)
    phase("serve7")
    first.forward_q(-1)
    first.forward_q(1)
    phase("upd_right")
    upd.across(1)
    up_part(around(upd.x, 1), False)
    phase("serve8")
    first.forward_q(2)
    last.near()
    phase("upd_far")
    upd.far()
    up_part(far_chip, False, upd.core)
    phase("upd_last")
    upd.across(2)
    up_part(far_chip, False, 1 - upd.core)
    phase("hidden")
    inv_rms = lax.rsqrt(jnp.sum(squares[...], axis=1, keepdims=True) / (SIDE * depth) + rms_eps)
    active = jnp.maximum(raised[...] * inv_rms, 0.0)
    hidden[:, own_units] = (active * active).astype(bf16)
    crossing.append(cross_copy(2, hidden.at[:, own_units], hidden.at[:, own_units]))
    crossing[2].start()
    phase("serve9")
    last.far()
    last.forward_q(0)
    last.near_rest()
    last.far_rest()

    span = piece // 2
    quarter = half // 2

    chunk = quarter // 2

    def turned(value, by=None):
        return pltpu.roll(value, span // 2 if by is None else by, 1)

    low_lanes = lax.broadcasted_iota(jnp.int32, (chunk, span), 1) < span // 2

    def packed(value, core):
        parts = []
        for c in range(value.shape[0] // quarter):
            top, low = (value[c * quarter + k * chunk : c * quarter + k * chunk + chunk] for k in range(2))
            parts.append(jnp.where(low_lanes, top, turned(low)) if core == 0 else jnp.where(low_lanes, turned(top), low))
        return jnp.concatenate(parts, axis=0)

    class Sum:
        def __init__(self, k, buf):
            self.k, self.buf = k, buf
            self.relays = [
                [
                    self.copy(
                        0, 2 * j + c, stage_far.at[k, j, c * quarter : c * quarter + quarter],
                        relay_in.at[k, j, c * quarter : c * quarter + quarter], target,
                    )
                    for c in range(2)
                ]
                for j, target in enumerate((right, left))
            ]
            self.own = self.copy(1, 4, stage_own.at[k], from_own.at[k], partner)
            self.near = self.copy(2, 5, stage_near.at[k], from_near.at[k], right)

        def copy(self, send, recv, src, dst, target):
            return pltpu.make_async_remote_copy(
                src_ref=src,
                dst_ref=dst,
                send_sem=sum_send.at[self.k, send],
                recv_sem=sum_recv.at[self.k, recv],
                device_id={"sp": here, "tp": target},
                device_id_type=AXES,
            )

        def product(self, dx):
            return products[:, pl.ds(pl.multiple_of(around(mix.x, dx) * span, span), span)]

        def send_near(self, side, part, value, first=0):
            chip = around(mix.x, 1 - 2 * side)
            rows = slice(first, first + value.shape[0] // 2)
            for core in range(2):
                stage_near[self.k, side, core, part, rows] = packed(value, core).astype(bf16)
                self.copy(
                    2, 5, stage_near.at[self.k, side, core, part, rows],
                    from_near.at[self.k, mix.core, side, part, rows], chip * 2 + core,
                ).start()

        def start(self, *serve):
            k = self.k
            products[...] = dot_t(hidden[...], self.buf[...])
            far = self.product(2).astype(bf16)
            for j in range(2):
                stage_far[k, j] = far[j * half : j * half + half]
            for c in range(2):
                for j in range(2):
                    self.relays[j][c].start()
            near = self.product(1)
            self.send_near(0, 1, near[half:])
            kept[k, 0] = near[:half]
            near = self.product(-1)
            self.send_near(1, 0, near[:half])
            kept[k, 1] = near[half:]
            if serve:
                serve[0]()
            own = self.product(0)
            for j in range(2):
                both = [packed(own[j * half : j * half + half], core) for core in range(2)]
                own_part[k, j] = jnp.where(mix.core == 0, both[0], both[1])
                stage_own[k, j] = jnp.where(mix.core == 0, both[1], both[0]).astype(bf16)
            self.own.start()
            if serve:
                serve[1]()

        def relay(self):
            k = self.k
            for c in range(2):
                rows = slice(c * quarter, c * quarter + quarter)
                for j in range(2):
                    self.relays[j][c].wait_recv()
                    self.send_near(j, j, kept[k, j, rows] + relay_in[k, j, rows].astype(f32), c * chunk)

        def result(self):
            k = self.k
            self.own.wait_recv()
            self.near.wait_recv()
            found = []
            for core in range(2):
                rows = []
                for j in range(2):
                    here_part = jnp.where(mix.core == core, own_part[k, j], from_own[k, j].astype(f32))
                    total = here_part + (from_near[k, core, 0, j].astype(f32) + from_near[k, core, 1, j].astype(f32))
                    for c in range(2):
                        part = total[c * chunk : c * chunk + chunk]
                        rows += [part, turned(part)]
                found.append(jnp.concatenate(rows, axis=0))
            return found

        def drain(self):
            self.own.wait_send()
            self.near.wait_send()
            self.copy(0, 0, stage_far.at[self.k], stage_far.at[self.k], right).wait_send()

    phase("first_wait")
    first.finish()
    crossing[2].wait_recv()
    phase("first_sum")
    early, late = Sum(0, down_first), Sum(1, down_last)

    def serve_near():
        last.forward_q(-1)
        last.forward_q(1)

    def serve_far():
        last.forward_q(2)

    early.start(serve_near, serve_far)
    phase("first_relay")
    early.relay()
    phase("last_wait")
    last.finish()
    phase("last_sum")
    late.start()
    phase("last_relay")
    late.relay()
    phase("first_result")
    lane_group = lax.broadcasted_iota(jnp.int32, (tokens, span), 1) // slim
    blocks = [upd_all[upd.x, :, own_cols].astype(f32)[:, b * span : b * span + span] for b in range(2)]

    def put_in(k, found):
        for b in range(2):
            for core in range(2):
                place = core * 2 + k
                moved = turned(found[core], (place - b) % 4 * slim) if place != b else found[core]
                blocks[b] = blocks[b] + jnp.where(lane_group == place, moved, 0.0)

    put_in(0, early.result())
    for b in range(2):
        kept_out[:, b * span : b * span + span] = blocks[b]
    phase("last_result")
    two = late.result()
    phase("result")
    blocks = [kept_out[:, b * span : b * span + span] for b in range(2)]
    put_in(1, two)
    out_ref[...] = jnp.concatenate(blocks, axis=1).astype(bf16)

    phase("drain")
    for count in range(1, planes):
        @pl.when(planes - 1 - here == count)
        def _():
            total_copy(totals.at[:count], totals.at[:count], lax.rem(here + 1, planes)).wait_send()

    for part in (up, first, last, mix, upd, early, late):
        part.drain()
    for copy in crossing:
        copy.wait_send()
    phase(None)


def per_device(
    resid, mixer_in, log_step, decay_real, frequency, input_matrix, output_matrix, skip_gain,
    value_weight, gate_weight, norm_gain, up_weight, down_weight,
):
    tokens, channels = mixer_in.shape
    groups, states = decay_real.shape
    width = groups * states
    planes, slots = lax.axis_size("sp"), lax.axis_size("tp")
    features = slots * channels
    hidden = up_weight.shape[1]
    span = channels // 2
    vmem = pl.BlockSpec(memory_space=pltpu.VMEM)
    hbm = pl.BlockSpec(memory_space=pl.ANY)
    wide = pltpu.VMEM((tokens, width), f32)
    block = pltpu.VMEM((tokens, channels), bf16)
    halves = pltpu.VMEM((2, 2, tokens // 2, span), bf16)
    packs = pltpu.VMEM((2, 2, tokens // 4, span), bf16)
    near = pltpu.VMEM((2, 2, 2, 2, tokens // 4, span), bf16)
    pieces = pltpu.VMEM((SIDE, tokens, 2 * channels), bf16)
    matrix = pltpu.VMEM((2, channels, states), f32)
    down = pltpu.VMEM((features // 4, 2 * hidden), bf16)
    dma = pltpu.SemaphoreType.DMA
    return pl.pallas_call(
        layer_kernel,
        out_shape=jax.ShapeDtypeStruct((tokens, channels), bf16),
        in_specs=[hbm] * 13,
        out_specs=vmem,
        scratch_shapes=[
            block, block, pltpu.VMEM((groups, tokens), f32),
            pltpu.VMEM((groups, states), f32), pltpu.VMEM((groups, states), f32), matrix, matrix,
            pltpu.VMEM((1, channels), f32), pltpu.VMEM((1, features), f32),
            pltpu.VMEM((features, hidden), bf16), down, down, pltpu.VMEM((features, 2 * channels), bf16),
            wide, wide, wide, wide, wide,
            pltpu.VMEM((8, width), f32), pltpu.VMEM((4, CHUNKS, width), f32),
            pltpu.VMEM((32, 128), f32), pltpu.VMEM((planes, 32, 128), f32), pltpu.VMEM((16, 128), f32),
            block, pltpu.VMEM((channels, 2 * width), bf16), pltpu.VMEM((tokens, 2 * width), bf16),
            pieces, pieces, pltpu.VMEM((tokens, 2 * channels), f32),
            pltpu.VMEM((tokens, hidden), f32), pltpu.VMEM((tokens, 128), f32), pltpu.VMEM((tokens, 2 * hidden), bf16),
            pltpu.VMEM((tokens, SIDE * span), f32), halves, halves, near, near, pltpu.VMEM((2, 2, tokens // 2, span), f32),
            packs, packs, pltpu.VMEM((2, 2, tokens // 4, span), f32), pltpu.VMEM((tokens, channels), f32),
            dma((14,)), pltpu.SemaphoreType.REGULAR((3,)), dma((5,)), dma((5, 8)),
            dma((1,)), dma((1,)), dma((3,)), dma((3,)), dma((2, 3)), dma((2, 6)),
        ],
        name="layer",
        compiler_params=pltpu.CompilerParams(
            vmem_limit_bytes=58 * 2**20, collective_id=0, has_side_effects=True
        ),
    )(
        resid, mixer_in, log_step.T, decay_real, frequency,
        input_matrix.transpose(0, 1, 3, 2).reshape(2, channels, states), output_matrix.reshape(2, channels, states),
        skip_gain.reshape(1, -1), norm_gain.reshape(1, -1), value_weight, gate_weight, up_weight, down_weight,
    )


def solution(mesh):
    in_specs = (
        P("sp", "tp"), P("sp", "tp"), P("sp", "tp"), P("tp", None), P("tp", None),
        P(None, "tp", None, None), P(None, "tp", None, None), P("tp"),
        P(None, "tp"), P(None, "tp"), P(), P("sp", "tp"), P("sp", "tp"),
    )
    return jax.shard_map(
        per_device, mesh=mesh, in_specs=in_specs, out_specs=P("sp", "tp"), check_vma=False
    )
```

```python
import functools
import math

import jax
import jax.numpy as jnp
from jax import lax
from jax.experimental import pallas as pl
from jax.experimental.pallas import tpu as pltpu
from jax.sharding import PartitionSpec as P

rms_eps = 1e-06
f32 = jnp.float32
bf16 = jnp.bfloat16
CHUNKS = 8


def onehot(shape, test):
    row = lax.broadcasted_iota(jnp.int32, shape, 0)
    col = lax.broadcasted_iota(jnp.int32, shape, 1)
    return jnp.where(test(row, col), 1.0, 0.0).astype(bf16)


def split3(x):
    hi = x.astype(bf16)
    rest = x - hi.astype(f32)
    mid = rest.astype(bf16)
    return hi, mid, (rest - mid.astype(f32)).astype(bf16)


def dot(a, b):
    return jnp.dot(a, b, preferred_element_type=f32)


def dot_t(a, b):
    return lax.dot_general(a, b, (((1,), (1,)), ((), ())), preferred_element_type=f32)


def spread_row(x, states):
    groups = x.shape[0]
    width = groups * states
    lanes = onehot((states, width), lambda r, c: r == c % states)
    wide = sum(dot(part, lanes) for part in split3(x))
    row = lax.broadcasted_iota(jnp.int32, wide.shape, 0)
    col = lax.broadcasted_iota(jnp.int32, wide.shape, 1)
    return jnp.sum(jnp.where(row == col // states, wide, 0.0), axis=0, keepdims=True)


def prepare(u_ref, ls_ref, dr_ref, fr_ref, bm_ref, cm_ref, uperm, step_wide, proj_re, proj_im, rows, wout):
    tokens, channels = u_ref.shape
    groups, states = dr_ref.shape
    width = groups * states
    per_group = channels // groups
    span = tokens // CHUNKS
    perm = onehot((tokens, tokens), lambda r, c: c == (r % CHUNKS) * span + r // CHUNKS)
    u_sorted = dot(perm, u_ref[...]).astype(bf16)
    uperm[...] = u_sorted
    decay = spread_row(dr_ref[...], states)
    angular = spread_row(fr_ref[...], states)
    rows[0:1, :] = -decay
    rows[1:2, :] = 0.5 * angular
    modulus = decay * decay + angular * angular
    inv_re = -decay / modulus
    inv_im = -angular / modulus
    step = jnp.exp(ls_ref[...])
    step = sum(dot_t(perm, part) for part in split3(step))
    group_lanes = onehot((groups, width), lambda r, c: r == c // states)
    step_wide[...] = sum(dot(part, group_lanes) for part in split3(step))
    state_lanes = onehot((states, width), lambda r, c: r == c % states)
    row = lax.broadcasted_iota(jnp.int32, (channels, width), 0)
    col = lax.broadcasted_iota(jnp.int32, (channels, width), 1)
    same = row // per_group == col // states
    b_re = dot(bm_ref[0].astype(bf16), state_lanes)
    b_im = dot(bm_ref[1].astype(bf16), state_lanes)
    w_re = jnp.where(same, b_re * inv_re - b_im * inv_im, 0.0).astype(bf16)
    w_im = jnp.where(same, b_re * inv_im + b_im * inv_re, 0.0).astype(bf16)
    proj_re[...] = dot(u_sorted, w_re)
    proj_im[...] = dot(u_sorted, w_im)
    wout[:, :width] = jnp.where(same, dot(cm_ref[0].astype(bf16), state_lanes), 0.0).astype(bf16)
    wout[:, width:] = jnp.where(same, -dot(cm_ref[1].astype(bf16), state_lanes), 0.0).astype(bf16)


SIN = (-1.0 / 6, 1.0 / 120, -1.0 / 5040, 1.0 / 362880, -1.0 / 39916800)
COS = (-0.5, 1.0 / 24, -1.0 / 720, 1.0 / 40320, -1.0 / 3628800)


def series(q, terms):
    total = terms[-1] * q
    for term in terms[-2::-1]:
        total = (total + term) * q
    return total


def first_pass(step_wide, proj_re, proj_im, rows, dec_re, dec_im, ends, first, last):
    tokens, width = step_wide.shape
    block = 256

    def one_block(b, _):
        lanes = pl.ds(pl.multiple_of(b * block, block), block)
        minus_decay = jnp.broadcast_to(rows[0:1, lanes], (CHUNKS, block))
        half_angular = jnp.broadcast_to(rows[1:2, lanes], (CHUNKS, block))

        def one_step(i, carry):
            a_re, a_im, x_re, x_im = carry
            at = pl.ds(pl.multiple_of(i * CHUNKS, CHUNKS), CHUNKS)
            step = step_wide[at, lanes]
            half = step * half_angular
            q = half * half
            sine = half + half * series(q, SIN)
            cosine = 1.0 + series(q, COS)
            factor = jnp.exp(step * minus_decay)
            twice = factor * (sine + sine)
            d_re = factor - twice * sine
            d_im = twice * cosine
            less = d_re - 1.0
            p_re = proj_re[at, lanes]
            p_im = proj_im[at, lanes]
            u_re = less * p_re - d_im * p_im
            u_im = less * p_im + d_im * p_re
            dec_re[at, lanes] = d_re
            dec_im[at, lanes] = d_im
            proj_re[at, lanes] = u_re
            proj_im[at, lanes] = u_im
            return (
                d_re * a_re - d_im * a_im,
                d_re * a_im + d_im * a_re,
                d_re * x_re - d_im * x_im + u_re,
                d_re * x_im + d_im * x_re + u_im,
            )

        zero = jnp.zeros((CHUNKS, block), f32)
        found = lax.fori_loop(0, tokens // CHUNKS, one_step, (zero + 1.0, zero, zero, zero), unroll=2)
        for k in range(4):
            ends[k, :, lanes] = found[k]
        return 0

    lax.fori_loop(first, last, one_block, 0)


def chain(early, late):
    return (
        early[0] * late[0] - early[1] * late[1],
        early[0] * late[1] + early[1] * late[0],
        late[0] * early[2] - late[1] * early[3] + late[2],
        late[0] * early[3] + late[1] * early[2] + late[3],
    )


def chunk_prefix(ends, total):
    width = ends.shape[2]
    value = tuple(ends[k] for k in range(4))
    row = lax.broadcasted_iota(jnp.int32, value[0].shape, 0)
    unit = (1.0, 0.0, 0.0, 0.0)

    def moved(value, by):
        return tuple(
            jnp.where(row >= by, pltpu.roll(part, by, 0), zero) for part, zero in zip(value, unit)
        )

    for by in (1, 2, 4):
        value = chain(moved(value, by), value)
    for k in range(4):
        for j in range(width // 128):
            total[8 * k + j : 8 * k + j + 1, :] = value[k][CHUNKS - 1 :, 128 * j : 128 * j + 128]
    before = moved(value, 1)
    for k in range(4):
        ends[k] = before[k]


def second_pass(dec_re, dec_im, feed_re, feed_im, ends, carry, states):
    tokens, width = dec_re.shape
    block = 512
    for b in range(width // block):
        lanes = pl.ds(b * block, block)
        lanes_im = pl.ds(width + b * block, block)
        per = block // 128
        h_re = jnp.concatenate([carry[per * b + j : per * b + j + 1, :] for j in range(per)], axis=1)
        h_im = jnp.concatenate([carry[8 + per * b + j : 9 + per * b + j, :] for j in range(per)], axis=1)
        a_re, a_im = ends[0, :, lanes], ends[1, :, lanes]
        x_re = ends[2, :, lanes] + a_re * h_re - a_im * h_im
        x_im = ends[3, :, lanes] + a_re * h_im + a_im * h_re

        def one_step(i, value):
            x_re, x_im = value
            seen = []
            for k in range(2):
                at = pl.ds(pl.multiple_of(i * 2 * CHUNKS + k * CHUNKS, CHUNKS), CHUNKS)
                d_re, d_im = dec_re[at, lanes], dec_im[at, lanes]
                x_re, x_im = (
                    d_re * x_re - d_im * x_im + feed_re[at, lanes],
                    d_re * x_im + d_im * x_re + feed_im[at, lanes],
                )
                seen.append((x_re, x_im))
            both = pl.ds(pl.multiple_of(i * 2 * CHUNKS, 2 * CHUNKS), 2 * CHUNKS)
            states[both, lanes] = jnp.concatenate([seen[0][0], seen[1][0]], axis=0).astype(bf16)
            states[both, lanes_im] = jnp.concatenate([seen[0][1], seen[1][1]], axis=0).astype(bf16)
            return x_re, x_im

        lax.fori_loop(0, tokens // (2 * CHUNKS), one_step, (x_re, x_im), unroll=2)


def read_out(states, wout, uperm, skip_ref):
    tokens = states.shape[0]
    span = tokens // CHUNKS
    out = dot_t(states[...], wout[...]) + skip_ref[...] * uperm[...].astype(f32)
    mixed = jax.nn.gelu(out).astype(bf16)
    back = onehot((tokens, tokens), lambda r, c: r == (c % CHUNKS) * span + c // CHUNKS)
    return dot(back, mixed).astype(bf16)


AXES = pl.DeviceIdType.MESH
SIDE = 4


def around(index, by):
    return lax.rem(index + by + SIDE, SIDE)


class Relay:
    def __init__(self, buf, first, rows, send_sem, recv_sem, own=None):
        here = lax.axis_index("sp")
        self.zy = here // SIDE, lax.rem(here, SIDE)
        self.buf, self.first, self.rows, self.own = buf, first, rows, own
        self.shard = buf.shape[0] // (SIDE * SIDE)
        self.send_sem, self.recv_sem = send_sem, recv_sem
        self.sent = 0

    def index(self, side, dp, dq):
        dz, dy = (dq, dp) if side == 0 else (dp, dq)
        return around(self.zy[0], dz) * SIDE + around(self.zy[1], dy)

    def group(self, dp, dq, half):
        if dq == 0:
            return 2 if dp == 2 else int((dp == -1) == (half == 1))
        return 3 + dp % SIDE if dq != 2 and (dq == -1) == (half == 0) else 7

    def send(self, side, dp, dq, half, to_p, to_q):
        width = self.buf.shape[1] // 2
        cols = slice(half * width, half * width + width)
        row = pl.multiple_of(self.index(side, dp, dq) * self.shard + side * self.rows, self.rows)
        piece = self.buf.at[pl.ds(row, self.rows), cols]
        own = self.own is not None and dp == 0 and dq == 0
        first = self.first + side * self.rows
        seen = [(d + 1) % SIDE - 1 for d in (dp - to_p, dq - to_q)]
        pltpu.make_async_remote_copy(
            src_ref=self.own.at[first : first + self.rows, cols] if own else piece,
            dst_ref=piece,
            send_sem=self.send_sem,
            recv_sem=self.recv_sem.at[self.group(*seen, half)],
            device_id={"sp": self.index(side, to_p, to_q), "tp": lax.axis_index("tp")},
            device_id_type=AXES,
        ).start()
        self.sent += 1

    def whole(self, count, group):
        rows = self.buf.at[: count * self.rows // 2, :]
        return pltpu.make_async_remote_copy(
            src_ref=rows,
            dst_ref=rows,
            send_sem=self.send_sem,
            recv_sem=self.recv_sem.at[group],
            device_id={"sp": self.index(0, 1, 0), "tp": lax.axis_index("tp")},
            device_id_type=AXES,
        )

    def arrived(self, group):
        self.whole(32 if group == 7 else 4, group).wait_recv()

    def send_p(self, k):
        for side in range(2):
            self.send(side, 0, 0, k, 1, 0)
            self.send(side, 0, 0, 1 - k, -1, 0)

    def send_q(self, dp, k):
        for side in range(2):
            self.send(side, dp, 0, k, 0, 1)
            self.send(side, dp, 0, 1 - k, 0, -1)

    def forward_p(self):
        self.arrived(0)
        for side in range(2):
            self.send(side, -1, 0, 0, 1, 0)
            self.send(side, 1, 0, 1, -1, 0)

    def near(self):
        self.arrived(1)
        self.send_q(-1, 0)
        self.send_q(1, 0)

    def near_rest(self):
        self.send_q(-1, 1)
        self.send_q(1, 1)

    def far(self):
        self.arrived(2)
        self.send_q(2, 0)

    def far_rest(self):
        self.send_q(2, 1)

    def forward_q(self, dp):
        self.arrived(3 + dp % SIDE)
        for side in range(2):
            self.send(side, dp, -1, 0, 0, 1)
            self.send(side, dp, 1, 1, 0, -1)

    def finish(self):
        self.arrived(7)

    def drain(self):
        self.whole(self.sent, 0).wait_send()


class Gather:
    def __init__(self, buf, send_sem, recv_sem):
        here = lax.axis_index("tp")
        self.x, self.core = here // 2, lax.rem(here, 2)
        self.buf, self.send_sem, self.recv_sem = buf, send_sem, recv_sem
        self.sent = 0

    def device(self, dx, other=False):
        return around(self.x, dx) * 2 + (1 - self.core if other else self.core)

    def cols(self, core):
        width = self.buf.shape[2] // 2
        return pl.ds(pl.multiple_of(core * width, width), width)

    def send(self, dx, half, to_x):
        rows = self.buf.shape[1] // 2
        piece = self.buf.at[around(self.x, dx), half * rows : half * rows + rows, self.cols(self.core)]
        if to_x:
            seen = (dx - to_x + 1) % SIDE - 1
            group = 2 if seen == 2 else int((seen == -1) == (half == 1))
        else:
            group = 3 + dx % SIDE
        pltpu.make_async_remote_copy(
            src_ref=piece,
            dst_ref=piece,
            send_sem=self.send_sem,
            recv_sem=self.recv_sem.at[group],
            device_id={"sp": lax.axis_index("sp"), "tp": self.device(to_x, not to_x)},
            device_id_type=AXES,
        ).start()
        self.sent += 1

    def whole(self, rows, group):
        return pltpu.make_async_remote_copy(
            src_ref=rows,
            dst_ref=rows,
            send_sem=self.send_sem,
            recv_sem=self.recv_sem.at[group],
            device_id={"sp": lax.axis_index("sp"), "tp": self.device(1)},
            device_id_type=AXES,
        )

    def arrived(self, group):
        self.whole(self.buf.at[0, :, : self.buf.shape[2] // 2], group).wait_recv()

    def start(self):
        for k in range(2):
            self.send(0, k, 1)
            self.send(0, 1 - k, -1)
        for k in range(2):
            self.send(0, k, 0)

    def near(self):
        self.arrived(0)
        self.send(-1, 0, 1)
        self.send(1, 1, -1)
        self.send(-1, 0, 0)
        self.send(1, 1, 0)
        self.arrived(1)
        self.send(-1, 1, 0)
        self.send(1, 0, 0)

    def far(self):
        self.arrived(2)
        self.send(2, 0, 0)
        self.send(2, 1, 0)

    def across(self, dx):
        self.arrived(3 + dx % SIDE)

    def drain(self):
        self.whole(self.buf.at[:, : self.buf.shape[1] * self.sent // 16, :], 0).wait_send()


class Phases:
    def __init__(self):
        self.scope = None

    def __call__(self, name):
        if self.scope is not None:
            self.scope.__exit__(None, None, None)
        self.scope = jax.named_scope(name) if name else None
        if self.scope is not None:
            self.scope.__enter__()


def layer_kernel(
    resid_hbm, u_hbm, ls_hbm, dr_hbm, fr_hbm, bm_hbm, cm_hbm, skip_hbm, gain_hbm, vw_ref, gw_ref, up_ref, down_ref,
    out_ref,
    resid_ref, u_ref, ls_ref, dr_ref, fr_ref, bm_ref, cm_ref, skip_ref, gain_ref,
    up_all, down_first, down_last, vg, dec_re, dec_im, feed_re, feed_im, step_wide, rows, ends, total, totals, carry,
    uperm, wout, states, mixed_all, upd_all, glu, raised, squares, hidden,
    products, stage_far, relay_in, stage_near, from_near, kept, stage_own, from_own, own_part, kept_out,
    local_sem, round_sem, ring_send, ring_recv, tot_send, tot_recv, cross_send, cross_recv, sum_send, sum_recv,
):
    phase = Phases()
    here, lane = lax.axis_index("sp"), lax.axis_index("tp")
    planes = SIDE * SIDE
    tokens, piece = resid_ref.shape
    half = tokens // 2
    shard = up_ref.shape[0]
    mix = Gather(mixed_all, ring_send.at[3], ring_recv.at[3])
    upd = Gather(upd_all, ring_send.at[4], ring_recv.at[4])
    right, left, partner = mix.device(1), mix.device(-1), mix.device(0, True)

    up = Relay(up_all, 0, shard // 2, ring_send.at[0], ring_recv.at[0], up_ref)
    first = Relay(down_first, 0, shard // 8, ring_send.at[1], ring_recv.at[1])
    last = Relay(down_last, 0, shard // 8, ring_send.at[2], ring_recv.at[2])
    near_planes = [up.index(0, *by) for by in ((1, 0), (-1, 0), (0, 1), (0, -1))]

    phase("signal")
    barrier = pltpu.get_barrier_semaphore()
    for target in near_planes:
        pl.semaphore_signal(barrier, inc=1, device_id={"sp": target, "tp": lane}, device_id_type=AXES)
    for target in (right, left, partner):
        pl.semaphore_signal(barrier, inc=1, device_id={"sp": here, "tp": target}, device_id_type=AXES)

    own_up = pl.ds(pl.multiple_of(here * shard, shard), shard)
    slim, width = shard // 4, up_ref.shape[1]
    own_down = pl.ds(pl.multiple_of(here * slim, slim), slim)
    own_units = pl.ds(pl.multiple_of(mix.core * width, width), width)

    def down_rows(core, k):
        return down_ref.at[pl.ds(pl.multiple_of(core * 2 * slim + k * slim, slim), slim), :]

    def cross_copy(number, src, dst):
        return pltpu.make_async_remote_copy(
            src_ref=src,
            dst_ref=dst,
            send_sem=cross_send.at[number],
            recv_sem=cross_recv.at[number],
            device_id={"sp": here, "tp": partner},
            device_id_type=AXES,
        )

    crossing = [
        cross_copy(k, down_rows(1 - mix.core, k), buf.at[own_down, own_units])
        for k, buf in enumerate((down_first, down_last))
    ]
    moves = (
        (u_hbm, u_ref), (dr_hbm, dr_ref), (fr_hbm, fr_ref), (ls_hbm, ls_ref), (bm_hbm, bm_ref), (cm_hbm, cm_ref),
        (up_ref, up_all.at[own_up, :]),
        (down_rows(mix.core, 0), down_first.at[own_down, own_units]),
        (down_rows(mix.core, 1), down_last.at[own_down, own_units]),
        (skip_hbm, skip_ref), (vw_ref, vg.at[:, :piece]), (gw_ref, vg.at[:, piece:]),
        (resid_hbm, resid_ref), (gain_hbm, gain_ref),
    )
    local = [pltpu.make_async_copy(src, dst, local_sem.at[k]) for k, (src, dst) in enumerate(moves)]
    for copy in local:
        copy.start()
    phase("barrier")
    pl.semaphore_wait(barrier, 7)
    phase("start_p")
    up.send_p(0)
    up.send_p(1)
    up.send_q(0, 0)
    up.send_q(0, 1)
    for copy in crossing:
        copy.start()

    def greet(number):
        for target in near_planes:
            pl.semaphore_signal(
                round_sem.at[number], inc=1, device_id={"sp": target, "tp": lane}, device_id_type=AXES
            )

    greet(0)
    for copy in local[:6]:
        copy.wait()
    phase("prepare")
    prepare(u_ref, ls_ref, dr_ref, fr_ref, bm_ref, cm_ref, uperm, step_wide, feed_re, feed_im, rows, wout)
    pl.semaphore_wait(round_sem.at[0], 4)
    greet(1)
    phase("first_pass")
    scan_refs = (step_wide, feed_re, feed_im, rows, dec_re, dec_im, ends)
    first_pass(*scan_refs, 0, 2)
    pl.semaphore_wait(round_sem.at[1], 4)
    greet(2)
    for copy in local[6:9]:
        copy.wait()
    for copy in crossing:
        copy.wait_recv()
    first.send_p(0)
    first_pass(*scan_refs, 2, 4)
    phase("chunk")
    chunk_prefix(ends, total)
    pl.semaphore_wait(round_sem.at[2], 4)

    def total_copy(src, dst, target):
        return pltpu.make_async_remote_copy(
            src_ref=src,
            dst_ref=dst,
            send_sem=tot_send.at[0],
            recv_sem=tot_recv.at[0],
            device_id={"sp": target, "tp": lane},
            device_id_type=AXES,
        )

    phase("totals")
    for by in range(1, planes):
        @pl.when(here + by < planes)
        def _():
            total_copy(total, totals.at[here], lax.rem(here + by, planes)).start()

    phase("serve1")
    up.forward_p()
    up.near()
    up.forward_q(0)
    up.near_rest()

    phase("fold")

    for count in range(1, planes):
        @pl.when(here == count)
        def _():
            total_copy(totals.at[:count], totals.at[:count], lax.rem(here + 1, planes)).wait_recv()

    def fold(j, value):
        h_re, h_im = value
        a_re, a_im = totals[j, 0:8, :], totals[j, 8:16, :]
        x_re, x_im = totals[j, 16:24, :], totals[j, 24:32, :]
        return a_re * h_re - a_im * h_im + x_re, a_re * h_im + a_im * h_re + x_im

    zero = jnp.zeros((8, 128), f32)
    h_re, h_im = lax.fori_loop(0, here, fold, (zero, zero))
    carry[0:8, :] = h_re
    carry[8:16, :] = h_im
    phase("second_pass")
    second_pass(dec_re, dec_im, feed_re, feed_im, ends, carry, states)
    phase("serve2")
    up.far()
    up.far_rest()
    first.send_p(1)
    local[9].wait()
    phase("read_out")
    own_cols = mix.cols(mix.core)
    mixed_all[mix.x, :, own_cols] = read_out(states, wout, uperm, skip_ref)
    phase("mix_start")
    mix.start()

    depth = 2 * piece

    def glu_part(chip, core=None):
        if core is None:
            lhs, at = mixed_all[chip], pl.ds(pl.multiple_of(chip * depth, depth), depth)
        else:
            lhs, at = mixed_all[chip, :, mix.cols(core)], pl.ds(pl.multiple_of((chip * 2 + core) * piece, piece), piece)
        return dot(lhs, vg[at, :])

    phase("mix_own")
    for copy in local[10:]:
        copy.wait()
    mix.across(0)
    glu[...] = glu_part(mix.x)
    phase("serve3")
    up.forward_q(-1)
    up.forward_q(1)
    first.send_q(0, 0)
    first.send_q(0, 1)
    phase("mix_near")
    mix.near()
    phase("serve4")
    up.forward_q(2)
    phase("mix_left")
    mix.across(-1)
    glu[...] += glu_part(around(mix.x, -1))
    phase("mix_right")
    mix.across(1)
    glu[...] += glu_part(around(mix.x, 1))
    phase("mix_far")
    mix.far()
    phase("mix_last")
    far_chip = around(mix.x, 2)
    glu[...] += glu_part(far_chip, mix.core)
    mix.across(2)
    glu[...] += glu_part(far_chip, 1 - mix.core)
    phase("updated")
    updated = (resid_ref[...].astype(f32) + glu[:, :piece] * jax.nn.sigmoid(glu[:, piece:])).astype(bf16)
    upd_all[upd.x, :, own_cols] = updated
    phase("upd_start")
    upd.start()
    phase("serve5")
    first.forward_p()
    first.near()
    first.near_rest()
    last.send_p(0)
    last.send_p(1)

    def up_part(chip, start, core=None):
        if core is None:
            wide, at = upd_all[chip], pl.ds(pl.multiple_of(chip * depth, depth), depth)
        else:
            wide, at = upd_all[chip, :, upd.cols(core)], pl.ds(pl.multiple_of((chip * 2 + core) * piece, piece), piece)
        wide = wide.astype(f32)
        square = wide * wide
        square = sum(square[:, 128 * k : 128 * k + 128] for k in range(square.shape[1] // 128))
        product = dot((wide * gain_ref[:, at]).astype(bf16), up_all[at, :])
        if start:
            squares[...] = square
            raised[...] = product
        else:
            squares[...] += square
            raised[...] += product

    phase("up_wait")
    up.finish()
    phase("upd_own")
    upd.across(0)
    up_part(upd.x, True)
    phase("serve6")
    first.forward_q(0)
    first.far()
    last.send_q(0, 0)
    first.far_rest()
    last.send_q(0, 1)
    phase("upd_near")
    upd.near()
    phase("upd_left")
    upd.across(-1)
    last.forward_p()
    up_part(around(upd.x, -1), False)
    phase("serve7")
    first.forward_q(-1)
    first.forward_q(1)
    phase("upd_right")
    upd.across(1)
    up_part(around(upd.x, 1), False)
    phase("serve8")
    first.forward_q(2)
    last.near()
    phase("upd_far")
    upd.far()
    up_part(far_chip, False, upd.core)
    phase("upd_last")
    upd.across(2)
    up_part(far_chip, False, 1 - upd.core)
    phase("hidden")
    inv_rms = lax.rsqrt(jnp.sum(squares[...], axis=1, keepdims=True) / (SIDE * depth) + rms_eps)
    active = jnp.maximum(raised[...] * inv_rms, 0.0)
    hidden[:, own_units] = (active * active).astype(bf16)
    crossing.append(cross_copy(2, hidden.at[:, own_units], hidden.at[:, own_units]))
    crossing[2].start()
    phase("serve9")
    last.far()
    last.forward_q(0)
    last.near_rest()
    last.far_rest()

    span = piece // 2
    quarter = half // 2

    chunk = quarter // 2

    def turned(value, by=None):
        return pltpu.roll(value, span // 2 if by is None else by, 1)

    low_lanes = lax.broadcasted_iota(jnp.int32, (chunk, span), 1) < span // 2

    def packed(value, core):
        parts = []
        for c in range(value.shape[0] // quarter):
            top, low = (value[c * quarter + k * chunk : c * quarter + k * chunk + chunk] for k in range(2))
            parts.append(jnp.where(low_lanes, top, turned(low)) if core == 0 else jnp.where(low_lanes, turned(top), low))
        return jnp.concatenate(parts, axis=0)

    class Sum:
        def __init__(self, k, buf):
            self.k, self.buf = k, buf
            self.relays = [
                [
                    self.copy(
                        0, 2 * j + c, stage_far.at[k, j, c * quarter : c * quarter + quarter],
                        relay_in.at[k, j, c * quarter : c * quarter + quarter], target,
                    )
                    for c in range(2)
                ]
                for j, target in enumerate((right, left))
            ]
            self.own = self.copy(1, 4, stage_own.at[k], from_own.at[k], partner)
            self.near = self.copy(2, 5, stage_near.at[k], from_near.at[k], right)

        def copy(self, send, recv, src, dst, target):
            return pltpu.make_async_remote_copy(
                src_ref=src,
                dst_ref=dst,
                send_sem=sum_send.at[self.k, send],
                recv_sem=sum_recv.at[self.k, recv],
                device_id={"sp": here, "tp": target},
                device_id_type=AXES,
            )

        def product(self, dx):
            return products[:, pl.ds(pl.multiple_of(around(mix.x, dx) * span, span), span)]

        def send_near(self, side, part, value, first=0):
            chip = around(mix.x, 1 - 2 * side)
            rows = slice(first, first + value.shape[0] // 2)
            for core in range(2):
                stage_near[self.k, side, core, part, rows] = packed(value, core).astype(bf16)
                self.copy(
                    2, 5, stage_near.at[self.k, side, core, part, rows],
                    from_near.at[self.k, mix.core, side, part, rows], chip * 2 + core,
                ).start()

        def start(self, *serve):
            k = self.k
            products[...] = dot_t(hidden[...], self.buf[...])
            far = self.product(2).astype(bf16)
            for j in range(2):
                stage_far[k, j] = far[j * half : j * half + half]
            for c in range(2):
                for j in range(2):
                    self.relays[j][c].start()
            near = self.product(1)
            self.send_near(0, 1, near[half:])
            kept[k, 0] = near[:half]
            near = self.product(-1)
            self.send_near(1, 0, near[:half])
            kept[k, 1] = near[half:]
            if serve:
                serve[0]()
            own = self.product(0)
            for j in range(2):
                both = [packed(own[j * half : j * half + half], core) for core in range(2)]
                own_part[k, j] = jnp.where(mix.core == 0, both[0], both[1])
                stage_own[k, j] = jnp.where(mix.core == 0, both[1], both[0]).astype(bf16)
            self.own.start()
            if serve:
                serve[1]()

        def relay(self):
            k = self.k
            for c in range(2):
                rows = slice(c * quarter, c * quarter + quarter)
                for j in range(2):
                    self.relays[j][c].wait_recv()
                    self.send_near(j, j, kept[k, j, rows] + relay_in[k, j, rows].astype(f32), c * chunk)

        def result(self):
            k = self.k
            self.own.wait_recv()
            self.near.wait_recv()
            found = []
            for core in range(2):
                rows = []
                for j in range(2):
                    here_part = jnp.where(mix.core == core, own_part[k, j], from_own[k, j].astype(f32))
                    total = here_part + (from_near[k, core, 0, j].astype(f32) + from_near[k, core, 1, j].astype(f32))
                    for c in range(2):
                        part = total[c * chunk : c * chunk + chunk]
                        rows += [part, turned(part)]
                found.append(jnp.concatenate(rows, axis=0))
            return found

        def drain(self):
            self.own.wait_send()
            self.near.wait_send()
            self.copy(0, 0, stage_far.at[self.k], stage_far.at[self.k], right).wait_send()

    phase("first_wait")
    first.finish()
    crossing[2].wait_recv()
    phase("first_sum")
    early, late = Sum(0, down_first), Sum(1, down_last)

    def serve_near():
        last.forward_q(-1)
        last.forward_q(1)

    def serve_far():
        last.forward_q(2)

    early.start(serve_near, serve_far)
    phase("first_relay")
    early.relay()
    phase("last_wait")
    last.finish()
    phase("last_sum")
    late.start()
    phase("last_relay")
    late.relay()
    phase("first_result")
    lane_group = lax.broadcasted_iota(jnp.int32, (tokens, span), 1) // slim
    blocks = [upd_all[upd.x, :, own_cols].astype(f32)[:, b * span : b * span + span] for b in range(2)]

    def put_in(k, found):
        for b in range(2):
            for core in range(2):
                place = core * 2 + k
                moved = turned(found[core], (place - b) % 4 * slim) if place != b else found[core]
                blocks[b] = blocks[b] + jnp.where(lane_group == place, moved, 0.0)

    put_in(0, early.result())
    for b in range(2):
        kept_out[:, b * span : b * span + span] = blocks[b]
    phase("last_result")
    two = late.result()
    phase("result")
    blocks = [kept_out[:, b * span : b * span + span] for b in range(2)]
    put_in(1, two)
    out_ref[...] = jnp.concatenate(blocks, axis=1).astype(bf16)

    phase("drain")
    for count in range(1, planes):
        @pl.when(planes - 1 - here == count)
        def _():
            total_copy(totals.at[:count], totals.at[:count], lax.rem(here + 1, planes)).wait_send()

    for part in (up, first, last, mix, upd, early, late):
        part.drain()
    for copy in crossing:
        copy.wait_send()
    phase(None)


def per_device(
    resid, mixer_in, log_step, decay_real, frequency, input_matrix, output_matrix, skip_gain,
    value_weight, gate_weight, norm_gain, up_weight, down_weight,
):
    tokens, channels = mixer_in.shape
    groups, states = decay_real.shape
    width = groups * states
    planes, slots = lax.axis_size("sp"), lax.axis_size("tp")
    features = slots * channels
    hidden = up_weight.shape[1]
    span = channels // 2
    vmem = pl.BlockSpec(memory_space=pltpu.VMEM)
    hbm = pl.BlockSpec(memory_space=pl.ANY)
    wide = pltpu.VMEM((tokens, width), f32)
    block = pltpu.VMEM((tokens, channels), bf16)
    halves = pltpu.VMEM((2, 2, tokens // 2, span), bf16)
    packs = pltpu.VMEM((2, 2, tokens // 4, span), bf16)
    near = pltpu.VMEM((2, 2, 2, 2, tokens // 4, span), bf16)
    pieces = pltpu.VMEM((SIDE, tokens, 2 * channels), bf16)
    matrix = pltpu.VMEM((2, channels, states), f32)
    down = pltpu.VMEM((features // 4, 2 * hidden), bf16)
    dma = pltpu.SemaphoreType.DMA
    return pl.pallas_call(
        layer_kernel,
        out_shape=pltpu.VMEM((tokens, channels), bf16),
        in_specs=[hbm] * 13,
        out_specs=vmem,
        scratch_shapes=[
            block, block, pltpu.VMEM((groups, tokens), f32),
            pltpu.VMEM((groups, states), f32), pltpu.VMEM((groups, states), f32), matrix, matrix,
            pltpu.VMEM((1, channels), f32), pltpu.VMEM((1, features), f32),
            pltpu.VMEM((features, hidden), bf16), down, down, pltpu.VMEM((features, 2 * channels), bf16),
            wide, wide, wide, wide, wide,
            pltpu.VMEM((8, width), f32), pltpu.VMEM((4, CHUNKS, width), f32),
            pltpu.VMEM((32, 128), f32), pltpu.VMEM((planes, 32, 128), f32), pltpu.VMEM((16, 128), f32),
            block, pltpu.VMEM((channels, 2 * width), bf16), pltpu.VMEM((tokens, 2 * width), bf16),
            pieces, pieces, pltpu.VMEM((tokens, 2 * channels), f32),
            pltpu.VMEM((tokens, hidden), f32), pltpu.VMEM((tokens, 128), f32), pltpu.VMEM((tokens, 2 * hidden), bf16),
            pltpu.VMEM((tokens, SIDE * span), f32), halves, halves, near, near, pltpu.VMEM((2, 2, tokens // 2, span), f32),
            packs, packs, pltpu.VMEM((2, 2, tokens // 4, span), f32), pltpu.VMEM((tokens, channels), f32),
            dma((14,)), pltpu.SemaphoreType.REGULAR((3,)), dma((5,)), dma((5, 8)),
            dma((1,)), dma((1,)), dma((3,)), dma((3,)), dma((2, 3)), dma((2, 6)),
        ],
        name="layer",
        compiler_params=pltpu.CompilerParams(
            vmem_limit_bytes=58 * 2**20, collective_id=0, has_side_effects=True
        ),
    )(
        resid, mixer_in, log_step.T, decay_real, frequency,
        input_matrix.transpose(0, 1, 3, 2).reshape(2, channels, states), output_matrix.reshape(2, channels, states),
        skip_gain.reshape(1, -1), norm_gain.reshape(1, -1), value_weight, gate_weight, up_weight, down_weight,
    )


def solution(mesh):
    in_specs = (
        P("sp", "tp"), P("sp", "tp"), P("sp", "tp"), P("tp", None), P("tp", None),
        P(None, "tp", None, None), P(None, "tp", None, None), P("tp"),
        P(None, "tp"), P(None, "tp"), P(), P("sp", "tp"), P("sp", "tp"),
    )
    return jax.shard_map(
        per_device, mesh=mesh, in_specs=in_specs, out_specs=P("sp", "tp"), check_vma=False
    )
```

```python
import functools
import math

import jax
import jax.numpy as jnp
from jax import lax
from jax.experimental import pallas as pl
from jax.experimental.pallas import tpu as pltpu
from jax.sharding import PartitionSpec as P

rms_eps = 1e-06
f32 = jnp.float32
bf16 = jnp.bfloat16
CHUNKS = 8


def onehot(shape, test):
    row = lax.broadcasted_iota(jnp.int32, shape, 0)
    col = lax.broadcasted_iota(jnp.int32, shape, 1)
    return jnp.where(test(row, col), 1.0, 0.0).astype(bf16)


def split3(x):
    hi = x.astype(bf16)
    rest = x - hi.astype(f32)
    mid = rest.astype(bf16)
    return hi, mid, (rest - mid.astype(f32)).astype(bf16)


def dot(a, b):
    return jnp.dot(a, b, preferred_element_type=f32)


def dot_t(a, b):
    return lax.dot_general(a, b, (((1,), (1,)), ((), ())), preferred_element_type=f32)


def spread_row(x, states):
    groups = x.shape[0]
    width = groups * states
    lanes = onehot((states, width), lambda r, c: r == c % states)
    wide = sum(dot(part, lanes) for part in split3(x))
    row = lax.broadcasted_iota(jnp.int32, wide.shape, 0)
    col = lax.broadcasted_iota(jnp.int32, wide.shape, 1)
    return jnp.sum(jnp.where(row == col // states, wide, 0.0), axis=0, keepdims=True)


def prepare(u_ref, ls_ref, dr_ref, fr_ref, bm_ref, cm_ref, uperm, step_wide, proj_re, proj_im, rows, wout):
    tokens, channels = u_ref.shape
    groups, states = dr_ref.shape
    width = groups * states
    per_group = channels // groups
    span = tokens // CHUNKS
    perm = onehot((tokens, tokens), lambda r, c: c == (r % CHUNKS) * span + r // CHUNKS)
    u_sorted = dot(perm, u_ref[...]).astype(bf16)
    uperm[...] = u_sorted
    decay = spread_row(dr_ref[...], states)
    angular = spread_row(fr_ref[...], states)
    rows[0:1, :] = -decay
    rows[1:2, :] = 0.5 * angular
    modulus = decay * decay + angular * angular
    inv_re = -decay / modulus
    inv_im = -angular / modulus
    step = jnp.exp(ls_ref[...])
    step = sum(dot_t(perm, part) for part in split3(step))
    group_lanes = onehot((groups, width), lambda r, c: r == c // states)
    step_wide[...] = sum(dot(part, group_lanes) for part in split3(step))
    state_lanes = onehot((states, width), lambda r, c: r == c % states)
    row = lax.broadcasted_iota(jnp.int32, (channels, width), 0)
    col = lax.broadcasted_iota(jnp.int32, (channels, width), 1)
    same = row // per_group == col // states
    b_re = dot(bm_ref[0].astype(bf16), state_lanes)
    b_im = dot(bm_ref[1].astype(bf16), state_lanes)
    w_re = jnp.where(same, b_re * inv_re - b_im * inv_im, 0.0).astype(bf16)
    w_im = jnp.where(same, b_re * inv_im + b_im * inv_re, 0.0).astype(bf16)
    proj_re[...] = dot(u_sorted, w_re)
    proj_im[...] = dot(u_sorted, w_im)
    wout[:, :width] = jnp.where(same, dot(cm_ref[0].astype(bf16), state_lanes), 0.0).astype(bf16)
    wout[:, width:] = jnp.where(same, -dot(cm_ref[1].astype(bf16), state_lanes), 0.0).astype(bf16)


SIN = (-1.0 / 6, 1.0 / 120, -1.0 / 5040, 1.0 / 362880, -1.0 / 39916800)
COS = (-0.5, 1.0 / 24, -1.0 / 720, 1.0 / 40320, -1.0 / 3628800)


def series(q, terms):
    total = terms[-1] * q
    for term in terms[-2::-1]:
        total = (total + term) * q
    return total


def first_pass(step_wide, proj_re, proj_im, rows, dec_re, dec_im, ends, first, last):
    tokens, width = step_wide.shape
    block = 256

    def one_block(b, _):
        lanes = pl.ds(pl.multiple_of(b * block, block), block)
        minus_decay = jnp.broadcast_to(rows[0:1, lanes], (CHUNKS, block))
        half_angular = jnp.broadcast_to(rows[1:2, lanes], (CHUNKS, block))

        def one_step(i, carry):
            a_re, a_im, x_re, x_im = carry
            at = pl.ds(pl.multiple_of(i * CHUNKS, CHUNKS), CHUNKS)
            step = step_wide[at, lanes]
            half = step * half_angular
            q = half * half
            sine = half + half * series(q, SIN)
            cosine = 1.0 + series(q, COS)
            factor = jnp.exp(step * minus_decay)
            twice = factor * (sine + sine)
            d_re = factor - twice * sine
            d_im = twice * cosine
            less = d_re - 1.0
            p_re = proj_re[at, lanes]
            p_im = proj_im[at, lanes]
            u_re = less * p_re - d_im * p_im
            u_im = less * p_im + d_im * p_re
            dec_re[at, lanes] = d_re
            dec_im[at, lanes] = d_im
            proj_re[at, lanes] = u_re
            proj_im[at, lanes] = u_im
            return (
                d_re * a_re - d_im * a_im,
                d_re * a_im + d_im * a_re,
                d_re * x_re - d_im * x_im + u_re,
                d_re * x_im + d_im * x_re + u_im,
            )

        zero = jnp.zeros((CHUNKS, block), f32)
        found = lax.fori_loop(0, tokens // CHUNKS, one_step, (zero + 1.0, zero, zero, zero), unroll=2)
        for k in range(4):
            ends[k, :, lanes] = found[k]
        return 0

    lax.fori_loop(first, last, one_block, 0)


def chain(early, late):
    return (
        early[0] * late[0] - early[1] * late[1],
        early[0] * late[1] + early[1] * late[0],
        late[0] * early[2] - late[1] * early[3] + late[2],
        late[0] * early[3] + late[1] * early[2] + late[3],
    )


def chunk_prefix(ends, total, total_x, wide_x):
    width = ends.shape[2]
    value = tuple(ends[k] for k in range(4))
    row = lax.broadcasted_iota(jnp.int32, value[0].shape, 0)
    unit = (1.0, 0.0, 0.0, 0.0)

    def moved(value, by):
        return tuple(
            jnp.where(row >= by, pltpu.roll(part, by, 0), zero) for part, zero in zip(value, unit)
        )

    for by in (1, 2, 4):
        value = chain(moved(value, by), value)
    for k in range(4):
        for j in range(width // 128):
            kept = total if k < 2 else wide_x
            at = 8 * (k % 2) + j
            kept[at : at + 1, :] = value[k][CHUNKS - 1 :, 128 * j : 128 * j + 128]
    total_x[...] = wide_x[...].astype(bf16)
    before = moved(value, 1)
    for k in range(4):
        ends[k] = before[k]


def second_pass(dec_re, dec_im, feed_re, feed_im, ends, carry, states):
    tokens, width = dec_re.shape
    block = 512
    for b in range(width // block):
        lanes = pl.ds(b * block, block)
        lanes_im = pl.ds(width + b * block, block)
        per = block // 128
        h_re = jnp.concatenate([carry[per * b + j : per * b + j + 1, :] for j in range(per)], axis=1)
        h_im = jnp.concatenate([carry[8 + per * b + j : 9 + per * b + j, :] for j in range(per)], axis=1)
        a_re, a_im = ends[0, :, lanes], ends[1, :, lanes]
        x_re = ends[2, :, lanes] + a_re * h_re - a_im * h_im
        x_im = ends[3, :, lanes] + a_re * h_im + a_im * h_re

        def one_step(i, value):
            x_re, x_im = value
            seen = []
            for k in range(2):
                at = pl.ds(pl.multiple_of(i * 2 * CHUNKS + k * CHUNKS, CHUNKS), CHUNKS)
                d_re, d_im = dec_re[at, lanes], dec_im[at, lanes]
                x_re, x_im = (
                    d_re * x_re - d_im * x_im + feed_re[at, lanes],
                    d_re * x_im + d_im * x_re + feed_im[at, lanes],
                )
                seen.append((x_re, x_im))
            both = pl.ds(pl.multiple_of(i * 2 * CHUNKS, 2 * CHUNKS), 2 * CHUNKS)
            states[both, lanes] = jnp.concatenate([seen[0][0], seen[1][0]], axis=0).astype(bf16)
            states[both, lanes_im] = jnp.concatenate([seen[0][1], seen[1][1]], axis=0).astype(bf16)
            return x_re, x_im

        lax.fori_loop(0, tokens // (2 * CHUNKS), one_step, (x_re, x_im), unroll=2)


def read_out(states, wout, uperm, skip_ref):
    tokens = states.shape[0]
    span = tokens // CHUNKS
    out = dot_t(states[...], wout[...]) + skip_ref[...] * uperm[...].astype(f32)
    mixed = jax.nn.gelu(out).astype(bf16)
    back = onehot((tokens, tokens), lambda r, c: r == (c % CHUNKS) * span + c // CHUNKS)
    return dot(back, mixed).astype(bf16)


AXES = pl.DeviceIdType.MESH
SIDE = 4


def around(index, by):
    return lax.rem(index + by + SIDE, SIDE)


class Relay:
    def __init__(self, buf, first, rows, send_sem, recv_sem, own=None):
        here = lax.axis_index("sp")
        self.zy = here // SIDE, lax.rem(here, SIDE)
        self.buf, self.first, self.rows, self.own = buf, first, rows, own
        self.shard = buf.shape[0] // (SIDE * SIDE)
        self.send_sem, self.recv_sem = send_sem, recv_sem
        self.sent = 0

    def index(self, side, dp, dq):
        dz, dy = (dq, dp) if side == 0 else (dp, dq)
        return around(self.zy[0], dz) * SIDE + around(self.zy[1], dy)

    def group(self, dp, dq, half):
        if dq == 0:
            return 2 if dp == 2 else int((dp == -1) == (half == 1))
        return 3 + dp % SIDE if dq != 2 and (dq == -1) == (half == 0) else 7

    def send(self, side, dp, dq, half, to_p, to_q):
        width = self.buf.shape[1] // 2
        cols = slice(half * width, half * width + width)
        row = pl.multiple_of(self.index(side, dp, dq) * self.shard + side * self.rows, self.rows)
        piece = self.buf.at[pl.ds(row, self.rows), cols]
        own = self.own is not None and dp == 0 and dq == 0
        first = self.first + side * self.rows
        seen = [(d + 1) % SIDE - 1 for d in (dp - to_p, dq - to_q)]
        pltpu.make_async_remote_copy(
            src_ref=self.own.at[first : first + self.rows, cols] if own else piece,
            dst_ref=piece,
            send_sem=self.send_sem,
            recv_sem=self.recv_sem.at[self.group(*seen, half)],
            device_id={"sp": self.index(side, to_p, to_q), "tp": lax.axis_index("tp")},
            device_id_type=AXES,
        ).start()
        self.sent += 1

    def whole(self, count, group):
        rows = self.buf.at[: count * self.rows // 2, :]
        return pltpu.make_async_remote_copy(
            src_ref=rows,
            dst_ref=rows,
            send_sem=self.send_sem,
            recv_sem=self.recv_sem.at[group],
            device_id={"sp": self.index(0, 1, 0), "tp": lax.axis_index("tp")},
            device_id_type=AXES,
        )

    def arrived(self, group):
        self.whole(32 if group == 7 else 4, group).wait_recv()

    def send_p(self, k):
        for side in range(2):
            self.send(side, 0, 0, k, 1, 0)
            self.send(side, 0, 0, 1 - k, -1, 0)

    def send_q(self, dp, k):
        for side in range(2):
            self.send(side, dp, 0, k, 0, 1)
            self.send(side, dp, 0, 1 - k, 0, -1)

    def forward_p(self):
        self.arrived(0)
        for side in range(2):
            self.send(side, -1, 0, 0, 1, 0)
            self.send(side, 1, 0, 1, -1, 0)

    def near(self):
        self.arrived(1)
        self.send_q(-1, 0)
        self.send_q(1, 0)

    def near_rest(self):
        self.send_q(-1, 1)
        self.send_q(1, 1)

    def far(self):
        self.arrived(2)
        self.send_q(2, 0)

    def far_rest(self):
        self.send_q(2, 1)

    def forward_q(self, dp):
        self.arrived(3 + dp % SIDE)
        for side in range(2):
            self.send(side, dp, -1, 0, 0, 1)
            self.send(side, dp, 1, 1, 0, -1)

    def finish(self):
        self.arrived(7)

    def drain(self):
        self.whole(self.sent, 0).wait_send()


class Gather:
    def __init__(self, buf, send_sem, recv_sem):
        here = lax.axis_index("tp")
        self.x, self.core = here // 2, lax.rem(here, 2)
        self.buf, self.send_sem, self.recv_sem = buf, send_sem, recv_sem
        self.sent = 0

    def device(self, dx, other=False):
        return around(self.x, dx) * 2 + (1 - self.core if other else self.core)

    def cols(self, core):
        width = self.buf.shape[2] // 2
        return pl.ds(pl.multiple_of(core * width, width), width)

    def send(self, dx, half, to_x):
        rows = self.buf.shape[1] // 2
        piece = self.buf.at[around(self.x, dx), half * rows : half * rows + rows, self.cols(self.core)]
        if to_x:
            seen = (dx - to_x + 1) % SIDE - 1
            group = 2 if seen == 2 else int((seen == -1) == (half == 1))
        else:
            group = 3 + dx % SIDE
        pltpu.make_async_remote_copy(
            src_ref=piece,
            dst_ref=piece,
            send_sem=self.send_sem,
            recv_sem=self.recv_sem.at[group],
            device_id={"sp": lax.axis_index("sp"), "tp": self.device(to_x, not to_x)},
            device_id_type=AXES,
        ).start()
        self.sent += 1

    def whole(self, rows, group):
        return pltpu.make_async_remote_copy(
            src_ref=rows,
            dst_ref=rows,
            send_sem=self.send_sem,
            recv_sem=self.recv_sem.at[group],
            device_id={"sp": lax.axis_index("sp"), "tp": self.device(1)},
            device_id_type=AXES,
        )

    def arrived(self, group):
        self.whole(self.buf.at[0, :, : self.buf.shape[2] // 2], group).wait_recv()

    def start(self):
        for k in range(2):
            self.send(0, k, 1)
            self.send(0, 1 - k, -1)
        for k in range(2):
            self.send(0, k, 0)

    def near(self):
        self.arrived(0)
        self.send(-1, 0, 1)
        self.send(1, 1, -1)
        self.send(-1, 0, 0)
        self.send(1, 1, 0)
        self.arrived(1)
        self.send(-1, 1, 0)
        self.send(1, 0, 0)

    def far(self):
        self.arrived(2)
        self.send(2, 0, 0)
        self.send(2, 1, 0)

    def across(self, dx):
        self.arrived(3 + dx % SIDE)

    def drain(self):
        self.whole(self.buf.at[:, : self.buf.shape[1] * self.sent // 16, :], 0).wait_send()


class Phases:
    def __init__(self):
        self.scope = None

    def __call__(self, name):
        if self.scope is not None:
            self.scope.__exit__(None, None, None)
        self.scope = jax.named_scope(name) if name else None
        if self.scope is not None:
            self.scope.__enter__()


def layer_kernel(
    resid_hbm, u_hbm, ls_hbm, dr_hbm, fr_hbm, bm_hbm, cm_hbm, skip_hbm, gain_hbm, vw_ref, gw_ref, up_ref, down_ref,
    out_ref,
    resid_ref, u_ref, ls_ref, dr_ref, fr_ref, bm_ref, cm_ref, skip_ref, gain_ref,
    up_all, down_first, down_last, vg, dec_re, dec_im, feed_re, feed_im, step_wide, rows, ends, total, totals, total_x, totals_x, carry,
    uperm, wout, states, mixed_all, upd_all, glu, raised, squares, hidden,
    products, stage_far, relay_in, stage_near, from_near, kept, stage_own, from_own, own_part, kept_out,
    local_sem, round_sem, ring_send, ring_recv, tot_send, tot_recv, cross_send, cross_recv, sum_send, sum_recv,
):
    phase = Phases()
    here, lane = lax.axis_index("sp"), lax.axis_index("tp")
    planes = SIDE * SIDE
    tokens, piece = resid_ref.shape
    half = tokens // 2
    shard = up_ref.shape[0]
    mix = Gather(mixed_all, ring_send.at[3], ring_recv.at[3])
    upd = Gather(upd_all, ring_send.at[4], ring_recv.at[4])
    right, left, partner = mix.device(1), mix.device(-1), mix.device(0, True)

    up = Relay(up_all, 0, shard // 2, ring_send.at[0], ring_recv.at[0], up_ref)
    first = Relay(down_first, 0, shard // 8, ring_send.at[1], ring_recv.at[1])
    last = Relay(down_last, 0, shard // 8, ring_send.at[2], ring_recv.at[2])
    near_planes = [up.index(0, *by) for by in ((1, 0), (-1, 0), (0, 1), (0, -1))]

    phase("signal")
    barrier = pltpu.get_barrier_semaphore()
    for target in near_planes:
        pl.semaphore_signal(barrier, inc=1, device_id={"sp": target, "tp": lane}, device_id_type=AXES)
    for target in (right, left, partner):
        pl.semaphore_signal(barrier, inc=1, device_id={"sp": here, "tp": target}, device_id_type=AXES)

    own_up = pl.ds(pl.multiple_of(here * shard, shard), shard)
    slim, width = shard // 4, up_ref.shape[1]
    own_down = pl.ds(pl.multiple_of(here * slim, slim), slim)
    own_units = pl.ds(pl.multiple_of(mix.core * width, width), width)

    def down_rows(core, k):
        return down_ref.at[pl.ds(pl.multiple_of(core * 2 * slim + k * slim, slim), slim), :]

    def cross_copy(number, src, dst):
        return pltpu.make_async_remote_copy(
            src_ref=src,
            dst_ref=dst,
            send_sem=cross_send.at[number],
            recv_sem=cross_recv.at[number],
            device_id={"sp": here, "tp": partner},
            device_id_type=AXES,
        )

    crossing = [
        cross_copy(k, down_rows(1 - mix.core, k), buf.at[own_down, own_units])
        for k, buf in enumerate((down_first, down_last))
    ]
    moves = (
        (u_hbm, u_ref), (dr_hbm, dr_ref), (fr_hbm, fr_ref), (ls_hbm, ls_ref), (bm_hbm, bm_ref), (cm_hbm, cm_ref),
        (up_ref, up_all.at[own_up, :]),
        (down_rows(mix.core, 0), down_first.at[own_down, own_units]),
        (down_rows(mix.core, 1), down_last.at[own_down, own_units]),
        (skip_hbm, skip_ref), (vw_ref, vg.at[:, :piece]), (gw_ref, vg.at[:, piece:]),
        (resid_hbm, resid_ref), (gain_hbm, gain_ref),
    )
    local = [pltpu.make_async_copy(src, dst, local_sem.at[k]) for k, (src, dst) in enumerate(moves)]
    for copy in local:
        copy.start()
    phase("barrier")
    pl.semaphore_wait(barrier, 7)
    phase("start_p")
    up.send_p(0)
    up.send_p(1)
    up.send_q(0, 0)
    up.send_q(0, 1)
    for copy in crossing:
        copy.start()

    def greet(number):
        for target in near_planes:
            pl.semaphore_signal(
                round_sem.at[number], inc=1, device_id={"sp": target, "tp": lane}, device_id_type=AXES
            )

    greet(0)
    for copy in local[:6]:
        copy.wait()
    phase("prepare")
    prepare(u_ref, ls_ref, dr_ref, fr_ref, bm_ref, cm_ref, uperm, step_wide, feed_re, feed_im, rows, wout)
    pl.semaphore_wait(round_sem.at[0], 4)
    greet(1)
    phase("first_pass")
    scan_refs = (step_wide, feed_re, feed_im, rows, dec_re, dec_im, ends)
    first_pass(*scan_refs, 0, 2)
    pl.semaphore_wait(round_sem.at[1], 4)
    greet(2)
    for copy in local[6:9]:
        copy.wait()
    for copy in crossing:
        copy.wait_recv()
    first.send_p(0)
    first_pass(*scan_refs, 2, 4)
    phase("chunk")
    chunk_prefix(ends, total, total_x, carry)
    pl.semaphore_wait(round_sem.at[2], 4)

    def total_copy(k, src, dst, target):
        return pltpu.make_async_remote_copy(
            src_ref=src,
            dst_ref=dst,
            send_sem=tot_send.at[k],
            recv_sem=tot_recv.at[k],
            device_id={"sp": target, "tp": lane},
            device_id_type=AXES,
        )

    phase("totals")
    for by in range(1, planes):
        @pl.when(here + by < planes)
        def _():
            for k, (src, dst) in enumerate(((total, totals), (total_x, totals_x))):
                total_copy(k, src, dst.at[here], lax.rem(here + by, planes)).start()

    phase("serve1")
    up.forward_p()
    up.near()
    up.forward_q(0)
    up.near_rest()

    phase("fold")

    for count in range(1, planes):
        @pl.when(here == count)
        def _():
            for k, part in enumerate((totals, totals_x)):
                total_copy(k, part.at[:count], part.at[:count], lax.rem(here + 1, planes)).wait_recv()

    def fold(j, value):
        h_re, h_im = value
        a_re, a_im = totals[j, 0:8, :], totals[j, 8:16, :]
        x_both = totals_x[j].astype(f32)
        x_re, x_im = x_both[0:8], x_both[8:16]
        return a_re * h_re - a_im * h_im + x_re, a_re * h_im + a_im * h_re + x_im

    zero = jnp.zeros((8, 128), f32)
    h_re, h_im = lax.fori_loop(0, here, fold, (zero, zero))
    carry[0:8, :] = h_re
    carry[8:16, :] = h_im
    phase("second_pass")
    second_pass(dec_re, dec_im, feed_re, feed_im, ends, carry, states)
    phase("serve2")
    up.far()
    up.far_rest()
    first.send_p(1)
    local[9].wait()
    phase("read_out")
    own_cols = mix.cols(mix.core)
    mixed_all[mix.x, :, own_cols] = read_out(states, wout, uperm, skip_ref)
    phase("mix_start")
    mix.start()

    depth = 2 * piece

    def glu_part(chip, core=None):
        if core is None:
            lhs, at = mixed_all[chip], pl.ds(pl.multiple_of(chip * depth, depth), depth)
        else:
            lhs, at = mixed_all[chip, :, mix.cols(core)], pl.ds(pl.multiple_of((chip * 2 + core) * piece, piece), piece)
        return dot(lhs, vg[at, :])

    phase("mix_own")
    for copy in local[10:]:
        copy.wait()
    mix.across(0)
    glu[...] = glu_part(mix.x)
    phase("serve3")
    up.forward_q(-1)
    up.forward_q(1)
    first.send_q(0, 0)
    first.send_q(0, 1)
    phase("mix_near")
    mix.near()
    phase("serve4")
    up.forward_q(2)
    phase("mix_left")
    mix.across(-1)
    glu[...] += glu_part(around(mix.x, -1))
    phase("mix_right")
    mix.across(1)
    glu[...] += glu_part(around(mix.x, 1))
    phase("mix_far")
    mix.far()
    phase("mix_last")
    far_chip = around(mix.x, 2)
    glu[...] += glu_part(far_chip, mix.core)
    mix.across(2)
    glu[...] += glu_part(far_chip, 1 - mix.core)
    phase("updated")
    updated = (resid_ref[...].astype(f32) + glu[:, :piece] * jax.nn.sigmoid(glu[:, piece:])).astype(bf16)
    upd_all[upd.x, :, own_cols] = updated
    phase("upd_start")
    upd.start()
    phase("serve5")
    first.forward_p()
    first.near()
    first.near_rest()
    last.send_p(0)
    last.send_p(1)

    def up_part(chip, start, core=None):
        if core is None:
            wide, at = upd_all[chip], pl.ds(pl.multiple_of(chip * depth, depth), depth)
        else:
            wide, at = upd_all[chip, :, upd.cols(core)], pl.ds(pl.multiple_of((chip * 2 + core) * piece, piece), piece)
        wide = wide.astype(f32)
        square = wide * wide
        square = sum(square[:, 128 * k : 128 * k + 128] for k in range(square.shape[1] // 128))
        product = dot((wide * gain_ref[:, at]).astype(bf16), up_all[at, :])
        if start:
            squares[...] = square
            raised[...] = product
        else:
            squares[...] += square
            raised[...] += product

    phase("up_wait")
    up.finish()
    phase("upd_own")
    upd.across(0)
    up_part(upd.x, True)
    phase("serve6")
    first.forward_q(0)
    first.far()
    last.send_q(0, 0)
    first.far_rest()
    last.send_q(0, 1)
    phase("upd_near")
    upd.near()
    phase("upd_left")
    upd.across(-1)
    last.forward_p()
    up_part(around(upd.x, -1), False)
    phase("serve7")
    first.forward_q(-1)
    first.forward_q(1)
    phase("upd_right")
    upd.across(1)
    up_part(around(upd.x, 1), False)
    phase("serve8")
    first.forward_q(2)
    last.near()
    phase("upd_far")
    upd.far()
    up_part(far_chip, False, upd.core)
    phase("upd_last")
    upd.across(2)
    up_part(far_chip, False, 1 - upd.core)
    phase("hidden")
    inv_rms = lax.rsqrt(jnp.sum(squares[...], axis=1, keepdims=True) / (SIDE * depth) + rms_eps)
    active = jnp.maximum(raised[...] * inv_rms, 0.0)
    hidden[:, own_units] = (active * active).astype(bf16)
    crossing.append(cross_copy(2, hidden.at[:, own_units], hidden.at[:, own_units]))
    crossing[2].start()
    phase("serve9")
    last.far()
    last.forward_q(0)
    last.near_rest()
    last.far_rest()

    span = piece // 2
    quarter = half // 2

    chunk = quarter // 2

    def turned(value, by=None):
        return pltpu.roll(value, span // 2 if by is None else by, 1)

    low_lanes = lax.broadcasted_iota(jnp.int32, (chunk, span), 1) < span // 2

    def packed(value, core):
        parts = []
        for c in range(value.shape[0] // quarter):
            top, low = (value[c * quarter + k * chunk : c * quarter + k * chunk + chunk] for k in range(2))
            parts.append(jnp.where(low_lanes, top, turned(low)) if core == 0 else jnp.where(low_lanes, turned(top), low))
        return jnp.concatenate(parts, axis=0)

    class Sum:
        def __init__(self, k, buf):
            self.k, self.buf = k, buf
            self.relays = [
                [
                    self.copy(
                        0, 2 * j + c, stage_far.at[k, j, c * quarter : c * quarter + quarter],
                        relay_in.at[k, j, c * quarter : c * quarter + quarter], target,
                    )
                    for c in range(2)
                ]
                for j, target in enumerate((right, left))
            ]
            self.own = self.copy(1, 4, stage_own.at[k], from_own.at[k], partner)
            self.near = self.copy(2, 5, stage_near.at[k], from_near.at[k], right)

        def copy(self, send, recv, src, dst, target):
            return pltpu.make_async_remote_copy(
                src_ref=src,
                dst_ref=dst,
                send_sem=sum_send.at[self.k, send],
                recv_sem=sum_recv.at[self.k, recv],
                device_id={"sp": here, "tp": target},
                device_id_type=AXES,
            )

        def product(self, dx):
            return products[:, pl.ds(pl.multiple_of(around(mix.x, dx) * span, span), span)]

        def send_near(self, side, part, value, first=0):
            chip = around(mix.x, 1 - 2 * side)
            rows = slice(first, first + value.shape[0] // 2)
            for core in range(2):
                stage_near[self.k, side, core, part, rows] = packed(value, core).astype(bf16)
                self.copy(
                    2, 5, stage_near.at[self.k, side, core, part, rows],
                    from_near.at[self.k, mix.core, side, part, rows], chip * 2 + core,
                ).start()

        def start(self, *serve):
            k = self.k
            products[...] = dot_t(hidden[...], self.buf[...])
            far = self.product(2).astype(bf16)
            for j in range(2):
                stage_far[k, j] = far[j * half : j * half + half]
            for c in range(2):
                for j in range(2):
                    self.relays[j][c].start()
            near = self.product(1)
            self.send_near(0, 1, near[half:])
            kept[k, 0] = near[:half]
            near = self.product(-1)
            self.send_near(1, 0, near[:half])
            kept[k, 1] = near[half:]
            if serve:
                serve[0]()
            own = self.product(0)
            for j in range(2):
                both = [packed(own[j * half : j * half + half], core) for core in range(2)]
                own_part[k, j] = jnp.where(mix.core == 0, both[0], both[1])
                stage_own[k, j] = jnp.where(mix.core == 0, both[1], both[0]).astype(bf16)
            self.own.start()
            if serve:
                serve[1]()

        def relay(self):
            k = self.k
            for c in range(2):
                rows = slice(c * quarter, c * quarter + quarter)
                for j in range(2):
                    self.relays[j][c].wait_recv()
                    self.send_near(j, j, kept[k, j, rows] + relay_in[k, j, rows].astype(f32), c * chunk)

        def result(self):
            k = self.k
            self.own.wait_recv()
            self.near.wait_recv()
            found = []
            for core in range(2):
                rows = []
                for j in range(2):
                    here_part = jnp.where(mix.core == core, own_part[k, j], from_own[k, j].astype(f32))
                    total = here_part + (from_near[k, core, 0, j].astype(f32) + from_near[k, core, 1, j].astype(f32))
                    for c in range(2):
                        part = total[c * chunk : c * chunk + chunk]
                        rows += [part, turned(part)]
                found.append(jnp.concatenate(rows, axis=0))
            return found

        def drain(self):
            self.own.wait_send()
            self.near.wait_send()
            self.copy(0, 0, stage_far.at[self.k], stage_far.at[self.k], right).wait_send()

    phase("first_wait")
    first.finish()
    crossing[2].wait_recv()
    phase("first_sum")
    early, late = Sum(0, down_first), Sum(1, down_last)

    def serve_near():
        last.forward_q(-1)
        last.forward_q(1)

    def serve_far():
        last.forward_q(2)

    early.start(serve_near, serve_far)
    phase("first_relay")
    early.relay()
    phase("last_wait")
    last.finish()
    phase("last_sum")
    late.start()
    phase("last_relay")
    late.relay()
    phase("first_result")
    lane_group = lax.broadcasted_iota(jnp.int32, (tokens, span), 1) // slim
    blocks = [upd_all[upd.x, :, own_cols].astype(f32)[:, b * span : b * span + span] for b in range(2)]

    def put_in(k, found):
        for b in range(2):
            for core in range(2):
                place = core * 2 + k
                moved = turned(found[core], (place - b) % 4 * slim) if place != b else found[core]
                blocks[b] = blocks[b] + jnp.where(lane_group == place, moved, 0.0)

    put_in(0, early.result())
    for b in range(2):
        kept_out[:, b * span : b * span + span] = blocks[b]
    phase("last_result")
    two = late.result()
    phase("result")
    blocks = [kept_out[:, b * span : b * span + span] for b in range(2)]
    put_in(1, two)
    out_ref[...] = jnp.concatenate(blocks, axis=1).astype(bf16)

    phase("drain")
    for count in range(1, planes):
        @pl.when(planes - 1 - here == count)
        def _():
            for k, part in enumerate((totals, totals_x)):
                total_copy(k, part.at[:count], part.at[:count], lax.rem(here + 1, planes)).wait_send()

    for part in (up, first, last, mix, upd, early, late):
        part.drain()
    for copy in crossing:
        copy.wait_send()
    phase(None)


def per_device(
    resid, mixer_in, log_step, decay_real, frequency, input_matrix, output_matrix, skip_gain,
    value_weight, gate_weight, norm_gain, up_weight, down_weight,
):
    tokens, channels = mixer_in.shape
    groups, states = decay_real.shape
    width = groups * states
    planes, slots = lax.axis_size("sp"), lax.axis_size("tp")
    features = slots * channels
    hidden = up_weight.shape[1]
    span = channels // 2
    vmem = pl.BlockSpec(memory_space=pltpu.VMEM)
    hbm = pl.BlockSpec(memory_space=pl.ANY)
    wide = pltpu.VMEM((tokens, width), f32)
    block = pltpu.VMEM((tokens, channels), bf16)
    halves = pltpu.VMEM((2, 2, tokens // 2, span), bf16)
    packs = pltpu.VMEM((2, 2, tokens // 4, span), bf16)
    near = pltpu.VMEM((2, 2, 2, 2, tokens // 4, span), bf16)
    pieces = pltpu.VMEM((SIDE, tokens, 2 * channels), bf16)
    matrix = pltpu.VMEM((2, channels, states), f32)
    down = pltpu.VMEM((features // 4, 2 * hidden), bf16)
    dma = pltpu.SemaphoreType.DMA
    return pl.pallas_call(
        layer_kernel,
        out_shape=pltpu.VMEM((tokens, channels), bf16),
        in_specs=[hbm] * 13,
        out_specs=vmem,
        scratch_shapes=[
            block, block, pltpu.VMEM((groups, tokens), f32),
            pltpu.VMEM((groups, states), f32), pltpu.VMEM((groups, states), f32), matrix, matrix,
            pltpu.VMEM((1, channels), f32), pltpu.VMEM((1, features), f32),
            pltpu.VMEM((features, hidden), bf16), down, down, pltpu.VMEM((features, 2 * channels), bf16),
            wide, wide, wide, wide, wide,
            pltpu.VMEM((8, width), f32), pltpu.VMEM((4, CHUNKS, width), f32),
            pltpu.VMEM((16, 128), f32), pltpu.VMEM((planes, 16, 128), f32),
            pltpu.VMEM((16, 128), bf16), pltpu.VMEM((planes, 16, 128), bf16), pltpu.VMEM((16, 128), f32),
            block, pltpu.VMEM((channels, 2 * width), bf16), pltpu.VMEM((tokens, 2 * width), bf16),
            pieces, pieces, pltpu.VMEM((tokens, 2 * channels), f32),
            pltpu.VMEM((tokens, hidden), f32), pltpu.VMEM((tokens, 128), f32), pltpu.VMEM((tokens, 2 * hidden), bf16),
            pltpu.VMEM((tokens, SIDE * span), f32), halves, halves, near, near, pltpu.VMEM((2, 2, tokens // 2, span), f32),
            packs, packs, pltpu.VMEM((2, 2, tokens // 4, span), f32), pltpu.VMEM((tokens, channels), f32),
            dma((14,)), pltpu.SemaphoreType.REGULAR((3,)), dma((5,)), dma((5, 8)),
            dma((2,)), dma((2,)), dma((3,)), dma((3,)), dma((2, 3)), dma((2, 6)),
        ],
        name="layer",
        compiler_params=pltpu.CompilerParams(
            vmem_limit_bytes=58 * 2**20, collective_id=0, has_side_effects=True
        ),
    )(
        resid, mixer_in, log_step.T, decay_real, frequency,
        input_matrix.transpose(0, 1, 3, 2).reshape(2, channels, states), output_matrix.reshape(2, channels, states),
        skip_gain.reshape(1, -1), norm_gain.reshape(1, -1), value_weight, gate_weight, up_weight, down_weight,
    )


def solution(mesh):
    in_specs = (
        P("sp", "tp"), P("sp", "tp"), P("sp", "tp"), P("tp", None), P("tp", None),
        P(None, "tp", None, None), P(None, "tp", None, None), P("tp"),
        P(None, "tp"), P(None, "tp"), P(), P("sp", "tp"), P("sp", "tp"),
    )
    return jax.shard_map(
        per_device, mesh=mesh, in_specs=in_specs, out_specs=P("sp", "tp"), check_vma=False
    )
```

```python
import functools
import math

import jax
import jax.numpy as jnp
from jax import lax
from jax.experimental import pallas as pl
from jax.experimental.pallas import tpu as pltpu
from jax.sharding import PartitionSpec as P

rms_eps = 1e-06
f32 = jnp.float32
bf16 = jnp.bfloat16
CHUNKS = 8


def onehot(shape, test):
    row = lax.broadcasted_iota(jnp.int32, shape, 0)
    col = lax.broadcasted_iota(jnp.int32, shape, 1)
    return jnp.where(test(row, col), 1.0, 0.0).astype(bf16)


def split3(x):
    hi = x.astype(bf16)
    rest = x - hi.astype(f32)
    mid = rest.astype(bf16)
    return hi, mid, (rest - mid.astype(f32)).astype(bf16)


def dot(a, b):
    return jnp.dot(a, b, preferred_element_type=f32)


def dot_t(a, b):
    return lax.dot_general(a, b, (((1,), (1,)), ((), ())), preferred_element_type=f32)


def spread_row(x, states):
    groups = x.shape[0]
    width = groups * states
    lanes = onehot((states, width), lambda r, c: r == c % states)
    wide = sum(dot(part, lanes) for part in split3(x))
    row = lax.broadcasted_iota(jnp.int32, wide.shape, 0)
    col = lax.broadcasted_iota(jnp.int32, wide.shape, 1)
    return jnp.sum(jnp.where(row == col // states, wide, 0.0), axis=0, keepdims=True)


def prepare(u_ref, ls_ref, dr_ref, fr_ref, bm_ref, cm_ref, uperm, step_wide, proj_re, proj_im, rows, wout):
    tokens, channels = u_ref.shape
    groups, states = dr_ref.shape
    width = groups * states
    per_group = channels // groups
    span = tokens // CHUNKS
    perm = onehot((tokens, tokens), lambda r, c: c == (r % CHUNKS) * span + r // CHUNKS)
    u_sorted = dot(perm, u_ref[...]).astype(bf16)
    uperm[...] = u_sorted
    decay = spread_row(dr_ref[...], states)
    angular = spread_row(fr_ref[...], states)
    rows[0:1, :] = -decay
    rows[1:2, :] = 0.5 * angular
    modulus = decay * decay + angular * angular
    inv_re = -decay / modulus
    inv_im = -angular / modulus
    step = jnp.exp(ls_ref[...])
    step = sum(dot_t(perm, part) for part in split3(step))
    group_lanes = onehot((groups, width), lambda r, c: r == c // states)
    step_wide[...] = sum(dot(part, group_lanes) for part in split3(step))
    state_lanes = onehot((states, width), lambda r, c: r == c % states)
    row = lax.broadcasted_iota(jnp.int32, (channels, width), 0)
    col = lax.broadcasted_iota(jnp.int32, (channels, width), 1)
    same = row // per_group == col // states
    b_re = dot(bm_ref[0].astype(bf16), state_lanes)
    b_im = dot(bm_ref[1].astype(bf16), state_lanes)
    w_re = jnp.where(same, b_re * inv_re - b_im * inv_im, 0.0).astype(bf16)
    w_im = jnp.where(same, b_re * inv_im + b_im * inv_re, 0.0).astype(bf16)
    proj_re[...] = dot(u_sorted, w_re)
    proj_im[...] = dot(u_sorted, w_im)
    wout[:, :width] = jnp.where(same, dot(cm_ref[0].astype(bf16), state_lanes), 0.0).astype(bf16)
    wout[:, width:] = jnp.where(same, -dot(cm_ref[1].astype(bf16), state_lanes), 0.0).astype(bf16)


SIN = (-1.0 / 6, 1.0 / 120, -1.0 / 5040, 1.0 / 362880, -1.0 / 39916800)
COS = (-0.5, 1.0 / 24, -1.0 / 720, 1.0 / 40320, -1.0 / 3628800)


def series(q, terms):
    total = terms[-1] * q
    for term in terms[-2::-1]:
        total = (total + term) * q
    return total


def first_pass(step_wide, proj_re, proj_im, rows, dec_re, dec_im, ends, first, last):
    tokens, width = step_wide.shape
    block = 256

    def one_block(b, _):
        lanes = pl.ds(pl.multiple_of(b * block, block), block)
        minus_decay = jnp.broadcast_to(rows[0:1, lanes], (CHUNKS, block))
        half_angular = jnp.broadcast_to(rows[1:2, lanes], (CHUNKS, block))

        def one_step(i, carry):
            a_re, a_im, x_re, x_im = carry
            at = pl.ds(pl.multiple_of(i * CHUNKS, CHUNKS), CHUNKS)
            step = step_wide[at, lanes]
            half = step * half_angular
            q = half * half
            sine = half + half * series(q, SIN)
            cosine = 1.0 + series(q, COS)
            factor = jnp.exp(step * minus_decay)
            twice = factor * (sine + sine)
            d_re = factor - twice * sine
            d_im = twice * cosine
            less = d_re - 1.0
            p_re = proj_re[at, lanes]
            p_im = proj_im[at, lanes]
            u_re = less * p_re - d_im * p_im
            u_im = less * p_im + d_im * p_re
            dec_re[at, lanes] = d_re
            dec_im[at, lanes] = d_im
            proj_re[at, lanes] = u_re
            proj_im[at, lanes] = u_im
            return (
                d_re * a_re - d_im * a_im,
                d_re * a_im + d_im * a_re,
                d_re * x_re - d_im * x_im + u_re,
                d_re * x_im + d_im * x_re + u_im,
            )

        zero = jnp.zeros((CHUNKS, block), f32)
        found = lax.fori_loop(0, tokens // CHUNKS, one_step, (zero + 1.0, zero, zero, zero), unroll=2)
        for k in range(4):
            ends[k, :, lanes] = found[k]
        return 0

    lax.fori_loop(first, last, one_block, 0)


def chain(early, late):
    return (
        early[0] * late[0] - early[1] * late[1],
        early[0] * late[1] + early[1] * late[0],
        late[0] * early[2] - late[1] * early[3] + late[2],
        late[0] * early[3] + late[1] * early[2] + late[3],
    )


def chunk_prefix(ends, total, total_x, wide_x):
    width = ends.shape[2]
    value = tuple(ends[k] for k in range(4))
    row = lax.broadcasted_iota(jnp.int32, value[0].shape, 0)
    unit = (1.0, 0.0, 0.0, 0.0)

    def moved(value, by):
        return tuple(
            jnp.where(row >= by, pltpu.roll(part, by, 0), zero) for part, zero in zip(value, unit)
        )

    for by in (1, 2, 4):
        value = chain(moved(value, by), value)
    for k in range(4):
        for j in range(width // 128):
            kept = total if k < 2 else wide_x
            at = 8 * (k % 2) + j
            kept[at : at + 1, :] = value[k][CHUNKS - 1 :, 128 * j : 128 * j + 128]
    total_x[...] = wide_x[...].astype(bf16)
    before = moved(value, 1)
    for k in range(4):
        ends[k] = before[k]


def second_pass(dec_re, dec_im, feed_re, feed_im, ends, carry, states):
    tokens, width = dec_re.shape
    block = 512
    for b in range(width // block):
        lanes = pl.ds(b * block, block)
        lanes_im = pl.ds(width + b * block, block)
        per = block // 128
        h_re = jnp.concatenate([carry[per * b + j : per * b + j + 1, :] for j in range(per)], axis=1)
        h_im = jnp.concatenate([carry[8 + per * b + j : 9 + per * b + j, :] for j in range(per)], axis=1)
        a_re, a_im = ends[0, :, lanes], ends[1, :, lanes]
        x_re = ends[2, :, lanes] + a_re * h_re - a_im * h_im
        x_im = ends[3, :, lanes] + a_re * h_im + a_im * h_re

        def one_step(i, value):
            x_re, x_im = value
            seen = []
            for k in range(2):
                at = pl.ds(pl.multiple_of(i * 2 * CHUNKS + k * CHUNKS, CHUNKS), CHUNKS)
                d_re, d_im = dec_re[at, lanes], dec_im[at, lanes]
                x_re, x_im = (
                    d_re * x_re - d_im * x_im + feed_re[at, lanes],
                    d_re * x_im + d_im * x_re + feed_im[at, lanes],
                )
                seen.append((x_re, x_im))
            both = pl.ds(pl.multiple_of(i * 2 * CHUNKS, 2 * CHUNKS), 2 * CHUNKS)
            states[both, lanes] = jnp.concatenate([seen[0][0], seen[1][0]], axis=0).astype(bf16)
            states[both, lanes_im] = jnp.concatenate([seen[0][1], seen[1][1]], axis=0).astype(bf16)
            return x_re, x_im

        lax.fori_loop(0, tokens // (2 * CHUNKS), one_step, (x_re, x_im), unroll=2)


def read_out(states, wout, uperm, skip_ref):
    tokens = states.shape[0]
    span = tokens // CHUNKS
    out = dot_t(states[...], wout[...]) + skip_ref[...] * uperm[...].astype(f32)
    mixed = jax.nn.gelu(out).astype(bf16)
    back = onehot((tokens, tokens), lambda r, c: r == (c % CHUNKS) * span + c // CHUNKS)
    return dot(back, mixed).astype(bf16)


AXES = pl.DeviceIdType.MESH
SIDE = 4


def around(index, by):
    return lax.rem(index + by + SIDE, SIDE)


class Relay:
    def __init__(self, buf, first, rows, send_sem, recv_sem, own=None):
        here = lax.axis_index("sp")
        self.zy = here // SIDE, lax.rem(here, SIDE)
        self.buf, self.first, self.rows, self.own = buf, first, rows, own
        self.shard = buf.shape[0] // (SIDE * SIDE)
        self.send_sem, self.recv_sem = send_sem, recv_sem
        self.sent = 0

    def index(self, side, dp, dq):
        dz, dy = (dq, dp) if side == 0 else (dp, dq)
        return around(self.zy[0], dz) * SIDE + around(self.zy[1], dy)

    def group(self, dp, dq, half):
        if dq == 0:
            return 2 if dp == 2 else int((dp == -1) == (half == 1))
        return 3 + dp % SIDE if dq != 2 and (dq == -1) == (half == 0) else 7

    def send(self, side, dp, dq, half, to_p, to_q):
        width = self.buf.shape[1] // 2
        cols = slice(half * width, half * width + width)
        row = pl.multiple_of(self.index(side, dp, dq) * self.shard + side * self.rows, self.rows)
        piece = self.buf.at[pl.ds(row, self.rows), cols]
        own = self.own is not None and dp == 0 and dq == 0
        first = self.first + side * self.rows
        seen = [(d + 1) % SIDE - 1 for d in (dp - to_p, dq - to_q)]
        pltpu.make_async_remote_copy(
            src_ref=self.own.at[first : first + self.rows, cols] if own else piece,
            dst_ref=piece,
            send_sem=self.send_sem,
            recv_sem=self.recv_sem.at[self.group(*seen, half)],
            device_id={"sp": self.index(side, to_p, to_q), "tp": lax.axis_index("tp")},
            device_id_type=AXES,
        ).start()
        self.sent += 1

    def whole(self, count, group):
        rows = self.buf.at[: count * self.rows // 2, :]
        return pltpu.make_async_remote_copy(
            src_ref=rows,
            dst_ref=rows,
            send_sem=self.send_sem,
            recv_sem=self.recv_sem.at[group],
            device_id={"sp": self.index(0, 1, 0), "tp": lax.axis_index("tp")},
            device_id_type=AXES,
        )

    def arrived(self, group):
        self.whole(32 if group == 7 else 4, group).wait_recv()

    def send_p(self, k):
        for side in range(2):
            self.send(side, 0, 0, k, 1, 0)
            self.send(side, 0, 0, 1 - k, -1, 0)

    def send_q(self, dp, k):
        for side in range(2):
            self.send(side, dp, 0, k, 0, 1)
            self.send(side, dp, 0, 1 - k, 0, -1)

    def forward_p(self):
        self.arrived(0)
        for side in range(2):
            self.send(side, -1, 0, 0, 1, 0)
            self.send(side, 1, 0, 1, -1, 0)

    def near(self):
        self.arrived(1)
        self.send_q(-1, 0)
        self.send_q(1, 0)

    def near_rest(self):
        self.send_q(-1, 1)
        self.send_q(1, 1)

    def far(self):
        self.arrived(2)
        self.send_q(2, 0)

    def far_rest(self):
        self.send_q(2, 1)

    def forward_q(self, dp):
        self.arrived(3 + dp % SIDE)
        for side in range(2):
            self.send(side, dp, -1, 0, 0, 1)
            self.send(side, dp, 1, 1, 0, -1)

    def finish(self):
        self.arrived(7)

    def drain(self):
        self.whole(self.sent, 0).wait_send()


class Gather:
    def __init__(self, buf, send_sem, recv_sem):
        here = lax.axis_index("tp")
        self.x, self.core = here // 2, lax.rem(here, 2)
        self.buf, self.send_sem, self.recv_sem = buf, send_sem, recv_sem
        self.sent = 0

    def device(self, dx, other=False):
        return around(self.x, dx) * 2 + (1 - self.core if other else self.core)

    def cols(self, core):
        width = self.buf.shape[2] // 2
        return pl.ds(pl.multiple_of(core * width, width), width)

    def send(self, dx, half, to_x):
        rows = self.buf.shape[1] // 2
        piece = self.buf.at[around(self.x, dx), half * rows : half * rows + rows, self.cols(self.core)]
        if to_x:
            seen = (dx - to_x + 1) % SIDE - 1
            group = 2 if seen == 2 else int((seen == -1) == (half == 1))
        else:
            group = 3 + dx % SIDE
        pltpu.make_async_remote_copy(
            src_ref=piece,
            dst_ref=piece,
            send_sem=self.send_sem,
            recv_sem=self.recv_sem.at[group],
            device_id={"sp": lax.axis_index("sp"), "tp": self.device(to_x, not to_x)},
            device_id_type=AXES,
        ).start()
        self.sent += 1

    def whole(self, rows, group):
        return pltpu.make_async_remote_copy(
            src_ref=rows,
            dst_ref=rows,
            send_sem=self.send_sem,
            recv_sem=self.recv_sem.at[group],
            device_id={"sp": lax.axis_index("sp"), "tp": self.device(1)},
            device_id_type=AXES,
        )

    def arrived(self, group):
        self.whole(self.buf.at[0, :, : self.buf.shape[2] // 2], group).wait_recv()

    def start(self):
        for k in range(2):
            self.send(0, k, 1)
            self.send(0, 1 - k, -1)
        for k in range(2):
            self.send(0, k, 0)

    def near(self):
        self.arrived(0)
        self.send(-1, 0, 1)
        self.send(1, 1, -1)
        self.send(-1, 0, 0)
        self.send(1, 1, 0)
        self.arrived(1)
        self.send(-1, 1, 0)
        self.send(1, 0, 0)

    def far(self):
        self.arrived(2)
        self.send(2, 0, 0)
        self.send(2, 1, 0)

    def across(self, dx):
        self.arrived(3 + dx % SIDE)

    def drain(self):
        self.whole(self.buf.at[:, : self.buf.shape[1] * self.sent // 16, :], 0).wait_send()


class Phases:
    def __init__(self):
        self.scope = None

    def __call__(self, name):
        if self.scope is not None:
            self.scope.__exit__(None, None, None)
        self.scope = jax.named_scope(name) if name else None
        if self.scope is not None:
            self.scope.__enter__()


def layer_kernel(
    resid_hbm, u_hbm, ls_hbm, dr_hbm, fr_hbm, bm_hbm, cm_hbm, skip_hbm, gain_hbm, vw_ref, gw_ref, up_ref, down_ref,
    out_ref,
    resid_ref, u_ref, ls_ref, dr_ref, fr_ref, bm_ref, cm_ref, skip_ref, gain_ref,
    up_all, down_first, down_last, vg, dec_re, dec_im, feed_re, feed_im, step_wide, rows, ends, total, totals, total_x, totals_x, carry,
    uperm, wout, states, mixed_all, upd_all, glu, raised, squares, hidden,
    products, stage_far, relay_in, stage_near, from_near, kept, stage_own, from_own, own_part, kept_out,
    local_sem, round_sem, ring_send, ring_recv, tot_send, tot_recv, cross_send, cross_recv, sum_send, sum_recv,
):
    phase = Phases()
    here, lane = lax.axis_index("sp"), lax.axis_index("tp")
    planes = SIDE * SIDE
    tokens, piece = resid_ref.shape
    half = tokens // 2
    shard = up_ref.shape[0]
    mix = Gather(mixed_all, ring_send.at[3], ring_recv.at[3])
    upd = Gather(upd_all, ring_send.at[4], ring_recv.at[4])
    right, left, partner = mix.device(1), mix.device(-1), mix.device(0, True)

    up = Relay(up_all, 0, shard // 2, ring_send.at[0], ring_recv.at[0], up_ref)
    first = Relay(down_first, 0, shard // 8, ring_send.at[1], ring_recv.at[1])
    last = Relay(down_last, 0, shard // 8, ring_send.at[2], ring_recv.at[2])
    near_planes = [up.index(0, *by) for by in ((1, 0), (-1, 0), (0, 1), (0, -1))]

    phase("signal")
    barrier = pltpu.get_barrier_semaphore()
    for target in near_planes:
        pl.semaphore_signal(barrier, inc=1, device_id={"sp": target, "tp": lane}, device_id_type=AXES)
    for target in (right, left, partner):
        pl.semaphore_signal(barrier, inc=1, device_id={"sp": here, "tp": target}, device_id_type=AXES)

    own_up = pl.ds(pl.multiple_of(here * shard, shard), shard)
    slim, width = shard // 4, up_ref.shape[1]
    own_down = pl.ds(pl.multiple_of(here * slim, slim), slim)
    own_units = pl.ds(pl.multiple_of(mix.core * width, width), width)

    def down_rows(core, k):
        return down_ref.at[pl.ds(pl.multiple_of(core * 2 * slim + k * slim, slim), slim), :]

    def cross_copy(number, src, dst):
        return pltpu.make_async_remote_copy(
            src_ref=src,
            dst_ref=dst,
            send_sem=cross_send.at[number],
            recv_sem=cross_recv.at[number],
            device_id={"sp": here, "tp": partner},
            device_id_type=AXES,
        )

    crossing = [
        cross_copy(k, down_rows(1 - mix.core, k), buf.at[own_down, own_units])
        for k, buf in enumerate((down_first, down_last))
    ]
    moves = (
        (u_hbm, u_ref), (dr_hbm, dr_ref), (fr_hbm, fr_ref), (ls_hbm, ls_ref), (bm_hbm, bm_ref), (cm_hbm, cm_ref),
        (up_ref, up_all.at[own_up, :]),
        (down_rows(mix.core, 0), down_first.at[own_down, own_units]),
        (down_rows(mix.core, 1), down_last.at[own_down, own_units]),
        (skip_hbm, skip_ref), (vw_ref, vg.at[:, :piece]), (gw_ref, vg.at[:, piece:]),
        (resid_hbm, resid_ref), (gain_hbm, gain_ref),
    )
    local = [pltpu.make_async_copy(src, dst, local_sem.at[k]) for k, (src, dst) in enumerate(moves)]
    for copy in local:
        copy.start()
    phase("barrier")
    pl.semaphore_wait(barrier, 7)
    phase("start_p")
    up.send_p(0)
    up.send_p(1)
    up.send_q(0, 0)
    up.send_q(0, 1)
    for copy in crossing:
        copy.start()

    def greet(number):
        for target in near_planes:
            pl.semaphore_signal(
                round_sem.at[number], inc=1, device_id={"sp": target, "tp": lane}, device_id_type=AXES
            )

    greet(0)
    for copy in local[:6]:
        copy.wait()
    phase("prepare")
    prepare(u_ref, ls_ref, dr_ref, fr_ref, bm_ref, cm_ref, uperm, step_wide, feed_re, feed_im, rows, wout)
    pl.semaphore_wait(round_sem.at[0], 4)
    greet(1)
    phase("first_pass")
    scan_refs = (step_wide, feed_re, feed_im, rows, dec_re, dec_im, ends)
    first_pass(*scan_refs, 0, 2)
    pl.semaphore_wait(round_sem.at[1], 4)
    greet(2)
    for copy in local[6:9]:
        copy.wait()
    for copy in crossing:
        copy.wait_recv()
    first.send_p(0)
    first_pass(*scan_refs, 2, 4)
    phase("chunk")
    chunk_prefix(ends, total, total_x, carry)
    pl.semaphore_wait(round_sem.at[2], 4)

    def total_copy(k, src, dst, target):
        return pltpu.make_async_remote_copy(
            src_ref=src,
            dst_ref=dst,
            send_sem=tot_send.at[k],
            recv_sem=tot_recv.at[k],
            device_id={"sp": target, "tp": lane},
            device_id_type=AXES,
        )

    phase("totals")
    for by in range(1, planes):
        @pl.when(here + by < planes)
        def _():
            for k, (src, dst) in enumerate(((total, totals), (total_x, totals_x))):
                total_copy(k, src, dst.at[here], lax.rem(here + by, planes)).start()

    phase("serve1")
    up.forward_p()
    up.near()
    up.forward_q(0)
    up.near_rest()

    phase("fold")

    for count in range(1, planes):
        @pl.when(here == count)
        def _():
            for k, part in enumerate((totals, totals_x)):
                total_copy(k, part.at[:count], part.at[:count], lax.rem(here + 1, planes)).wait_recv()

    def fold(j, value):
        h_re, h_im = value
        a_re, a_im = totals[j, 0:8, :], totals[j, 8:16, :]
        x_both = totals_x[j].astype(f32)
        x_re, x_im = x_both[0:8], x_both[8:16]
        return a_re * h_re - a_im * h_im + x_re, a_re * h_im + a_im * h_re + x_im

    zero = jnp.zeros((8, 128), f32)
    h_re, h_im = lax.fori_loop(0, here, fold, (zero, zero))
    carry[0:8, :] = h_re
    carry[8:16, :] = h_im
    phase("second_pass")
    second_pass(dec_re, dec_im, feed_re, feed_im, ends, carry, states)
    phase("serve2")
    up.far()
    up.far_rest()
    first.send_p(1)
    local[9].wait()
    phase("read_out")
    own_cols = mix.cols(mix.core)
    mixed_all[mix.x, :, own_cols] = read_out(states, wout, uperm, skip_ref)
    phase("mix_start")
    mix.start()

    depth = 2 * piece

    def glu_part(chip, core=None):
        if core is None:
            lhs, at = mixed_all[chip], pl.ds(pl.multiple_of(chip * depth, depth), depth)
        else:
            lhs, at = mixed_all[chip, :, mix.cols(core)], pl.ds(pl.multiple_of((chip * 2 + core) * piece, piece), piece)
        return dot(lhs, vg[at, :])

    phase("mix_own")
    for copy in local[10:]:
        copy.wait()
    mix.across(0)
    glu[...] = glu_part(mix.x)
    phase("serve3")
    up.forward_q(-1)
    up.forward_q(1)
    first.send_q(0, 0)
    first.send_q(0, 1)
    phase("mix_near")
    mix.near()
    phase("serve4")
    up.forward_q(2)
    phase("mix_left")
    mix.across(-1)
    glu[...] += glu_part(around(mix.x, -1))
    phase("mix_right")
    mix.across(1)
    glu[...] += glu_part(around(mix.x, 1))
    phase("mix_far")
    mix.far()
    phase("mix_last")
    far_chip = around(mix.x, 2)
    glu[...] += glu_part(far_chip, mix.core)
    mix.across(2)
    glu[...] += glu_part(far_chip, 1 - mix.core)
    phase("updated")
    updated = (resid_ref[...].astype(f32) + glu[:, :piece] * jax.nn.sigmoid(glu[:, piece:])).astype(bf16)
    upd_all[upd.x, :, own_cols] = updated
    phase("upd_start")
    upd.start()
    phase("serve5")
    first.forward_p()
    first.near()
    first.near_rest()
    last.send_p(0)
    last.send_p(1)

    def up_part(chip, start, core=None):
        if core is None:
            wide, at = upd_all[chip], pl.ds(pl.multiple_of(chip * depth, depth), depth)
        else:
            wide, at = upd_all[chip, :, upd.cols(core)], pl.ds(pl.multiple_of((chip * 2 + core) * piece, piece), piece)
        wide = wide.astype(f32)
        square = wide * wide
        square = sum(square[:, 128 * k : 128 * k + 128] for k in range(square.shape[1] // 128))
        product = dot((wide * gain_ref[:, at]).astype(bf16), up_all[at, :])
        if start:
            squares[...] = square
            raised[...] = product
        else:
            squares[...] += square
            raised[...] += product

    phase("up_wait")
    up.finish()
    phase("upd_own")
    upd.across(0)
    up_part(upd.x, True)
    phase("serve6")
    first.forward_q(0)
    first.far()
    last.send_q(0, 0)
    first.far_rest()
    last.send_q(0, 1)
    phase("upd_near")
    upd.near()
    phase("upd_left")
    upd.across(-1)
    last.forward_p()
    up_part(around(upd.x, -1), False)
    phase("serve7")
    first.forward_q(-1)
    first.forward_q(1)
    phase("upd_right")
    upd.across(1)
    up_part(around(upd.x, 1), False)
    phase("serve8")
    first.forward_q(2)
    last.near()
    last.send_q(-1, 1)
    phase("upd_far")
    upd.far()
    up_part(far_chip, False, upd.core)
    phase("upd_last")
    upd.across(2)
    up_part(far_chip, False, 1 - upd.core)
    phase("hidden")
    inv_rms = lax.rsqrt(jnp.sum(squares[...], axis=1, keepdims=True) / (SIDE * depth) + rms_eps)
    active = jnp.maximum(raised[...] * inv_rms, 0.0)
    hidden[:, own_units] = (active * active).astype(bf16)
    crossing.append(cross_copy(2, hidden.at[:, own_units], hidden.at[:, own_units]))
    crossing[2].start()
    phase("serve9")
    last.far()
    last.forward_q(0)
    last.send_q(1, 1)
    last.far_rest()

    span = piece // 2
    quarter = half // 2

    chunk = quarter // 2

    def turned(value, by=None):
        return pltpu.roll(value, span // 2 if by is None else by, 1)

    low_lanes = lax.broadcasted_iota(jnp.int32, (chunk, span), 1) < span // 2

    def packed(value, core):
        parts = []
        for c in range(value.shape[0] // quarter):
            top, low = (value[c * quarter + k * chunk : c * quarter + k * chunk + chunk] for k in range(2))
            parts.append(jnp.where(low_lanes, top, turned(low)) if core == 0 else jnp.where(low_lanes, turned(top), low))
        return jnp.concatenate(parts, axis=0)

    class Sum:
        def __init__(self, k, buf):
            self.k, self.buf = k, buf
            self.relays = [
                [
                    self.copy(
                        0, 2 * j + c, stage_far.at[k, j, c * quarter : c * quarter + quarter],
                        relay_in.at[k, j, c * quarter : c * quarter + quarter], target,
                    )
                    for c in range(2)
                ]
                for j, target in enumerate((right, left))
            ]
            self.own = self.copy(1, 4, stage_own.at[k], from_own.at[k], partner)
            self.near = self.copy(2, 5, stage_near.at[k], from_near.at[k], right)

        def copy(self, send, recv, src, dst, target):
            return pltpu.make_async_remote_copy(
                src_ref=src,
                dst_ref=dst,
                send_sem=sum_send.at[self.k, send],
                recv_sem=sum_recv.at[self.k, recv],
                device_id={"sp": here, "tp": target},
                device_id_type=AXES,
            )

        def product(self, dx):
            return products[:, pl.ds(pl.multiple_of(around(mix.x, dx) * span, span), span)]

        def send_near(self, side, part, value, first=0):
            chip = around(mix.x, 1 - 2 * side)
            rows = slice(first, first + value.shape[0] // 2)
            for core in range(2):
                stage_near[self.k, side, core, part, rows] = packed(value, core).astype(bf16)
                self.copy(
                    2, 5, stage_near.at[self.k, side, core, part, rows],
                    from_near.at[self.k, mix.core, side, part, rows], chip * 2 + core,
                ).start()

        def start(self, *serve):
            k = self.k
            products[...] = dot_t(hidden[...], self.buf[...])
            far = self.product(2).astype(bf16)
            for j in range(2):
                stage_far[k, j] = far[j * half : j * half + half]
            for c in range(2):
                for j in range(2):
                    self.relays[j][c].start()
            near = self.product(1)
            self.send_near(0, 1, near[half:])
            kept[k, 0] = near[:half]
            near = self.product(-1)
            self.send_near(1, 0, near[:half])
            kept[k, 1] = near[half:]
            if serve:
                serve[0]()
            own = self.product(0)
            for j in range(2):
                both = [packed(own[j * half : j * half + half], core) for core in range(2)]
                own_part[k, j] = jnp.where(mix.core == 0, both[0], both[1])
                stage_own[k, j] = jnp.where(mix.core == 0, both[1], both[0]).astype(bf16)
            self.own.start()
            if serve:
                serve[1]()

        def relay(self):
            k = self.k
            for c in range(2):
                rows = slice(c * quarter, c * quarter + quarter)
                for j in range(2):
                    self.relays[j][c].wait_recv()
                    self.send_near(j, j, kept[k, j, rows] + relay_in[k, j, rows].astype(f32), c * chunk)

        def result(self):
            k = self.k
            self.own.wait_recv()
            self.near.wait_recv()
            found = []
            for core in range(2):
                rows = []
                for j in range(2):
                    here_part = jnp.where(mix.core == core, own_part[k, j], from_own[k, j].astype(f32))
                    total = here_part + (from_near[k, core, 0, j].astype(f32) + from_near[k, core, 1, j].astype(f32))
                    for c in range(2):
                        part = total[c * chunk : c * chunk + chunk]
                        rows += [part, turned(part)]
                found.append(jnp.concatenate(rows, axis=0))
            return found

        def drain(self):
            self.own.wait_send()
            self.near.wait_send()
            self.copy(0, 0, stage_far.at[self.k], stage_far.at[self.k], right).wait_send()

    phase("first_wait")
    first.finish()
    crossing[2].wait_recv()
    phase("first_sum")
    early, late = Sum(0, down_first), Sum(1, down_last)

    def serve_near():
        last.forward_q(-1)
        last.forward_q(1)

    def serve_far():
        last.forward_q(2)

    early.start(serve_near, serve_far)
    phase("first_relay")
    early.relay()
    phase("last_wait")
    last.finish()
    phase("last_sum")
    late.start()
    phase("last_relay")
    late.relay()
    phase("first_result")
    lane_group = lax.broadcasted_iota(jnp.int32, (tokens, span), 1) // slim
    blocks = [upd_all[upd.x, :, own_cols].astype(f32)[:, b * span : b * span + span] for b in range(2)]

    def put_in(k, found):
        for b in range(2):
            for core in range(2):
                place = core * 2 + k
                moved = turned(found[core], (place - b) % 4 * slim) if place != b else found[core]
                blocks[b] = blocks[b] + jnp.where(lane_group == place, moved, 0.0)

    put_in(0, early.result())
    for b in range(2):
        kept_out[:, b * span : b * span + span] = blocks[b]
    phase("last_result")
    two = late.result()
    phase("result")
    blocks = [kept_out[:, b * span : b * span + span] for b in range(2)]
    put_in(1, two)
    out_ref[...] = jnp.concatenate(blocks, axis=1).astype(bf16)

    phase("drain")
    for count in range(1, planes):
        @pl.when(planes - 1 - here == count)
        def _():
            for k, part in enumerate((totals, totals_x)):
                total_copy(k, part.at[:count], part.at[:count], lax.rem(here + 1, planes)).wait_send()

    for part in (up, first, last, mix, upd, early, late):
        part.drain()
    for copy in crossing:
        copy.wait_send()
    phase(None)


def per_device(
    resid, mixer_in, log_step, decay_real, frequency, input_matrix, output_matrix, skip_gain,
    value_weight, gate_weight, norm_gain, up_weight, down_weight,
):
    tokens, channels = mixer_in.shape
    groups, states = decay_real.shape
    width = groups * states
    planes, slots = lax.axis_size("sp"), lax.axis_size("tp")
    features = slots * channels
    hidden = up_weight.shape[1]
    span = channels // 2
    vmem = pl.BlockSpec(memory_space=pltpu.VMEM)
    hbm = pl.BlockSpec(memory_space=pl.ANY)
    wide = pltpu.VMEM((tokens, width), f32)
    block = pltpu.VMEM((tokens, channels), bf16)
    halves = pltpu.VMEM((2, 2, tokens // 2, span), bf16)
    packs = pltpu.VMEM((2, 2, tokens // 4, span), bf16)
    near = pltpu.VMEM((2, 2, 2, 2, tokens // 4, span), bf16)
    pieces = pltpu.VMEM((SIDE, tokens, 2 * channels), bf16)
    matrix = pltpu.VMEM((2, channels, states), f32)
    down = pltpu.VMEM((features // 4, 2 * hidden), bf16)
    dma = pltpu.SemaphoreType.DMA
    return pl.pallas_call(
        layer_kernel,
        out_shape=pltpu.VMEM((tokens, channels), bf16),
        in_specs=[hbm] * 13,
        out_specs=vmem,
        scratch_shapes=[
            block, block, pltpu.VMEM((groups, tokens), f32),
            pltpu.VMEM((groups, states), f32), pltpu.VMEM((groups, states), f32), matrix, matrix,
            pltpu.VMEM((1, channels), f32), pltpu.VMEM((1, features), f32),
            pltpu.VMEM((features, hidden), bf16), down, down, pltpu.VMEM((features, 2 * channels), bf16),
            wide, wide, wide, wide, wide,
            pltpu.VMEM((8, width), f32), pltpu.VMEM((4, CHUNKS, width), f32),
            pltpu.VMEM((16, 128), f32), pltpu.VMEM((planes, 16, 128), f32),
            pltpu.VMEM((16, 128), bf16), pltpu.VMEM((planes, 16, 128), bf16), pltpu.VMEM((16, 128), f32),
            block, pltpu.VMEM((channels, 2 * width), bf16), pltpu.VMEM((tokens, 2 * width), bf16),
            pieces, pieces, pltpu.VMEM((tokens, 2 * channels), f32),
            pltpu.VMEM((tokens, hidden), f32), pltpu.VMEM((tokens, 128), f32), pltpu.VMEM((tokens, 2 * hidden), bf16),
            pltpu.VMEM((tokens, SIDE * span), f32), halves, halves, near, near, pltpu.VMEM((2, 2, tokens // 2, span), f32),
            packs, packs, pltpu.VMEM((2, 2, tokens // 4, span), f32), pltpu.VMEM((tokens, channels), f32),
            dma((14,)), pltpu.SemaphoreType.REGULAR((3,)), dma((5,)), dma((5, 8)),
            dma((2,)), dma((2,)), dma((3,)), dma((3,)), dma((2, 3)), dma((2, 6)),
        ],
        name="layer",
        compiler_params=pltpu.CompilerParams(
            vmem_limit_bytes=58 * 2**20, collective_id=0, has_side_effects=True
        ),
    )(
        resid, mixer_in, log_step.T, decay_real, frequency,
        input_matrix.transpose(0, 1, 3, 2).reshape(2, channels, states), output_matrix.reshape(2, channels, states),
        skip_gain.reshape(1, -1), norm_gain.reshape(1, -1), value_weight, gate_weight, up_weight, down_weight,
    )


def solution(mesh):
    in_specs = (
        P("sp", "tp"), P("sp", "tp"), P("sp", "tp"), P("tp", None), P("tp", None),
        P(None, "tp", None, None), P(None, "tp", None, None), P("tp"),
        P(None, "tp"), P(None, "tp"), P(), P("sp", "tp"), P("sp", "tp"),
    )
    return jax.shard_map(
        per_device, mesh=mesh, in_specs=in_specs, out_specs=P("sp", "tp"), check_vma=False
    )
```

```python
import functools
import math

import jax
import jax.numpy as jnp
from jax import lax
from jax.experimental import pallas as pl
from jax.experimental.pallas import tpu as pltpu
from jax.sharding import PartitionSpec as P

rms_eps = 1e-06
f32 = jnp.float32
bf16 = jnp.bfloat16
CHUNKS = 8


def onehot(shape, test):
    row = lax.broadcasted_iota(jnp.int32, shape, 0)
    col = lax.broadcasted_iota(jnp.int32, shape, 1)
    return jnp.where(test(row, col), 1.0, 0.0).astype(bf16)


def split3(x):
    hi = x.astype(bf16)
    rest = x - hi.astype(f32)
    mid = rest.astype(bf16)
    return hi, mid, (rest - mid.astype(f32)).astype(bf16)


def dot(a, b):
    return jnp.dot(a, b, preferred_element_type=f32)


def dot_t(a, b):
    return lax.dot_general(a, b, (((1,), (1,)), ((), ())), preferred_element_type=f32)


def spread_row(x, states):
    groups = x.shape[0]
    width = groups * states
    lanes = onehot((states, width), lambda r, c: r == c % states)
    wide = sum(dot(part, lanes) for part in split3(x))
    row = lax.broadcasted_iota(jnp.int32, wide.shape, 0)
    col = lax.broadcasted_iota(jnp.int32, wide.shape, 1)
    return jnp.sum(jnp.where(row == col // states, wide, 0.0), axis=0, keepdims=True)


def prepare(u_ref, ls_ref, dr_ref, fr_ref, bm_ref, cm_ref, uperm, step_wide, proj_re, proj_im, rows, wout):
    tokens, channels = u_ref.shape
    groups, states = dr_ref.shape
    width = groups * states
    per_group = channels // groups
    span = tokens // CHUNKS
    perm = onehot((tokens, tokens), lambda r, c: c == (r % CHUNKS) * span + r // CHUNKS)
    u_sorted = dot(perm, u_ref[...]).astype(bf16)
    uperm[...] = u_sorted
    decay = spread_row(dr_ref[...], states)
    angular = spread_row(fr_ref[...], states)
    rows[0:1, :] = -decay
    rows[1:2, :] = 0.5 * angular
    modulus = decay * decay + angular * angular
    inv_re = -decay / modulus
    inv_im = -angular / modulus
    step = jnp.exp(ls_ref[...])
    step = sum(dot_t(perm, part) for part in split3(step))
    group_lanes = onehot((groups, width), lambda r, c: r == c // states)
    step_wide[...] = sum(dot(part, group_lanes) for part in split3(step))
    state_lanes = onehot((states, width), lambda r, c: r == c % states)
    row = lax.broadcasted_iota(jnp.int32, (channels, width), 0)
    col = lax.broadcasted_iota(jnp.int32, (channels, width), 1)
    same = row // per_group == col // states
    b_re = dot(bm_ref[0].astype(bf16), state_lanes)
    b_im = dot(bm_ref[1].astype(bf16), state_lanes)
    w_re = jnp.where(same, b_re * inv_re - b_im * inv_im, 0.0).astype(bf16)
    w_im = jnp.where(same, b_re * inv_im + b_im * inv_re, 0.0).astype(bf16)
    proj_re[...] = dot(u_sorted, w_re)
    proj_im[...] = dot(u_sorted, w_im)
    wout[:, :width] = jnp.where(same, dot(cm_ref[0].astype(bf16), state_lanes), 0.0).astype(bf16)
    wout[:, width:] = jnp.where(same, -dot(cm_ref[1].astype(bf16), state_lanes), 0.0).astype(bf16)


SIN = (-1.0 / 6, 1.0 / 120, -1.0 / 5040, 1.0 / 362880, -1.0 / 39916800)
COS = (-0.5, 1.0 / 24, -1.0 / 720, 1.0 / 40320, -1.0 / 3628800)


def series(q, terms):
    total = terms[-1] * q
    for term in terms[-2::-1]:
        total = (total + term) * q
    return total


def first_pass(step_wide, proj_re, proj_im, rows, dec_re, dec_im, ends, first, last):
    tokens, width = step_wide.shape
    block = 256

    def one_block(b, _):
        lanes = pl.ds(pl.multiple_of(b * block, block), block)
        minus_decay = jnp.broadcast_to(rows[0:1, lanes], (CHUNKS, block))
        half_angular = jnp.broadcast_to(rows[1:2, lanes], (CHUNKS, block))

        def one_step(i, carry):
            a_re, a_im, x_re, x_im = carry
            at = pl.ds(pl.multiple_of(i * CHUNKS, CHUNKS), CHUNKS)
            step = step_wide[at, lanes]
            half = step * half_angular
            q = half * half
            sine = half + half * series(q, SIN)
            cosine = 1.0 + series(q, COS)
            factor = jnp.exp(step * minus_decay)
            twice = factor * (sine + sine)
            d_re = factor - twice * sine
            d_im = twice * cosine
            less = d_re - 1.0
            p_re = proj_re[at, lanes]
            p_im = proj_im[at, lanes]
            u_re = less * p_re - d_im * p_im
            u_im = less * p_im + d_im * p_re
            dec_re[at, lanes] = d_re
            dec_im[at, lanes] = d_im
            proj_re[at, lanes] = u_re
            proj_im[at, lanes] = u_im
            return (
                d_re * a_re - d_im * a_im,
                d_re * a_im + d_im * a_re,
                d_re * x_re - d_im * x_im + u_re,
                d_re * x_im + d_im * x_re + u_im,
            )

        zero = jnp.zeros((CHUNKS, block), f32)
        found = lax.fori_loop(0, tokens // CHUNKS, one_step, (zero + 1.0, zero, zero, zero), unroll=2)
        for k in range(4):
            ends[k, :, lanes] = found[k]
        return 0

    lax.fori_loop(first, last, one_block, 0)


def chain(early, late):
    return (
        early[0] * late[0] - early[1] * late[1],
        early[0] * late[1] + early[1] * late[0],
        late[0] * early[2] - late[1] * early[3] + late[2],
        late[0] * early[3] + late[1] * early[2] + late[3],
    )


def chunk_prefix(ends, total, total_x, wide_x):
    width = ends.shape[2]
    value = tuple(ends[k] for k in range(4))
    row = lax.broadcasted_iota(jnp.int32, value[0].shape, 0)
    unit = (1.0, 0.0, 0.0, 0.0)

    def moved(value, by):
        return tuple(
            jnp.where(row >= by, pltpu.roll(part, by, 0), zero) for part, zero in zip(value, unit)
        )

    for by in (1, 2, 4):
        value = chain(moved(value, by), value)
    for k in range(4):
        for j in range(width // 128):
            kept = total if k < 2 else wide_x
            at = 8 * (k % 2) + j
            kept[at : at + 1, :] = value[k][CHUNKS - 1 :, 128 * j : 128 * j + 128]
    total_x[...] = wide_x[...].astype(bf16)
    before = moved(value, 1)
    for k in range(4):
        ends[k] = before[k]


def second_pass(dec_re, dec_im, feed_re, feed_im, ends, carry, states):
    tokens, width = dec_re.shape
    block = 512
    for b in range(width // block):
        lanes = pl.ds(b * block, block)
        lanes_im = pl.ds(width + b * block, block)
        per = block // 128
        h_re = jnp.concatenate([carry[per * b + j : per * b + j + 1, :] for j in range(per)], axis=1)
        h_im = jnp.concatenate([carry[8 + per * b + j : 9 + per * b + j, :] for j in range(per)], axis=1)
        a_re, a_im = ends[0, :, lanes], ends[1, :, lanes]
        x_re = ends[2, :, lanes] + a_re * h_re - a_im * h_im
        x_im = ends[3, :, lanes] + a_re * h_im + a_im * h_re

        def one_step(i, value):
            x_re, x_im = value
            seen = []
            for k in range(2):
                at = pl.ds(pl.multiple_of(i * 2 * CHUNKS + k * CHUNKS, CHUNKS), CHUNKS)
                d_re, d_im = dec_re[at, lanes], dec_im[at, lanes]
                x_re, x_im = (
                    d_re * x_re - d_im * x_im + feed_re[at, lanes],
                    d_re * x_im + d_im * x_re + feed_im[at, lanes],
                )
                seen.append((x_re, x_im))
            both = pl.ds(pl.multiple_of(i * 2 * CHUNKS, 2 * CHUNKS), 2 * CHUNKS)
            states[both, lanes] = jnp.concatenate([seen[0][0], seen[1][0]], axis=0).astype(bf16)
            states[both, lanes_im] = jnp.concatenate([seen[0][1], seen[1][1]], axis=0).astype(bf16)
            return x_re, x_im

        lax.fori_loop(0, tokens // (2 * CHUNKS), one_step, (x_re, x_im), unroll=2)


def read_out(states, wout, uperm, skip_ref):
    tokens = states.shape[0]
    span = tokens // CHUNKS
    out = dot_t(states[...], wout[...]) + skip_ref[...] * uperm[...].astype(f32)
    mixed = jax.nn.gelu(out).astype(bf16)
    back = onehot((tokens, tokens), lambda r, c: r == (c % CHUNKS) * span + c // CHUNKS)
    return dot(back, mixed).astype(bf16)


AXES = pl.DeviceIdType.MESH
SIDE = 4


def around(index, by):
    return lax.rem(index + by + SIDE, SIDE)


class Relay:
    def __init__(self, buf, first, rows, send_sem, recv_sem, own=None):
        here = lax.axis_index("sp")
        self.zy = here // SIDE, lax.rem(here, SIDE)
        self.buf, self.first, self.rows, self.own = buf, first, rows, own
        self.shard = buf.shape[0] // (SIDE * SIDE)
        self.send_sem, self.recv_sem = send_sem, recv_sem
        self.sent = 0

    def index(self, side, dp, dq):
        dz, dy = (dq, dp) if side == 0 else (dp, dq)
        return around(self.zy[0], dz) * SIDE + around(self.zy[1], dy)

    def group(self, dp, dq, half):
        if dq == 0:
            return 2 if dp == 2 else int((dp == -1) == (half == 1))
        return 3 + dp % SIDE if dq != 2 and (dq == -1) == (half == 0) else 7

    def send(self, side, dp, dq, half, to_p, to_q):
        width = self.buf.shape[1] // 2
        cols = slice(half * width, half * width + width)
        row = pl.multiple_of(self.index(side, dp, dq) * self.shard + side * self.rows, self.rows)
        piece = self.buf.at[pl.ds(row, self.rows), cols]
        own = self.own is not None and dp == 0 and dq == 0
        first = self.first + side * self.rows
        seen = [(d + 1) % SIDE - 1 for d in (dp - to_p, dq - to_q)]
        pltpu.make_async_remote_copy(
            src_ref=self.own.at[first : first + self.rows, cols] if own else piece,
            dst_ref=piece,
            send_sem=self.send_sem,
            recv_sem=self.recv_sem.at[self.group(*seen, half)],
            device_id={"sp": self.index(side, to_p, to_q), "tp": lax.axis_index("tp")},
            device_id_type=AXES,
        ).start()
        self.sent += 1

    def whole(self, count, group):
        rows = self.buf.at[: count * self.rows // 2, :]
        return pltpu.make_async_remote_copy(
            src_ref=rows,
            dst_ref=rows,
            send_sem=self.send_sem,
            recv_sem=self.recv_sem.at[group],
            device_id={"sp": self.index(0, 1, 0), "tp": lax.axis_index("tp")},
            device_id_type=AXES,
        )

    def arrived(self, group):
        self.whole(32 if group == 7 else 4, group).wait_recv()

    def send_p(self, k):
        for side in range(2):
            self.send(side, 0, 0, k, 1, 0)
            self.send(side, 0, 0, 1 - k, -1, 0)

    def send_q(self, dp, k):
        for side in range(2):
            self.send(side, dp, 0, k, 0, 1)
            self.send(side, dp, 0, 1 - k, 0, -1)

    def forward_p(self):
        self.arrived(0)
        for side in range(2):
            self.send(side, -1, 0, 0, 1, 0)
            self.send(side, 1, 0, 1, -1, 0)

    def near(self):
        self.arrived(1)
        self.send_q(-1, 0)
        self.send_q(1, 0)

    def near_rest(self):
        self.send_q(-1, 1)
        self.send_q(1, 1)

    def far(self):
        self.arrived(2)
        self.send_q(2, 0)

    def far_rest(self):
        self.send_q(2, 1)

    def forward_q(self, dp):
        self.arrived(3 + dp % SIDE)
        for side in range(2):
            self.send(side, dp, -1, 0, 0, 1)
            self.send(side, dp, 1, 1, 0, -1)

    def finish(self):
        self.arrived(7)

    def drain(self):
        self.whole(self.sent, 0).wait_send()


class Gather:
    def __init__(self, buf, send_sem, recv_sem):
        here = lax.axis_index("tp")
        self.x, self.core = here // 2, lax.rem(here, 2)
        self.buf, self.send_sem, self.recv_sem = buf, send_sem, recv_sem
        self.sent = 0

    def device(self, dx, other=False):
        return around(self.x, dx) * 2 + (1 - self.core if other else self.core)

    def cols(self, core):
        width = self.buf.shape[2] // 2
        return pl.ds(pl.multiple_of(core * width, width), width)

    def send(self, dx, half, to_x):
        rows = self.buf.shape[1] // 2
        piece = self.buf.at[around(self.x, dx), half * rows : half * rows + rows, self.cols(self.core)]
        if to_x:
            seen = (dx - to_x + 1) % SIDE - 1
            group = 2 if seen == 2 else int((seen == -1) == (half == 1))
        else:
            group = 3 + dx % SIDE
        pltpu.make_async_remote_copy(
            src_ref=piece,
            dst_ref=piece,
            send_sem=self.send_sem,
            recv_sem=self.recv_sem.at[group],
            device_id={"sp": lax.axis_index("sp"), "tp": self.device(to_x, not to_x)},
            device_id_type=AXES,
        ).start()
        self.sent += 1

    def whole(self, rows, group):
        return pltpu.make_async_remote_copy(
            src_ref=rows,
            dst_ref=rows,
            send_sem=self.send_sem,
            recv_sem=self.recv_sem.at[group],
            device_id={"sp": lax.axis_index("sp"), "tp": self.device(1)},
            device_id_type=AXES,
        )

    def arrived(self, group):
        self.whole(self.buf.at[0, :, : self.buf.shape[2] // 2], group).wait_recv()

    def start(self):
        for k in range(2):
            self.send(0, k, 1)
            self.send(0, 1 - k, -1)
        for k in range(2):
            self.send(0, k, 0)

    def near(self):
        self.arrived(0)
        self.send(-1, 0, 1)
        self.send(1, 1, -1)
        self.send(-1, 0, 0)
        self.send(1, 1, 0)
        self.arrived(1)
        self.send(-1, 1, 0)
        self.send(1, 0, 0)

    def far(self):
        self.arrived(2)
        self.send(2, 0, 0)
        self.send(2, 1, 0)

    def across(self, dx):
        self.arrived(3 + dx % SIDE)

    def drain(self):
        self.whole(self.buf.at[:, : self.buf.shape[1] * self.sent // 16, :], 0).wait_send()


class Phases:
    def __init__(self):
        self.scope = None

    def __call__(self, name):
        if self.scope is not None:
            self.scope.__exit__(None, None, None)
        self.scope = jax.named_scope(name) if name else None
        if self.scope is not None:
            self.scope.__enter__()


def layer_kernel(
    resid_hbm, u_hbm, ls_hbm, dr_hbm, fr_hbm, bm_hbm, cm_hbm, skip_hbm, gain_hbm, vw_ref, gw_ref, up_ref, down_ref,
    out_ref,
    resid_ref, u_ref, ls_ref, dr_ref, fr_ref, bm_ref, cm_ref, skip_ref, gain_ref,
    up_all, down_first, down_last, vg, dec_re, dec_im, feed_re, feed_im, step_wide, rows, ends, total, totals, total_x, totals_x, carry,
    uperm, wout, states, mixed_all, upd_all, glu, raised, squares, hidden,
    products, stage_far, relay_in, stage_near, from_near, kept, stage_own, from_own, own_part, kept_out,
    local_sem, round_sem, ring_send, ring_recv, tot_send, tot_recv, cross_send, cross_recv, sum_send, sum_recv,
):
    phase = Phases()
    here, lane = lax.axis_index("sp"), lax.axis_index("tp")
    planes = SIDE * SIDE
    tokens, piece = resid_ref.shape
    half = tokens // 2
    shard = up_ref.shape[0]
    mix = Gather(mixed_all, ring_send.at[3], ring_recv.at[3])
    upd = Gather(upd_all, ring_send.at[4], ring_recv.at[4])
    right, left, partner = mix.device(1), mix.device(-1), mix.device(0, True)

    up = Relay(up_all, 0, shard // 2, ring_send.at[0], ring_recv.at[0], up_ref)
    first = Relay(down_first, 0, shard // 8, ring_send.at[1], ring_recv.at[1])
    last = Relay(down_last, 0, shard // 8, ring_send.at[2], ring_recv.at[2])
    near_planes = [up.index(0, *by) for by in ((1, 0), (-1, 0), (0, 1), (0, -1))]

    phase("signal")
    barrier = pltpu.get_barrier_semaphore()
    for target in near_planes:
        pl.semaphore_signal(barrier, inc=1, device_id={"sp": target, "tp": lane}, device_id_type=AXES)
    for target in (right, left, partner):
        pl.semaphore_signal(barrier, inc=1, device_id={"sp": here, "tp": target}, device_id_type=AXES)

    own_up = pl.ds(pl.multiple_of(here * shard, shard), shard)
    slim, width = shard // 4, up_ref.shape[1]
    own_down = pl.ds(pl.multiple_of(here * slim, slim), slim)
    own_units = pl.ds(pl.multiple_of(mix.core * width, width), width)

    def down_rows(core, k):
        return down_ref.at[pl.ds(pl.multiple_of(core * 2 * slim + k * slim, slim), slim), :]

    def cross_copy(number, src, dst):
        return pltpu.make_async_remote_copy(
            src_ref=src,
            dst_ref=dst,
            send_sem=cross_send.at[number],
            recv_sem=cross_recv.at[number],
            device_id={"sp": here, "tp": partner},
            device_id_type=AXES,
        )

    crossing = [
        cross_copy(k, down_rows(1 - mix.core, k), buf.at[own_down, own_units])
        for k, buf in enumerate((down_first, down_last))
    ]
    moves = (
        (u_hbm, u_ref), (dr_hbm, dr_ref), (fr_hbm, fr_ref), (ls_hbm, ls_ref), (bm_hbm, bm_ref), (cm_hbm, cm_ref),
        (up_ref, up_all.at[own_up, :]),
        (down_rows(mix.core, 0), down_first.at[own_down, own_units]),
        (down_rows(mix.core, 1), down_last.at[own_down, own_units]),
        (skip_hbm, skip_ref), (vw_ref, vg.at[:, :piece]), (gw_ref, vg.at[:, piece:]),
        (resid_hbm, resid_ref), (gain_hbm, gain_ref),
    )
    local = [pltpu.make_async_copy(src, dst, local_sem.at[k]) for k, (src, dst) in enumerate(moves)]
    for copy in local:
        copy.start()
    phase("barrier")
    pl.semaphore_wait(barrier, 7)
    phase("start_p")
    up.send_p(0)
    up.send_p(1)
    up.send_q(0, 0)
    up.send_q(0, 1)
    for copy in crossing:
        copy.start()

    def greet(number):
        for target in near_planes:
            pl.semaphore_signal(
                round_sem.at[number], inc=1, device_id={"sp": target, "tp": lane}, device_id_type=AXES
            )

    greet(0)
    for copy in local[:6]:
        copy.wait()
    phase("prepare")
    prepare(u_ref, ls_ref, dr_ref, fr_ref, bm_ref, cm_ref, uperm, step_wide, feed_re, feed_im, rows, wout)
    pl.semaphore_wait(round_sem.at[0], 4)
    greet(1)
    phase("first_pass")
    scan_refs = (step_wide, feed_re, feed_im, rows, dec_re, dec_im, ends)
    first_pass(*scan_refs, 0, 2)
    pl.semaphore_wait(round_sem.at[1], 4)
    greet(2)
    for copy in local[6:9]:
        copy.wait()
    for copy in crossing:
        copy.wait_recv()
    first.send_p(0)
    first_pass(*scan_refs, 2, 4)
    phase("chunk")
    chunk_prefix(ends, total, total_x, carry)
    pl.semaphore_wait(round_sem.at[2], 4)

    def total_copy(k, src, dst, target):
        return pltpu.make_async_remote_copy(
            src_ref=src,
            dst_ref=dst,
            send_sem=tot_send.at[k],
            recv_sem=tot_recv.at[k],
            device_id={"sp": target, "tp": lane},
            device_id_type=AXES,
        )

    phase("totals")
    for by in range(1, planes):
        @pl.when(here + by < planes)
        def _():
            for k, (src, dst) in enumerate(((total, totals), (total_x, totals_x))):
                total_copy(k, src, dst.at[here], lax.rem(here + by, planes)).start()

    phase("serve1")
    up.forward_p()
    up.near()
    up.forward_q(0)
    up.near_rest()

    phase("fold")

    for count in range(1, planes):
        @pl.when(here == count)
        def _():
            for k, part in enumerate((totals, totals_x)):
                total_copy(k, part.at[:count], part.at[:count], lax.rem(here + 1, planes)).wait_recv()

    def fold(j, value):
        h_re, h_im = value
        a_re, a_im = totals[j, 0:8, :], totals[j, 8:16, :]
        x_both = totals_x[j].astype(f32)
        x_re, x_im = x_both[0:8], x_both[8:16]
        return a_re * h_re - a_im * h_im + x_re, a_re * h_im + a_im * h_re + x_im

    zero = jnp.zeros((8, 128), f32)
    h_re, h_im = lax.fori_loop(0, here, fold, (zero, zero))
    carry[0:8, :] = h_re
    carry[8:16, :] = h_im
    phase("second_pass")
    second_pass(dec_re, dec_im, feed_re, feed_im, ends, carry, states)
    phase("serve2")
    up.far()
    up.far_rest()
    first.send_p(1)
    local[9].wait()
    phase("read_out")
    own_cols = mix.cols(mix.core)
    mixed_all[mix.x, :, own_cols] = read_out(states, wout, uperm, skip_ref)
    phase("mix_start")
    mix.start()

    depth = 2 * piece

    def glu_part(chip, core=None):
        if core is None:
            lhs, at = mixed_all[chip], pl.ds(pl.multiple_of(chip * depth, depth), depth)
        else:
            lhs, at = mixed_all[chip, :, mix.cols(core)], pl.ds(pl.multiple_of((chip * 2 + core) * piece, piece), piece)
        return dot(lhs, vg[at, :])

    phase("mix_own")
    for copy in local[10:]:
        copy.wait()
    mix.across(0)
    glu[...] = glu_part(mix.x)
    phase("serve3")
    up.forward_q(-1)
    up.forward_q(1)
    first.send_q(0, 0)
    first.send_q(0, 1)
    phase("mix_near")
    mix.near()
    phase("mix_left")
    mix.across(-1)
    glu[...] += glu_part(around(mix.x, -1))
    phase("serve4")
    up.forward_q(2)
    phase("mix_right")
    mix.across(1)
    glu[...] += glu_part(around(mix.x, 1))
    phase("mix_far")
    mix.far()
    phase("mix_last")
    far_chip = around(mix.x, 2)
    glu[...] += glu_part(far_chip, mix.core)
    mix.across(2)
    glu[...] += glu_part(far_chip, 1 - mix.core)
    phase("updated")
    updated = (resid_ref[...].astype(f32) + glu[:, :piece] * jax.nn.sigmoid(glu[:, piece:])).astype(bf16)
    upd_all[upd.x, :, own_cols] = updated
    phase("upd_start")
    upd.start()
    phase("serve5")
    first.forward_p()
    first.near()
    first.near_rest()
    last.send_p(0)
    last.send_p(1)

    def up_part(chip, start, core=None):
        if core is None:
            wide, at = upd_all[chip], pl.ds(pl.multiple_of(chip * depth, depth), depth)
        else:
            wide, at = upd_all[chip, :, upd.cols(core)], pl.ds(pl.multiple_of((chip * 2 + core) * piece, piece), piece)
        wide = wide.astype(f32)
        square = wide * wide
        square = sum(square[:, 128 * k : 128 * k + 128] for k in range(square.shape[1] // 128))
        product = dot((wide * gain_ref[:, at]).astype(bf16), up_all[at, :])
        if start:
            squares[...] = square
            raised[...] = product
        else:
            squares[...] += square
            raised[...] += product

    phase("up_wait")
    up.finish()
    phase("upd_own")
    upd.across(0)
    up_part(upd.x, True)
    phase("serve6")
    first.forward_q(0)
    first.far()
    last.send_q(0, 0)
    first.far_rest()
    last.send_q(0, 1)
    phase("upd_near")
    upd.near()
    phase("upd_left")
    upd.across(-1)
    last.forward_p()
    up_part(around(upd.x, -1), False)
    phase("serve7")
    first.forward_q(-1)
    first.forward_q(1)
    phase("upd_right")
    upd.across(1)
    up_part(around(upd.x, 1), False)
    phase("serve8")
    first.forward_q(2)
    last.near()
    last.send_q(-1, 1)
    phase("upd_far")
    upd.far()
    up_part(far_chip, False, upd.core)
    phase("upd_last")
    upd.across(2)
    up_part(far_chip, False, 1 - upd.core)
    phase("hidden")
    inv_rms = lax.rsqrt(jnp.sum(squares[...], axis=1, keepdims=True) / (SIDE * depth) + rms_eps)
    active = jnp.maximum(raised[...] * inv_rms, 0.0)
    hidden[:, own_units] = (active * active).astype(bf16)
    crossing.append(cross_copy(2, hidden.at[:, own_units], hidden.at[:, own_units]))
    crossing[2].start()
    phase("serve9")
    last.far()
    last.forward_q(0)
    last.send_q(1, 1)
    last.far_rest()

    span = piece // 2
    quarter = half // 2

    chunk = quarter // 2

    def turned(value, by=None):
        return pltpu.roll(value, span // 2 if by is None else by, 1)

    low_lanes = lax.broadcasted_iota(jnp.int32, (chunk, span), 1) < span // 2

    def packed(value, core):
        parts = []
        for c in range(value.shape[0] // quarter):
            top, low = (value[c * quarter + k * chunk : c * quarter + k * chunk + chunk] for k in range(2))
            parts.append(jnp.where(low_lanes, top, turned(low)) if core == 0 else jnp.where(low_lanes, turned(top), low))
        return jnp.concatenate(parts, axis=0)

    class Sum:
        def __init__(self, k, buf):
            self.k, self.buf = k, buf
            self.relays = [
                [
                    self.copy(
                        0, 2 * j + c, stage_far.at[k, j, c * quarter : c * quarter + quarter],
                        relay_in.at[k, j, c * quarter : c * quarter + quarter], target,
                    )
                    for c in range(2)
                ]
                for j, target in enumerate((right, left))
            ]
            self.own = self.copy(1, 4, stage_own.at[k], from_own.at[k], partner)
            self.near = self.copy(2, 5, stage_near.at[k], from_near.at[k], right)

        def copy(self, send, recv, src, dst, target):
            return pltpu.make_async_remote_copy(
                src_ref=src,
                dst_ref=dst,
                send_sem=sum_send.at[self.k, send],
                recv_sem=sum_recv.at[self.k, recv],
                device_id={"sp": here, "tp": target},
                device_id_type=AXES,
            )

        def product(self, dx):
            return products[:, pl.ds(pl.multiple_of(around(mix.x, dx) * span, span), span)]

        def send_near(self, side, part, value, first=0):
            chip = around(mix.x, 1 - 2 * side)
            rows = slice(first, first + value.shape[0] // 2)
            for core in range(2):
                stage_near[self.k, side, core, part, rows] = packed(value, core).astype(bf16)
                self.copy(
                    2, 5, stage_near.at[self.k, side, core, part, rows],
                    from_near.at[self.k, mix.core, side, part, rows], chip * 2 + core,
                ).start()

        def start(self, *serve):
            k = self.k
            products[...] = dot_t(hidden[...], self.buf[...])
            far = self.product(2).astype(bf16)
            for j in range(2):
                stage_far[k, j] = far[j * half : j * half + half]
            for c in range(2):
                for j in range(2):
                    self.relays[j][c].start()
            near = self.product(1)
            self.send_near(0, 1, near[half:])
            kept[k, 0] = near[:half]
            near = self.product(-1)
            self.send_near(1, 0, near[:half])
            kept[k, 1] = near[half:]
            if serve:
                serve[0]()
            own = self.product(0)
            for j in range(2):
                both = [packed(own[j * half : j * half + half], core) for core in range(2)]
                own_part[k, j] = jnp.where(mix.core == 0, both[0], both[1])
                stage_own[k, j] = jnp.where(mix.core == 0, both[1], both[0]).astype(bf16)
            self.own.start()
            if serve:
                serve[1]()

        def relay(self):
            k = self.k
            for c in range(2):
                rows = slice(c * quarter, c * quarter + quarter)
                for j in range(2):
                    self.relays[j][c].wait_recv()
                    self.send_near(j, j, kept[k, j, rows] + relay_in[k, j, rows].astype(f32), c * chunk)

        def result(self):
            k = self.k
            self.own.wait_recv()
            self.near.wait_recv()
            found = []
            for core in range(2):
                rows = []
                for j in range(2):
                    here_part = jnp.where(mix.core == core, own_part[k, j], from_own[k, j].astype(f32))
                    total = here_part + (from_near[k, core, 0, j].astype(f32) + from_near[k, core, 1, j].astype(f32))
                    for c in range(2):
                        part = total[c * chunk : c * chunk + chunk]
                        rows += [part, turned(part)]
                found.append(jnp.concatenate(rows, axis=0))
            return found

        def drain(self):
            self.own.wait_send()
            self.near.wait_send()
            self.copy(0, 0, stage_far.at[self.k], stage_far.at[self.k], right).wait_send()

    phase("first_wait")
    first.finish()
    crossing[2].wait_recv()
    phase("first_sum")
    early, late = Sum(0, down_first), Sum(1, down_last)

    def serve_near():
        last.forward_q(-1)
        last.forward_q(1)

    def serve_far():
        last.forward_q(2)

    early.start(serve_near, serve_far)
    phase("first_relay")
    early.relay()
    phase("last_wait")
    last.finish()
    phase("last_sum")
    late.start()
    phase("last_relay")
    late.relay()
    phase("first_result")
    lane_group = lax.broadcasted_iota(jnp.int32, (tokens, span), 1) // slim
    blocks = [upd_all[upd.x, :, own_cols].astype(f32)[:, b * span : b * span + span] for b in range(2)]

    def put_in(k, found):
        for b in range(2):
            for core in range(2):
                place = core * 2 + k
                moved = turned(found[core], (place - b) % 4 * slim) if place != b else found[core]
                blocks[b] = blocks[b] + jnp.where(lane_group == place, moved, 0.0)

    put_in(0, early.result())
    for b in range(2):
        kept_out[:, b * span : b * span + span] = blocks[b]
    phase("last_result")
    two = late.result()
    phase("result")
    blocks = [kept_out[:, b * span : b * span + span] for b in range(2)]
    put_in(1, two)
    out_ref[...] = jnp.concatenate(blocks, axis=1).astype(bf16)

    phase("drain")
    for count in range(1, planes):
        @pl.when(planes - 1 - here == count)
        def _():
            for k, part in enumerate((totals, totals_x)):
                total_copy(k, part.at[:count], part.at[:count], lax.rem(here + 1, planes)).wait_send()

    for part in (up, first, last, mix, upd, early, late):
        part.drain()
    for copy in crossing:
        copy.wait_send()
    phase(None)


def per_device(
    resid, mixer_in, log_step, decay_real, frequency, input_matrix, output_matrix, skip_gain,
    value_weight, gate_weight, norm_gain, up_weight, down_weight,
):
    tokens, channels = mixer_in.shape
    groups, states = decay_real.shape
    width = groups * states
    planes, slots = lax.axis_size("sp"), lax.axis_size("tp")
    features = slots * channels
    hidden = up_weight.shape[1]
    span = channels // 2
    vmem = pl.BlockSpec(memory_space=pltpu.VMEM)
    hbm = pl.BlockSpec(memory_space=pl.ANY)
    wide = pltpu.VMEM((tokens, width), f32)
    block = pltpu.VMEM((tokens, channels), bf16)
    halves = pltpu.VMEM((2, 2, tokens // 2, span), bf16)
    packs = pltpu.VMEM((2, 2, tokens // 4, span), bf16)
    near = pltpu.VMEM((2, 2, 2, 2, tokens // 4, span), bf16)
    pieces = pltpu.VMEM((SIDE, tokens, 2 * channels), bf16)
    matrix = pltpu.VMEM((2, channels, states), f32)
    down = pltpu.VMEM((features // 4, 2 * hidden), bf16)
    dma = pltpu.SemaphoreType.DMA
    return pl.pallas_call(
        layer_kernel,
        out_shape=pltpu.VMEM((tokens, channels), bf16),
        in_specs=[hbm] * 13,
        out_specs=vmem,
        scratch_shapes=[
            block, block, pltpu.VMEM((groups, tokens), f32),
            pltpu.VMEM((groups, states), f32), pltpu.VMEM((groups, states), f32), matrix, matrix,
            pltpu.VMEM((1, channels), f32), pltpu.VMEM((1, features), f32),
            pltpu.VMEM((features, hidden), bf16), down, down, pltpu.VMEM((features, 2 * channels), bf16),
            wide, wide, wide, wide, wide,
            pltpu.VMEM((8, width), f32), pltpu.VMEM((4, CHUNKS, width), f32),
            pltpu.VMEM((16, 128), f32), pltpu.VMEM((planes, 16, 128), f32),
            pltpu.VMEM((16, 128), bf16), pltpu.VMEM((planes, 16, 128), bf16), pltpu.VMEM((16, 128), f32),
            block, pltpu.VMEM((channels, 2 * width), bf16), pltpu.VMEM((tokens, 2 * width), bf16),
            pieces, pieces, pltpu.VMEM((tokens, 2 * channels), f32),
            pltpu.VMEM((tokens, hidden), f32), pltpu.VMEM((tokens, 128), f32), pltpu.VMEM((tokens, 2 * hidden), bf16),
            pltpu.VMEM((tokens, SIDE * span), f32), halves, halves, near, near, pltpu.VMEM((2, 2, tokens // 2, span), f32),
            packs, packs, pltpu.VMEM((2, 2, tokens // 4, span), f32), pltpu.VMEM((tokens, channels), f32),
            dma((14,)), pltpu.SemaphoreType.REGULAR((3,)), dma((5,)), dma((5, 8)),
            dma((2,)), dma((2,)), dma((3,)), dma((3,)), dma((2, 3)), dma((2, 6)),
        ],
        name="layer",
        compiler_params=pltpu.CompilerParams(
            vmem_limit_bytes=58 * 2**20, collective_id=0, has_side_effects=True
        ),
    )(
        resid, mixer_in, log_step.T, decay_real, frequency,
        input_matrix.transpose(0, 1, 3, 2).reshape(2, channels, states), output_matrix.reshape(2, channels, states),
        skip_gain.reshape(1, -1), norm_gain.reshape(1, -1), value_weight, gate_weight, up_weight, down_weight,
    )


def solution(mesh):
    in_specs = (
        P("sp", "tp"), P("sp", "tp"), P("sp", "tp"), P("tp", None), P("tp", None),
        P(None, "tp", None, None), P(None, "tp", None, None), P("tp"),
        P(None, "tp"), P(None, "tp"), P(), P("sp", "tp"), P("sp", "tp"),
    )
    return jax.shard_map(
        per_device, mesh=mesh, in_specs=in_specs, out_specs=P("sp", "tp"), check_vma=False
    )
```
